512 devices in a mesh: sp: 32 (over z, x), tp: 16 (over y, core).
Axes of the slice: x: 4, y: 8, z: 8, core: 2. Of those that a mesh axis runs over, the one named last changes fastest.
Arguments:
- readout_query_vectors: bfloat16 [8192, 2048], P('sp', 'tp'), may hold values from -6 to 6
- attention_key_vectors: bfloat16 [8192, 2048], P('sp', 'tp'), may hold values from -6 to 6
- attention_content_vectors: bfloat16 [8192, 2048], P('sp', 'tp'), may hold values from -6 to 6
- step_size_preactivation: bfloat16 [8192, 2048], P('sp', 'tp'), may hold values from -16 to 8
- forgetting_preactivation: float32 [8192, 2048], P('sp', 'tp'), may hold values from -22 to 3
- extra_forgetting_bias: float32 [8192, 32], P('sp', 'tp'), may hold values from -0.7 to 0
- subspace_normalizer_gain: float32 [2048], P('tp'), may hold values from 0.1 to 1.9
- skip_connection_stream: bfloat16 [8192, 2048], P('sp'), may hold values from -40 to 40
- blender_projection_matrix: bfloat16 [2048, 2048], P('tp'), may hold values from -0.125 to 0.125
- specialist_prenormal_gain: float32 [2048], replicated, may hold values from 0.1 to 1.9
- cluster_router_chance: float32 [8192], P('sp'), may hold values from 0.4 to 1
- specialist_chance_within_cluster: float32 [8192, 2], P('sp'), may hold values from 0.1 to 1
- chosen_specialist_ids: int32 [8192, 2], P('sp'), may hold values from 0 to 31, all different within a row; in each aligned block of 256 rows (0 to 255, 256 to 511, ...) at most 32 rows name the same one
- specialist_switch_matrix: bfloat16 [32, 2048, 2048], P('sp', None, 'tp'), may hold values from -0.125 to 0.125
- specialist_expansion_matrix: bfloat16 [32, 2048, 2048], P('sp', None, 'tp'), may hold values from -0.125 to 0.125
- specialist_contraction_matrix: bfloat16 [32, 2048, 2048], P('sp', 'tp'), may hold values from -0.375 to 0.375
Outputs:
- layer_out: bfloat16 [8192, 2048], P('sp')
The draws below stay inside these ranges and needn't reach their ends.
Inputs may be any that keep to these rules, and one draw needn't show every extreme that they name: `chosen_specialist_ids`: in each aligned block of 256 rows every expert is named at most 32 times.
All inputs are finite; a program needn't handle non-finite values.
Results may differ from the reference program's by a relative error of at most 0.022.
Values may be sent and summed in bfloat16 or wider, within the bound.
No kernel may reach another device: no remote copies, remote signals or barrier semaphores. Data moves between devices by JAX's collectives and lax.ppermute only.
A program may use at most 64 MiB of HBM per device.

```python
import math
import jax
import jax.numpy as jnp
import numpy as np
from jax import lax

D = 2048
HEAD_DIM = 64
HEAD_TOTAL = 32
FF = 2048
TOP = 2
TOK_DEV = 256
TOKEN_TOTAL = 8192
EXPERTS = 32
CAP = 32
N_SP = 32
N_TP = 16


def slow_heads(key):
    chance = jax.random.uniform(jax.random.fold_in(key, 11), (HEAD_TOTAL,))
    return chance < 0.5


def draw_forgetting_preactivation(key, part):
    slow = slow_heads(key)
    head_base = jnp.where(slow, jnp.log(0.7 / TOKEN_TOTAL) + 0.5, -3.2)
    first_key = jax.random.fold_in(key, 3)
    second_key = jax.random.fold_in(key, 4)
    third_key = jax.random.fold_in(key, 5)
    jitter = 0.3 * jax.random.normal(first_key, (HEAD_TOTAL,))
    offset = jax.random.uniform(second_key, (TOKEN_TOTAL // 64, HEAD_TOTAL), minval=-0.7, maxval=0.7)
    offset = jnp.repeat(offset, 64, axis=0)
    noise_part = 0.6 * jax.random.normal(third_key, (TOKEN_TOTAL, HEAD_TOTAL, HEAD_DIM))
    result = head_base[None, :, None] + jitter[None, :, None] + offset[:, :, None] + noise_part
    return result.reshape(TOKEN_TOTAL, HEAD_TOTAL * HEAD_DIM).astype(jnp.float32)


def draw_step_size_preactivation(key, part):
    slow = slow_heads(key)
    head_base = jnp.where(slow, jnp.log(0.25 * HEAD_DIM / TOKEN_TOTAL), 0.0)
    noise_key = jax.random.fold_in(key, 6)
    noise_part = 0.8 * jax.random.normal(noise_key, (TOKEN_TOTAL, HEAD_TOTAL, HEAD_DIM))
    result = head_base[None, :, None] + noise_part
    return result.reshape(TOKEN_TOTAL, HEAD_TOTAL * HEAD_DIM).astype(jnp.bfloat16)


def draw_extra_forgetting_bias(key, part):
    spike_positions = jax.random.randint(jax.random.fold_in(key, 1), (8,), 0, TOKEN_TOTAL)
    spiked_values = jnp.any(jnp.arange(TOKEN_TOTAL)[:, None] == spike_positions[None, :], axis=1)
    spike_depth = jnp.log(jax.random.uniform(jax.random.fold_in(key, 2), (TOKEN_TOTAL, HEAD_TOTAL), minval=0.5, maxval=0.8))
    return jnp.where(spiked_values[:, None], spike_depth, 0.0).astype(jnp.float32)


def draw_skip_connection_stream(key, part):
    column = jnp.exp(jax.random.uniform(jax.random.fold_in(key, 1), (D,), minval=-0.6, maxval=0.6))
    result = jax.random.normal(jax.random.fold_in(key, 2), (TOKEN_TOTAL, D)) * column
    return result.astype(jnp.bfloat16)


def steps_of(key, extent, shards, low, top_value):
    level, own = 1.0, jax.random.fold_in(key, 6)
    for position, parts in shards:
        steps = jnp.exp(jax.random.uniform(jax.random.fold_in(own, position), (parts,), jnp.float32, low / len(shards), top_value / len(shards)))
        level = level * jnp.repeat(steps, extent[position] // parts).reshape([-1 if axis == position else 1 for axis in range(len(extent))])
    return level


def assign_block(stream_key, own, number, rows, number_of, top, limit, skew):
    order = jax.random.permutation(stream_key, number_of)
    heavy_load, common = portions_of(number_of, rows * top, limit, skew, True), portions_of(number_of, rows * top, limit, skew, False)
    places = jnp.arange(number_of)

    def named(sizes, rotation):
        used = int((sizes > 0).sum())
        fixed = max(1, used // 4)
        moved = fixed + (places - fixed + rotation * (used - fixed)) % max(1, number_of - fixed)
        return jnp.zeros((number_of,), jnp.int32).at[order[jnp.where(places < fixed, places, moved)]].set(jnp.asarray(sizes, jnp.int32))

    sizes = jnp.where(number % 4 == 0, named(heavy_load, number // 4), named(common, number - number // 4 - 1))
    mixed = jax.random.permutation(jax.random.fold_in(own, 3), number_of)
    source_of, receiver = mixed[0:number_of // 2 * 2:2], mixed[1:number_of // 2 * 2:2]
    margin = jnp.minimum(sizes[source_of] - 1, limit - sizes[receiver]) // 2
    margin = jnp.where((source_of == order[0]) | (receiver == order[0]) | (sizes[receiver] == 0), 0, jnp.maximum(margin, 0))
    moved = jax.random.randint(jax.random.fold_in(own, 4), (number_of // 2,), 0, 1 << 20) % (margin + 1)
    sizes = sizes.at[source_of].add(-moved).at[receiver].add(moved)
    members = jnp.searchsorted(jnp.cumsum(sizes), jnp.arange(rows * top), side="right").astype(jnp.int32)
    grid = members.reshape(top, rows).T
    grid = grid[jax.random.permutation(jax.random.fold_in(own, 1), rows)]
    rotation = jax.random.randint(jax.random.fold_in(own, 2), (rows, 1), 0, top)
    return jnp.take_along_axis(grid, (jnp.arange(top)[None, :] + rotation) % top, axis=1)


def portions_of(number_of, total, most, skew, full):
    loads = [(1 << 20) // math.isqrt(standing ** skew) + 1 for standing in range(1, number_of + 1)]
    largest = most if full else min(most, max(-(-total // number_of), total * loads[0] // sum(loads)))
    least = 1 if total - largest >= number_of - 1 else 0
    holding, rest = [largest] + [least] * (number_of - 1), total - largest - least * (number_of - 1)
    while rest > 0:
        free = [i for i in range(1, number_of) if holding[i] < largest] or [i for i in range(1, number_of) if holding[i] < most]
        pool, remaining = sum([loads[i] for i in free]), rest
        for i in free:
            addition = min(most - holding[i], max(1, remaining * loads[i] // pool), rest)
            holding[i] = holding[i] + addition
            rest = rest - addition
    return np.array(holding)


def centred(rng, extent, deviation, most, pieces=(), held_as=jnp.bfloat16):
    gain = steps_of(rng, extent, pieces, -0.22, 0.18) if pieces else 1.0
    values = jax.random.normal(rng, extent, jnp.float32) * deviation * gain
    return jnp.minimum(jnp.maximum(values, -most), most).astype(held_as)


def setup_inputs(seed: int = 0) -> dict:
    key_of = jax.random.split(jax.random.key(seed), 17)
    readout_query_vectors = centred(key_of[0], (TOKEN_TOTAL, D), 1.0, 6.0, ((0, 32), (1, 16)))
    attention_key_vectors = centred(key_of[1], (TOKEN_TOTAL, D), 1.0, 6.0, ((0, 32), (1, 16)))
    attention_content_vectors = centred(key_of[2], (TOKEN_TOTAL, D), 1.0, 6.0, ((0, 32), (1, 16)))
    step_size_preactivation = draw_step_size_preactivation(jax.random.fold_in(key_of[16], 71), 0)
    forgetting_preactivation = draw_forgetting_preactivation(jax.random.fold_in(key_of[16], 71), 0)
    extra_forgetting_bias = draw_extra_forgetting_bias(jax.random.fold_in(key_of[16], 71), 0)
    subspace_normalizer_gain = jnp.clip(1.0 + 0.18 * jax.random.normal(key_of[6], (D,), jnp.float32), 0.1, 1.9)
    skip_connection_stream = draw_skip_connection_stream(jax.random.fold_in(key_of[16], 71), 0)
    blender_projection_matrix = centred(key_of[8], (D, D), D ** -0.5, 0.125, ((0, 16),))
    specialist_prenormal_gain = jnp.clip(1.0 + 0.18 * jax.random.normal(key_of[9], (D,), jnp.float32), 0.1, 1.9)
    cluster_router_chance = jnp.clip(0.4 + 0.6 * jax.random.uniform(key_of[10], (TOKEN_TOTAL,), jnp.float32) ** steps_of(key_of[10], (TOKEN_TOTAL,), ((0, 32),), -0.2, 0.2), 0.4, 1.0)
    specialist_chance_within_cluster = jnp.clip(0.1 + 0.9 * jax.random.uniform(key_of[11], (TOKEN_TOTAL, TOP), jnp.float32) ** steps_of(key_of[11], (TOKEN_TOTAL, TOP), ((0, 32),), -0.2, 0.2), 0.1, 1.0)
    chosen_specialist_ids_keys = jax.random.split(jax.random.fold_in(key_of[12], 1), TOKEN_TOTAL // TOK_DEV)
    chosen_specialist_ids_turns = jax.random.permutation(jax.random.fold_in(key_of[12], 3), TOKEN_TOTAL // TOK_DEV)
    chosen_specialist_ids = jax.vmap(lambda own, number: assign_block(jax.random.fold_in(key_of[12], 2), own, number, TOK_DEV, EXPERTS, TOP, CAP, 1))(chosen_specialist_ids_keys, chosen_specialist_ids_turns).reshape((TOKEN_TOTAL, TOP))
    specialist_switch_matrix = centred(key_of[13], (EXPERTS, D, FF), D ** -0.5, 0.125, ((0, 32), (2, 16)))
    specialist_expansion_matrix = centred(key_of[14], (EXPERTS, D, FF), D ** -0.5, 0.125, ((0, 32), (2, 16)))
    specialist_contraction_matrix = centred(key_of[15], (EXPERTS, FF, D), (FF // 8) ** -0.5, 0.375, ((0, 32), (1, 16)))
    return dict(readout_query_vectors=readout_query_vectors, attention_key_vectors=attention_key_vectors, attention_content_vectors=attention_content_vectors, step_size_preactivation=step_size_preactivation, forgetting_preactivation=forgetting_preactivation, extra_forgetting_bias=extra_forgetting_bias, subspace_normalizer_gain=subspace_normalizer_gain, skip_connection_stream=skip_connection_stream, blender_projection_matrix=blender_projection_matrix, specialist_prenormal_gain=specialist_prenormal_gain, cluster_router_chance=cluster_router_chance, specialist_chance_within_cluster=specialist_chance_within_cluster, chosen_specialist_ids=chosen_specialist_ids, specialist_switch_matrix=specialist_switch_matrix, specialist_expansion_matrix=specialist_expansion_matrix, specialist_contraction_matrix=specialist_contraction_matrix)


HIGH = lax.Precision.HIGHEST

def sequence_state_blender(readout_query_vectors, attention_key_vectors, attention_content_vectors, step_size_preactivation, forgetting_preactivation, extra_forgetting_bias, subspace_normalizer_gain):
    token_count = readout_query_vectors.shape[0]
    attention_subspace_count = extra_forgetting_bias.shape[1]

    def divide_among_subspaces(data):
        return data.astype(jnp.float32).reshape(token_count, attention_subspace_count, -1)
    query_rows = divide_among_subspaces(readout_query_vectors)
    key_rows = divide_among_subspaces(attention_key_vectors)
    value_rows = divide_among_subspaces(attention_content_vectors)
    learn_rate = jax.nn.sigmoid(divide_among_subspaces(step_size_preactivation))
    logarithmic_forgetting_amounts = divide_among_subspaces(-jnp.exp(-jax.nn.softplus(-forgetting_preactivation) - 0.5)) + extra_forgetting_bias[:, :, None]
    removal = key_rows / jnp.sqrt(lax.optimization_barrier(jnp.sum(key_rows * key_rows, axis=-1, keepdims=True)) + 1e-06)
    head_dim = key_rows.shape[-1]

    def advance(state_now, inputs):
        query_t, decay_t, key_t, value_t, removal_t, rate_t = inputs
        along_removal = jnp.einsum('hvk,hk->hv', state_now, removal_t, precision=HIGH)
        state_now = state_now * jnp.exp(decay_t)[:, None, :] - along_removal[:, :, None] * (removal_t * rate_t)[:, None, :] + value_t[:, :, None] * key_t[:, None, :]
        return (state_now, jnp.einsum('hvk,hk->hv', state_now, query_t, precision=HIGH))
    initial = jnp.zeros((attention_subspace_count, head_dim, head_dim), jnp.float32)
    _, readout = lax.scan(advance, initial, (query_rows, logarithmic_forgetting_amounts, key_rows, value_rows, removal, learn_rate))
    centered = readout - lax.optimization_barrier(jnp.mean(readout, axis=-1, keepdims=True))
    spread = lax.optimization_barrier(jnp.mean(centered * centered, axis=-1, keepdims=True))
    gains = subspace_normalizer_gain.reshape(attention_subspace_count, head_dim)[None]
    normed = centered * lax.rsqrt(spread + 0.00064) * gains
    return normed.reshape(token_count, attention_subspace_count * head_dim).astype(jnp.bfloat16)

def reference(readout_query_vectors, attention_key_vectors, attention_content_vectors, step_size_preactivation, forgetting_preactivation, extra_forgetting_bias, subspace_normalizer_gain, skip_connection_stream, blender_projection_matrix, specialist_prenormal_gain, cluster_router_chance, specialist_chance_within_cluster, chosen_specialist_ids, specialist_switch_matrix, specialist_expansion_matrix, specialist_contraction_matrix):
    blender_result = sequence_state_blender(readout_query_vectors, attention_key_vectors, attention_content_vectors, step_size_preactivation, forgetting_preactivation, extra_forgetting_bias, subspace_normalizer_gain)
    token_count = blender_result.shape[0]
    group_rows = D // N_TP

    def add_group(running, group):
        first_row = (group * group_rows).astype(jnp.int32)
        columns = lax.dynamic_slice_in_dim(blender_result, first_row, group_rows, 1)
        weight_rows = lax.dynamic_slice_in_dim(blender_projection_matrix, first_row, group_rows, 0)
        term = jnp.dot(columns, weight_rows, preferred_element_type=jnp.float32)
        rounded = lax.optimization_barrier(term.astype(jnp.bfloat16)).astype(jnp.float32)
        return (running + rounded, None)
    branch, _ = lax.scan(add_group, jnp.zeros((token_count, D), jnp.float32), jnp.arange(N_TP, dtype=jnp.int32))
    hidden_state = skip_connection_stream.astype(jnp.float32) + branch
    inverse_rms = lax.rsqrt(lax.optimization_barrier(jnp.mean(hidden_state * hidden_state, axis=1, keepdims=True)) + 1e-06)
    normed = (hidden_state * inverse_rms * specialist_prenormal_gain).astype(jnp.bfloat16)
    flat_expert = chosen_specialist_ids.reshape(N_SP, TOK_DEV * TOP)
    one_hot = (flat_expert[:, :, None] == jnp.arange(EXPERTS, dtype=jnp.int32)[None, None, :]).astype(jnp.int32)
    earlier = lax.optimization_barrier(jnp.sum((jnp.cumsum(one_hot, axis=1) - one_hot) * one_hot, axis=2))
    source = jnp.arange(N_SP, dtype=jnp.int32)[:, None]
    slot_index = (flat_expert * (N_SP * CAP) + source * CAP + earlier).reshape(-1)
    token_of = jnp.arange(N_SP * TOK_DEV * TOP, dtype=jnp.int32) // TOP
    slot_owner = jnp.full((EXPERTS * N_SP * CAP,), N_SP * TOK_DEV, jnp.int32).at[slot_index].set(token_of)
    padded = jnp.concatenate([normed, jnp.zeros((1, D), jnp.bfloat16)], axis=0)

    def expert_rows(operands):
        owners, w_gate, w_up, w_down = operands
        rows_in = padded[owners]
        gate_act = jnp.dot(rows_in, w_gate, preferred_element_type=jnp.float32)
        upward = jnp.dot(rows_in, w_up, preferred_element_type=jnp.float32)
        hidden = (jax.nn.silu(gate_act) * upward).astype(jnp.bfloat16)
        unit_group = w_down.shape[0] // N_TP
        hidden_split = hidden.astype(jnp.float32).reshape(-1, N_TP, unit_group)
        down_split = w_down.astype(jnp.float32).reshape(N_TP, unit_group, D)
        partial_value = jnp.einsum('rtf,tfd->trd', hidden_split, down_split)
        rounded = lax.optimization_barrier(partial_value.astype(jnp.bfloat16)).astype(jnp.float32)
        return lax.optimization_barrier(jnp.sum(rounded, axis=0))
    results = lax.map(expert_rows, (slot_owner.reshape(EXPERTS, N_SP * CAP), specialist_switch_matrix, specialist_expansion_matrix, specialist_contraction_matrix))
    picked = results.reshape(-1, D)[slot_index].reshape(N_SP * TOK_DEV, TOP, D)
    route_weight = cluster_router_chance[:, None] * specialist_chance_within_cluster / lax.optimization_barrier(jnp.sum(specialist_chance_within_cluster, axis=1, keepdims=True))
    mixture = lax.optimization_barrier(jnp.sum(route_weight[:, :, None] * picked, axis=1))
    return (hidden_state + mixture).astype(jnp.bfloat16)
```

```python
import jax
import jax.numpy as jnp
from jax import lax
from jax.experimental import pallas as pl
from jax.experimental.pallas import tpu as pltpu
from jax.sharding import Mesh
from jax.sharding import PartitionSpec as P


SP = ("z", "x")
TP = ("y", "c")
F32 = jnp.float32
BF16 = jnp.bfloat16
SEG = 64
W = 128
DECAY = 0.6065306597126334
INTERPRET = False


def mm(a, b, contract=((1,), (0,)), precision=lax.Precision.HIGHEST):
    return lax.dot_general(
        a, b, (contract, ((), ())), precision=precision, preferred_element_type=F32
    )


def iota(shape, dim):
    return lax.broadcasted_iota(jnp.int32, shape, dim)


def stack_heads(rows):
    first = iota(rows.shape, 1) < SEG
    zero = jnp.zeros_like(rows)
    return jnp.concatenate([jnp.where(first, rows, zero), jnp.where(first, zero, rows)], axis=0)


def flat_heads(stacked):
    half = stacked.shape[0] // 2
    return stacked[:half] + stacked[half:]


def eye128():
    return (iota((W, W), 0) == iota((W, W), 1)).astype(F32)


def same_head_ones():
    return (iota((W, W), 0) // SEG == iota((W, W), 1) // SEG).astype(F32)


def mixer_kernel(q_ref, k_ref, v_ref, s_ref, f_ref, b_ref, pair_ref, map_ref, loc_ref):
    rows = q_ref.shape[0]
    chunks = rows // SEG
    query = q_ref[...].astype(F32)
    key = k_ref[...].astype(F32)
    value = v_ref[...].astype(F32)
    rate = 1.0 / (1.0 + jnp.exp(-s_ref[...].astype(F32)))
    bias = jnp.where(iota((rows, W), 1) < SEG, b_ref[:, 0:1], b_ref[:, 1:2])
    decay = bias - DECAY / (1.0 + jnp.exp(-f_ref[...]))
    removal = key * lax.rsqrt(mm(key * key, same_head_ones()) + 1e-06)
    beta = removal * rate
    row, col = iota((rows, rows), 0), iota((rows, rows), 1)
    below = ((row // SEG == col // SEG) & (row >= col)).astype(F32)
    total = mm(below, decay)

    row, col = iota((W, W), 0), iota((W, W), 1)
    same = row // SEG == col // SEG
    strict = same & (row > col)
    inclusive = same & (row >= col)
    eye = eye128()

    part = []
    for n in range(chunks):
        at = slice(n * SEG, (n + 1) * SEG)
        cum = total[at]
        before = cum - decay[at]
        middle = cum[SEG // 2 - 1 : SEG // 2]
        closing = cum[SEG - 1 : SEG]
        up = jnp.exp(cum - middle)
        down = jnp.exp(middle - cum)
        left = jnp.exp(before - middle)
        opening = jnp.exp(middle)
        ending = jnp.exp(closing - middle)
        alpha = -removal[at] * left
        asked = query[at] * up
        beta_hat = beta[at] * down
        key_hat = key[at] * down
        scores = mm(
            jnp.concatenate([stack_heads(alpha), stack_heads(asked)], axis=0),
            jnp.concatenate([stack_heads(beta_hat), stack_heads(key_hat)], axis=0),
            ((1,), (1,)),
        )
        remove_remove = jnp.where(strict, scores[:W, :W], 0.0)
        remove_write = jnp.where(strict, scores[:W, W:], 0.0)
        read_remove = jnp.where(inclusive, scores[W:, :W], 0.0)
        read_write = jnp.where(inclusive, scores[W:, W:], 0.0)
        part.append(
            dict(
                near=remove_remove,
                write=remove_write,
                read=jnp.concatenate([read_remove, read_write], axis=1),
                read_remove=read_remove,
                alpha=stack_heads(alpha * opening),
                asked=stack_heads(asked * opening),
                value=stack_heads(value[at]),
                bar=jnp.concatenate(
                    [stack_heads(beta_hat * ending), stack_heads(key_hat * ending)], axis=0
                ),
                closing=jnp.exp(closing),
            )
        )
    inverse = [eye + jnp.where(row // 2 == col // 2, p["near"], 0.0) for p in part]
    for level in (4, 8, 16, 32, 64):
        joint = (row // level == col // level) & (row // (level // 2) != col // (level // 2))
        step = [mm(jnp.where(joint, p["near"], 0.0), x) for p, x in zip(part, inverse)]
        inverse = [x + mm(x, s) for x, s in zip(inverse, step)]
    wrote = [mm(p["write"], p["value"]) for p in part]
    solved = [
        mm(x, jnp.concatenate([p["alpha"], w], axis=1)) for x, p, w in zip(inverse, part, wrote)
    ]
    keeps, adds, reads, locals_ = [], [], [], []
    for p, s in zip(part, solved):
        absorb, carried = s[:, :W], s[:, W:]
        keeps.append(mm(absorb, p["bar"][:W], ((0,), (0,))) + eye * p["closing"])
        adds.append(
            mm(jnp.concatenate([carried, p["value"]], axis=0), p["bar"], ((0,), (0,)))
        )
        locals_.append(
            flat_heads(mm(p["read"], jnp.concatenate([carried, p["value"]], axis=0)))
        )
        reads.append(flat_heads(p["asked"] + mm(p["read_remove"], absorb)))
    map_ref[:SEG, :] = reads[0]
    loc_ref[:SEG, :] = locals_[0]
    run = jnp.concatenate([keeps[0], adds[0]], axis=0)
    for n in range(1, chunks):
        at = slice(n * SEG, (n + 1) * SEG)
        both = mm(reads[n], run, ((1,), (1,)))
        map_ref[at, :] = both[:, :W]
        loc_ref[at, :] = locals_[n] + both[:, W:]
        run = mm(run, keeps[n])
        run = jnp.concatenate([run[:W], run[W:] + adds[n]], axis=0)
    pair = jnp.concatenate([flat_heads(run[:W] - eye), flat_heads(run[W:])], axis=0).astype(BF16)
    for n in range(pair_ref.shape[0]):
        pair_ref[n] = pair


def unpack(pair):
    pair = pair.astype(F32)
    return stack_heads(pair[:SEG]), stack_heads(pair[SEG:])


def compose_kernel(pos_ref, got_ref, pair_ref, prefix_ref):
    mine = pos_ref[0]
    eye = eye128()
    change, add = unpack(got_ref[0])
    run = jnp.concatenate([eye + change, add], axis=0)
    prefix = jnp.where(mine > 0, run, jnp.concatenate([eye, jnp.zeros((W, W), F32)], axis=0))
    for n in range(1, got_ref.shape[0]):
        change, add = unpack(got_ref[n])
        run = run + mm(run, change)
        run = jnp.concatenate([run[:W], run[W:] + add], axis=0)
        prefix = jnp.where(n < mine, run, prefix)
    pair = jnp.concatenate([flat_heads(run[:W] - eye), flat_heads(run[W:])], axis=0).astype(BF16)
    for n in range(pair_ref.shape[0]):
        pair_ref[n] = pair
    prefix_ref[...] = prefix


def readout_kernel(pos_ref, got_ref, prefix_ref, map_ref, loc_ref, gain_ref, w_ref, keep_ref, send_ref):
    mine, core = pos_ref[1], pos_ref[3]
    state = jnp.where(mine > 0, unpack(got_ref[0])[1], 0.0)
    for n in range(1, got_ref.shape[0] - 1):
        change, add = unpack(got_ref[n])
        state = jnp.where(n < mine, state + mm(state, change) + add, state)
    state = mm(state, prefix_ref[:W]) + prefix_ref[W:]
    out = loc_ref[...] + mm(map_ref[...], state, ((1,), (1,)))
    ones = same_head_ones()
    centered = out - mm(out, ones) * (1.0 / SEG)
    spread = mm(centered * centered, ones) * (1.0 / SEG)
    mixed = (centered * lax.rsqrt(spread + 0.00064) * gain_ref[...]).astype(BF16)
    for n in range(keep_ref.shape[0]):
        part = jnp.dot(mixed, w_ref[:, n * 2 * W : (n + 1) * 2 * W], preferred_element_type=F32)
        first, second = part[:, :W], part[:, W:]
        keep_ref[n] = jnp.where(core == 0, first, second)
        send_ref[n] = jnp.where(core == 0, second, first).astype(BF16)


def slots_of(ids_ref, experts, capacity):
    tokens = ids_ref.shape[0]
    names = [ids_ref[:, k : k + 1] for k in range(2)]
    hot = [(iota((tokens, experts), 1) == name).astype(F32) for name in names]
    earlier = (iota((tokens, tokens), 0) > iota((tokens, tokens), 1)).astype(BF16)
    ahead = jnp.dot(earlier, (hot[0] + hot[1]).astype(BF16), preferred_element_type=F32)
    ranks = [
        jnp.sum(hot[0] * ahead, axis=1, keepdims=True),
        jnp.sum(hot[1] * (ahead + hot[0]), axis=1, keepdims=True),
    ]
    return [name * capacity + rank.astype(jnp.int32) for name, rank in zip(names, ranks)]


def dispatch_kernel(parts_ref, skip_ref, gain_ref, ids_ref, hid_ref, out_ref):
    hidden = skip_ref[...].astype(F32)
    for n in range(parts_ref.shape[0]):
        hidden = hidden + parts_ref[n].astype(F32)
    hid_ref[...] = hidden
    scaled = (hidden * gain_ref[...]).astype(BF16)
    tokens, places = ids_ref.shape[0], out_ref.shape[0]
    first, second = slots_of(ids_ref, 32, 32)
    lane = iota((tokens, places), 1)
    hot = ((lane == first) | (lane == second)).astype(F32).astype(BF16)
    out_ref[...] = lax.dot_general(
        hot, scaled, (((0,), (0,)), ((), ())), preferred_element_type=F32
    ).astype(BF16)


def expert_kernel(pos_ref, own_ref, other_ref, inv_gain_ref, w0, w1, w2, w3, keep_ref, send_ref):
    core = pos_ref[3]
    ways, rows = own_ref.shape[0], own_ref.shape[1]
    blocks = []
    for n in range(ways):
        own, other = own_ref[n], other_ref[n]
        blocks.append(jnp.where(core == 0, own, other))
        blocks.append(jnp.where(core == 0, other, own))
    data = jnp.concatenate(blocks, axis=1)
    width = data.shape[1]
    squares = jnp.zeros((rows, W), F32)
    for n, block in enumerate(blocks):
        plain = block.astype(F32) * inv_gain_ref[:, n * W : (n + 1) * W]
        squares = squares + plain * plain
    scale = lax.rsqrt(jnp.sum(squares, axis=1, keepdims=True) * (1.0 / width) + 1e-06)
    hidden = []
    for w_ref in (w0, w1, w2, w3):
        both = jnp.concatenate([w_ref[:width], w_ref[width : 2 * width]], axis=1)
        act = jnp.dot(data, both, preferred_element_type=F32) * scale
        gate, up = act[:, :W], act[:, W:]
        hidden.append((gate / (1.0 + jnp.exp(-gate)) * up).astype(BF16))
    hidden = jnp.concatenate(hidden, axis=1)
    for n in range(ways):
        at = 2 * width + 2 * n * W
        pieces = [
            jnp.concatenate([w_ref[at : at + W], w_ref[at + W : at + 2 * W]], axis=1)
            for w_ref in (w0, w1, w2, w3)
        ]
        part = jnp.dot(hidden, jnp.concatenate(pieces, axis=0), preferred_element_type=F32)
        first, second = part[:, :W], part[:, W:]
        keep_ref[n] = jnp.where(core == 0, first, second)
        send_ref[n] = jnp.where(core == 0, second, first).astype(BF16)


def combine_kernel(ret_ref, hid_ref, ids_ref, chance_ref, within_ref, out_ref):
    tokens, places = ids_ref.shape[0], ret_ref.shape[0]
    slots = slots_of(ids_ref, 32, 32)
    lane = iota((tokens, places), 1)
    within = within_ref[...]
    whole = within[:, 0:1] + within[:, 1:2]
    result = hid_ref[...]
    for k in range(2):
        hot = (lane == slots[k]).astype(F32).astype(BF16)
        picked = jnp.dot(hot, ret_ref[...], preferred_element_type=F32)
        result = result + picked * (chance_ref[...] * within[:, k : k + 1] / whole)
    result = result.astype(BF16)
    for n in range(out_ref.shape[0]):
        out_ref[n] = result


def assemble_kernel(pos_ref, own_ref, other_ref, out_ref):
    core = pos_ref[3]
    for n in range(own_ref.shape[0]):
        own, other = own_ref[n], other_ref[n]
        out_ref[:, 2 * n * W : (2 * n + 1) * W] = jnp.where(core == 0, own, other)
        out_ref[:, (2 * n + 1) * W : (2 * n + 2) * W] = jnp.where(core == 0, other, own)


def call(kernel, name, outs, *args, scalars=0, flops=1_000_000):
    specs = [
        pl.BlockSpec(memory_space=pltpu.SMEM if n < scalars else pltpu.VMEM)
        for n in range(len(args))
    ]
    shapes = [jax.ShapeDtypeStruct(shape, kind) for shape, kind in outs]
    result = pl.pallas_call(
        kernel,
        name=name,
        out_shape=shapes if len(shapes) > 1 else shapes[0],
        in_specs=specs,
        out_specs=[pl.BlockSpec(memory_space=pltpu.VMEM)] * len(shapes)
        if len(shapes) > 1
        else pl.BlockSpec(memory_space=pltpu.VMEM),
        compiler_params=pltpu.CompilerParams(vmem_limit_bytes=40 * 1024 * 1024),
        cost_estimate=pl.CostEstimate(flops=flops, bytes_accessed=1_000_000, transcendentals=0),
        interpret=INTERPRET,
    )(*args)
    return result


def exchange(parts, axes):
    return lax.all_to_all(parts, axes, split_axis=0, concat_axis=0, tiled=True)


def swap_cores(data):
    return lax.ppermute(data, "c", [(0, 1), (1, 0)])


def body(
    queries,
    keys,
    values,
    step_sizes,
    forgetting,
    forgetting_bias,
    head_gain,
    skip,
    blender,
    norm_gain,
    cluster_chance,
    within_chance,
    ids,
    switch,
    expansion,
    contraction,
):
    n_z, n_x, n_y = (lax.axis_size(a) for a in ("z", "x", "y"))
    here = [lax.axis_index(a) for a in ("x", "z", "y", "c")]
    pos = jnp.stack(here).astype(jnp.int32)
    tokens, width = skip.shape
    column = (here[2] * 2 + here[3]) * W

    ring = [(((y + 1) % n_y) * 2, y * 2) for y in range(n_y)]
    ring += [(((y - 1) % n_y) * 2 + 1, y * 2 + 1) for y in range(n_y)]
    down = contraction[0].reshape(W, width // W, W).transpose(1, 0, 2).reshape(width, W)
    weights = [jnp.concatenate([switch[0], expansion[0], down], axis=0)]
    for _ in range(3):
        weights.append(lax.ppermute(weights[-1], TP, ring))

    pairs, state_map, local = call(
        mixer_kernel,
        "mixer",
        [((n_x, W, W), BF16), ((tokens, W), F32), ((tokens, W), F32)],
        queries,
        keys,
        values,
        step_sizes,
        forgetting,
        forgetting_bias,
    )
    pairs, prefix = call(
        compose_kernel,
        "compose",
        [((n_z, W, W), BF16), ((2 * W, W), F32)],
        pos,
        exchange(pairs, "x"),
        scalars=1,
    )
    keep, send = call(
        readout_kernel,
        "readout",
        [((n_y, tokens, W), F32), ((n_y, tokens, W), BF16)],
        pos,
        exchange(pairs, "z"),
        prefix,
        state_map,
        local,
        head_gain[None],
        blender,
        scalars=1,
    )
    parts = exchange((keep + swap_cores(send).astype(F32)).astype(BF16), "y")
    hidden, outgoing = call(
        dispatch_kernel,
        "dispatch",
        [((tokens, W), F32), ((4 * tokens, W), BF16)],
        parts,
        lax.dynamic_slice_in_dim(skip, column, W, 1),
        lax.dynamic_slice_in_dim(norm_gain, column, W, 0)[None],
        ids,
    )
    arrived = exchange(outgoing.reshape(n_z * n_x, -1, W), SP).reshape(4, tokens, W)
    own = exchange(jnp.concatenate([arrived, arrived], axis=0), "y")
    keep, send = call(
        expert_kernel,
        "expert",
        [((n_y, tokens, W), F32), ((n_y, tokens, W), BF16)],
        pos,
        own,
        swap_cores(own),
        (1.0 / norm_gain)[None],
        *weights,
        scalars=1,
    )
    summed = exchange((keep + swap_cores(send).astype(F32)).astype(BF16), "y")
    summed = (summed[:4].astype(F32) + summed[4:].astype(F32)).astype(BF16)
    returned = exchange(summed.reshape(n_z * n_x, -1, W), SP).reshape(4 * tokens, W)
    copies = call(
        combine_kernel,
        "combine",
        [((n_y, tokens, W), BF16)],
        returned,
        hidden,
        ids,
        cluster_chance[:, None],
        within_chance,
    )
    own = exchange(copies, "y")
    return call(
        assemble_kernel, "assemble", [((tokens, width), BF16)], pos, own, swap_cores(own), scalars=1
    )


def solution(mesh):
    split = Mesh(mesh.devices.reshape(8, 4, 8, 2), ("z", "x", "y", "c"))
    in_specs = (
        P(SP, TP),
        P(SP, TP),
        P(SP, TP),
        P(SP, TP),
        P(SP, TP),
        P(SP, TP),
        P(TP),
        P(SP, None),
        P(TP, None),
        P(),
        P(SP),
        P(SP, None),
        P(SP, None),
        P(SP, None, TP),
        P(SP, None, TP),
        P(SP, TP, None),
    )
    out_specs = P(SP, None)
    return jax.shard_map(body, mesh=split, in_specs=in_specs, out_specs=out_specs, check_vma=False)
```

```python
import jax
import jax.numpy as jnp
from jax import lax
from jax.experimental import pallas as pl
from jax.experimental.pallas import tpu as pltpu
from jax.sharding import Mesh
from jax.sharding import PartitionSpec as P


SP = ("z", "x")
TP = ("y", "c")
F32 = jnp.float32
BF16 = jnp.bfloat16
SEG = 64
W = 128
DECAY = 0.6065306597126334
INTERPRET = False


def mm(a, b, contract=((1,), (0,)), precision=lax.Precision.HIGHEST):
    return lax.dot_general(
        a, b, (contract, ((), ())), precision=precision, preferred_element_type=F32
    )


def iota(shape, dim):
    return lax.broadcasted_iota(jnp.int32, shape, dim)


def stack_heads(rows):
    first = iota(rows.shape, 1) < SEG
    zero = jnp.zeros_like(rows)
    return jnp.concatenate([jnp.where(first, rows, zero), jnp.where(first, zero, rows)], axis=0)


def flat_heads(stacked):
    half = stacked.shape[0] // 2
    return stacked[:half] + stacked[half:]


def eye128():
    return (iota((W, W), 0) == iota((W, W), 1)).astype(F32)


def same_head_ones():
    return (iota((W, W), 0) // SEG == iota((W, W), 1) // SEG).astype(F32)


def mixer_kernel(q_ref, k_ref, v_ref, s_ref, f_ref, b_ref, pair_ref, map_ref, loc_ref):
    rows = q_ref.shape[0]
    chunks = rows // SEG
    query = q_ref[...].astype(F32)
    key = k_ref[...].astype(F32)
    value = v_ref[...].astype(F32)
    rate = 1.0 / (1.0 + jnp.exp(-s_ref[...].astype(F32)))
    bias = jnp.where(iota((rows, W), 1) < SEG, b_ref[:, 0:1], b_ref[:, 1:2])
    decay = bias - DECAY / (1.0 + jnp.exp(-f_ref[...]))
    removal = key * lax.rsqrt(mm(key * key, same_head_ones()) + 1e-06)
    beta = removal * rate
    row, col = iota((rows, rows), 0), iota((rows, rows), 1)
    below = ((row // SEG == col // SEG) & (row >= col)).astype(F32)
    total = mm(below, decay)

    row, col = iota((W, W), 0), iota((W, W), 1)
    same = row // SEG == col // SEG
    strict = same & (row > col)
    inclusive = same & (row >= col)
    eye = eye128()

    part = []
    for n in range(chunks):
        at = slice(n * SEG, (n + 1) * SEG)
        cum = total[at]
        before = cum - decay[at]
        middle = cum[SEG // 2 - 1 : SEG // 2]
        closing = cum[SEG - 1 : SEG]
        up = jnp.exp(cum - middle)
        down = jnp.exp(middle - cum)
        left = jnp.exp(before - middle)
        opening = jnp.exp(middle)
        ending = jnp.exp(closing - middle)
        alpha = -removal[at] * left
        asked = query[at] * up
        beta_hat = beta[at] * down
        key_hat = key[at] * down
        scores = mm(
            jnp.concatenate([stack_heads(alpha), stack_heads(asked)], axis=0),
            jnp.concatenate([stack_heads(beta_hat), stack_heads(key_hat)], axis=0),
            ((1,), (1,)),
        )
        remove_remove = jnp.where(strict, scores[:W, :W], 0.0)
        remove_write = jnp.where(strict, scores[:W, W:], 0.0)
        read_remove = jnp.where(inclusive, scores[W:, :W], 0.0)
        read_write = jnp.where(inclusive, scores[W:, W:], 0.0)
        part.append(
            dict(
                near=remove_remove,
                write=remove_write,
                read=jnp.concatenate([read_remove, read_write], axis=1),
                read_remove=read_remove,
                alpha=stack_heads(alpha * opening),
                asked=stack_heads(asked * opening),
                value=stack_heads(value[at]),
                bar=jnp.concatenate(
                    [stack_heads(beta_hat * ending), stack_heads(key_hat * ending)], axis=0
                ),
                closing=jnp.exp(closing),
            )
        )
    inverse = [eye + jnp.where(row // 2 == col // 2, p["near"], 0.0) for p in part]
    for level in (4, 8, 16, 32, 64):
        joint = (row // level == col // level) & (row // (level // 2) != col // (level // 2))
        step = [mm(jnp.where(joint, p["near"], 0.0), x) for p, x in zip(part, inverse)]
        inverse = [x + mm(x, s) for x, s in zip(inverse, step)]
    wrote = [mm(p["write"], p["value"]) for p in part]
    solved = [
        mm(x, jnp.concatenate([p["alpha"], w], axis=1)) for x, p, w in zip(inverse, part, wrote)
    ]
    keeps, adds, reads, locals_ = [], [], [], []
    for p, s in zip(part, solved):
        absorb, carried = s[:, :W], s[:, W:]
        keeps.append(mm(absorb, p["bar"][:W], ((0,), (0,))) + eye * p["closing"])
        adds.append(
            mm(jnp.concatenate([carried, p["value"]], axis=0), p["bar"], ((0,), (0,)))
        )
        locals_.append(
            flat_heads(mm(p["read"], jnp.concatenate([carried, p["value"]], axis=0)))
        )
        reads.append(flat_heads(p["asked"] + mm(p["read_remove"], absorb)))
    map_ref[:SEG, :] = reads[0]
    loc_ref[:SEG, :] = locals_[0]
    run = jnp.concatenate([keeps[0], adds[0]], axis=0)
    for n in range(1, chunks):
        at = slice(n * SEG, (n + 1) * SEG)
        both = mm(reads[n], run, ((1,), (1,)))
        map_ref[at, :] = both[:, :W]
        loc_ref[at, :] = locals_[n] + both[:, W:]
        run = mm(run, keeps[n])
        run = jnp.concatenate([run[:W], run[W:] + adds[n]], axis=0)
    pair = jnp.concatenate([flat_heads(run[:W] - eye), flat_heads(run[W:])], axis=0).astype(BF16)
    for n in range(pair_ref.shape[0]):
        pair_ref[n] = pair


def unpack(pair):
    pair = pair.astype(F32)
    return stack_heads(pair[:SEG]), stack_heads(pair[SEG:])


def compose_kernel(pos_ref, got_ref, pair_ref, prefix_ref):
    mine = pos_ref[0]
    eye = eye128()
    change, add = unpack(got_ref[0])
    run = jnp.concatenate([eye + change, add], axis=0)
    prefix = jnp.where(mine > 0, run, jnp.concatenate([eye, jnp.zeros((W, W), F32)], axis=0))
    for n in range(1, got_ref.shape[0]):
        change, add = unpack(got_ref[n])
        run = run + mm(run, change)
        run = jnp.concatenate([run[:W], run[W:] + add], axis=0)
        prefix = jnp.where(n < mine, run, prefix)
    pair = jnp.concatenate([flat_heads(run[:W] - eye), flat_heads(run[W:])], axis=0).astype(BF16)
    for n in range(pair_ref.shape[0]):
        pair_ref[n] = pair
    prefix_ref[...] = prefix


def readout_kernel(pos_ref, got_ref, prefix_ref, map_ref, loc_ref, gain_ref, w_ref, keep_ref, send_ref):
    mine, core = pos_ref[1], pos_ref[3]
    state = jnp.where(mine > 0, unpack(got_ref[0])[1], 0.0)
    for n in range(1, got_ref.shape[0] - 1):
        change, add = unpack(got_ref[n])
        state = jnp.where(n < mine, state + mm(state, change) + add, state)
    state = mm(state, prefix_ref[:W]) + prefix_ref[W:]
    out = loc_ref[...] + mm(map_ref[...], state, ((1,), (1,)))
    ones = same_head_ones()
    centered = out - mm(out, ones) * (1.0 / SEG)
    spread = mm(centered * centered, ones) * (1.0 / SEG)
    mixed = (centered * lax.rsqrt(spread + 0.00064) * gain_ref[...]).astype(BF16)
    for n in range(keep_ref.shape[0]):
        part = jnp.dot(mixed, w_ref[:, n * 2 * W : (n + 1) * 2 * W], preferred_element_type=F32)
        first, second = part[:, :W], part[:, W:]
        keep_ref[n] = jnp.where(core == 0, first, second)
        send_ref[n] = jnp.where(core == 0, second, first).astype(BF16)


def slots_of(ids_ref, experts, capacity):
    tokens = ids_ref.shape[0]
    names = [ids_ref[:, k : k + 1] for k in range(2)]
    hot = [(iota((tokens, experts), 1) == name).astype(F32) for name in names]
    earlier = (iota((tokens, tokens), 0) > iota((tokens, tokens), 1)).astype(BF16)
    ahead = jnp.dot(earlier, (hot[0] + hot[1]).astype(BF16), preferred_element_type=F32)
    ranks = [
        jnp.sum(hot[0] * ahead, axis=1, keepdims=True),
        jnp.sum(hot[1] * (ahead + hot[0]), axis=1, keepdims=True),
    ]
    return [name * capacity + rank.astype(jnp.int32) for name, rank in zip(names, ranks)]


def dispatch_kernel(parts_ref, skip_ref, gain_ref, ids_ref, hid_ref, out_ref):
    hidden = skip_ref[...].astype(F32)
    for n in range(parts_ref.shape[0]):
        hidden = hidden + parts_ref[n].astype(F32)
    hid_ref[...] = hidden
    scaled = (hidden * gain_ref[...]).astype(BF16)
    tokens, places = ids_ref.shape[0], out_ref.shape[0]
    first, second = slots_of(ids_ref, 32, 32)
    lane = iota((tokens, places), 1)
    hot = ((lane == first) | (lane == second)).astype(F32).astype(BF16)
    out_ref[...] = lax.dot_general(
        hot, scaled, (((0,), (0,)), ((), ())), preferred_element_type=F32
    ).astype(BF16)


def expert_kernel(pos_ref, own_ref, other_ref, inv_gain_ref, w0, w1, w2, w3, keep_ref, send_ref):
    core = pos_ref[3]
    ways, rows = own_ref.shape[0], own_ref.shape[1]
    blocks = []
    for n in range(ways):
        own, other = own_ref[n], other_ref[n]
        blocks.append(jnp.where(core == 0, own, other))
        blocks.append(jnp.where(core == 0, other, own))
    data = jnp.concatenate(blocks, axis=1)
    width = data.shape[1]
    squares = jnp.zeros((rows, W), F32)
    for n, block in enumerate(blocks):
        plain = block.astype(F32) * inv_gain_ref[:, n * W : (n + 1) * W]
        squares = squares + plain * plain
    scale = lax.rsqrt(jnp.sum(squares, axis=1, keepdims=True) * (1.0 / width) + 1e-06)
    hidden = []
    for w_ref in (w0, w1, w2, w3):
        both = jnp.concatenate([w_ref[:width], w_ref[width : 2 * width]], axis=1)
        act = jnp.dot(data, both, preferred_element_type=F32) * scale
        gate, up = act[:, :W], act[:, W:]
        hidden.append((gate / (1.0 + jnp.exp(-gate)) * up).astype(BF16))
    hidden = jnp.concatenate(hidden, axis=1)
    for n in range(ways):
        at = 2 * width + 2 * n * W
        pieces = [
            jnp.concatenate([w_ref[at : at + W], w_ref[at + W : at + 2 * W]], axis=1)
            for w_ref in (w0, w1, w2, w3)
        ]
        part = jnp.dot(hidden, jnp.concatenate(pieces, axis=0), preferred_element_type=F32)
        first, second = part[:, :W], part[:, W:]
        keep_ref[n] = jnp.where(core == 0, first, second)
        send_ref[n] = jnp.where(core == 0, second, first).astype(BF16)


def combine_kernel(ret_ref, hid_ref, ids_ref, chance_ref, within_ref, out_ref):
    tokens, places = ids_ref.shape[0], ret_ref.shape[0]
    slots = slots_of(ids_ref, 32, 32)
    lane = iota((tokens, places), 1)
    within = within_ref[...]
    whole = within[:, 0:1] + within[:, 1:2]
    result = hid_ref[...]
    for k in range(2):
        hot = (lane == slots[k]).astype(F32).astype(BF16)
        picked = jnp.dot(hot, ret_ref[...], preferred_element_type=F32)
        result = result + picked * (chance_ref[...] * within[:, k : k + 1] / whole)
    result = result.astype(BF16)
    for n in range(out_ref.shape[0]):
        out_ref[n] = result


def assemble_kernel(pos_ref, own_ref, other_ref, out_ref):
    core = pos_ref[3]
    for n in range(own_ref.shape[0]):
        own, other = own_ref[n], other_ref[n]
        out_ref[:, 2 * n * W : (2 * n + 1) * W] = jnp.where(core == 0, own, other)
        out_ref[:, (2 * n + 1) * W : (2 * n + 2) * W] = jnp.where(core == 0, other, own)


def call(kernel, outs, *args, scalars=0, flops=1_000_000):
    specs = [
        pl.BlockSpec(memory_space=pltpu.SMEM if n < scalars else pltpu.VMEM)
        for n in range(len(args))
    ]
    shapes = [jax.ShapeDtypeStruct(shape, kind) for shape, kind in outs]
    result = pl.pallas_call(
        kernel,
        out_shape=shapes if len(shapes) > 1 else shapes[0],
        in_specs=specs,
        out_specs=[pl.BlockSpec(memory_space=pltpu.VMEM)] * len(shapes)
        if len(shapes) > 1
        else pl.BlockSpec(memory_space=pltpu.VMEM),
        compiler_params=pltpu.CompilerParams(vmem_limit_bytes=40 * 1024 * 1024),
        cost_estimate=pl.CostEstimate(flops=flops, bytes_accessed=1_000_000, transcendentals=0),
        interpret=INTERPRET,
    )(*args)
    return result


def exchange(parts, axes):
    return lax.all_to_all(parts, axes, split_axis=0, concat_axis=0, tiled=True)


def swap_cores(data):
    return lax.ppermute(data, "c", [(0, 1), (1, 0)])


def body(
    queries,
    keys,
    values,
    step_sizes,
    forgetting,
    forgetting_bias,
    head_gain,
    skip,
    blender,
    norm_gain,
    cluster_chance,
    within_chance,
    ids,
    switch,
    expansion,
    contraction,
):
    n_z, n_x, n_y = (lax.axis_size(a) for a in ("z", "x", "y"))
    here = [lax.axis_index(a) for a in ("x", "z", "y", "c")]
    pos = jnp.stack(here).astype(jnp.int32)
    tokens, width = skip.shape
    column = (here[2] * 2 + here[3]) * W

    ring = [(((y + 1) % n_y) * 2, y * 2) for y in range(n_y)]
    ring += [(((y - 1) % n_y) * 2 + 1, y * 2 + 1) for y in range(n_y)]
    pairs, state_map, local = call(
        mixer_kernel,
        [((n_x, W, W), BF16), ((tokens, W), F32), ((tokens, W), F32)],
        queries,
        keys,
        values,
        step_sizes,
        forgetting,
        forgetting_bias,
    )
    pairs, switch, expansion, contraction = lax.optimization_barrier(
        (pairs, switch, expansion, contraction)
    )
    down = contraction[0].reshape(W, width // W, W).transpose(1, 0, 2).reshape(width, W)
    weights = [jnp.concatenate([switch[0], expansion[0], down], axis=0)]
    weights.append(lax.ppermute(weights[-1], TP, ring))
    gathered = exchange(pairs, "x")
    pairs, prefix = call(
        compose_kernel, [((n_z, W, W), BF16), ((2 * W, W), F32)], pos, gathered, scalars=1
    )
    weights.append(lax.ppermute(weights[-1], TP, ring))
    gathered = exchange(pairs, "z")
    keep, send = call(
        readout_kernel,
        [((n_y, tokens, W), F32), ((n_y, tokens, W), BF16)],
        pos,
        gathered,
        prefix,
        state_map,
        local,
        head_gain[None],
        blender,
        scalars=1,
    )
    parts = exchange((keep + swap_cores(send).astype(F32)).astype(BF16), "y")
    parts, weights[2] = lax.optimization_barrier((parts, weights[2]))
    weights.append(lax.ppermute(weights[-1], TP, ring))
    hidden, outgoing = call(
        dispatch_kernel,
        [((tokens, W), F32), ((4 * tokens, W), BF16)],
        parts,
        lax.dynamic_slice_in_dim(skip, column, W, 1),
        lax.dynamic_slice_in_dim(norm_gain, column, W, 0)[None],
        ids,
    )
    arrived = exchange(outgoing.reshape(n_z * n_x, -1, W), SP).reshape(4, tokens, W)
    own = exchange(jnp.concatenate([arrived, arrived], axis=0), "y")
    keep, send = call(
        expert_kernel,
        [((n_y, tokens, W), F32), ((n_y, tokens, W), BF16)],
        pos,
        own,
        swap_cores(own),
        (1.0 / norm_gain)[None],
        *weights,
        scalars=1,
    )
    summed = exchange((keep + swap_cores(send).astype(F32)).astype(BF16), "y")
    summed = (summed[:4].astype(F32) + summed[4:].astype(F32)).astype(BF16)
    returned = exchange(summed.reshape(n_z * n_x, -1, W), SP).reshape(4 * tokens, W)
    copies = call(
        combine_kernel,
        [((n_y, tokens, W), BF16)],
        returned,
        hidden,
        ids,
        cluster_chance[:, None],
        within_chance,
    )
    own = exchange(copies, "y")
    return call(assemble_kernel, [((tokens, width), BF16)], pos, own, swap_cores(own), scalars=1)


def solution(mesh):
    split = Mesh(mesh.devices.reshape(8, 4, 8, 2), ("z", "x", "y", "c"))
    in_specs = (
        P(SP, TP),
        P(SP, TP),
        P(SP, TP),
        P(SP, TP),
        P(SP, TP),
        P(SP, TP),
        P(TP),
        P(SP, None),
        P(TP, None),
        P(),
        P(SP),
        P(SP, None),
        P(SP, None),
        P(SP, None, TP),
        P(SP, None, TP),
        P(SP, TP, None),
    )
    out_specs = P(SP, None)

    return jax.shard_map(body, mesh=split, in_specs=in_specs, out_specs=out_specs, check_vma=False)
```

```python
import jax
import jax.numpy as jnp
from jax import lax
from jax.experimental import pallas as pl
from jax.experimental.pallas import tpu as pltpu
from jax.sharding import Mesh
from jax.sharding import PartitionSpec as P


SP = ("z", "x")
TP = ("y", "c")
F32 = jnp.float32
BF16 = jnp.bfloat16
SEG = 64
W = 128
DECAY = 0.6065306597126334
INTERPRET = False


def mm(a, b, contract=((1,), (0,)), precision=lax.Precision.HIGHEST):
    return lax.dot_general(
        a, b, (contract, ((), ())), precision=precision, preferred_element_type=F32
    )


def iota(shape, dim):
    return lax.broadcasted_iota(jnp.int32, shape, dim)


def stack_heads(rows):
    first = iota(rows.shape, 1) < SEG
    zero = jnp.zeros_like(rows)
    return jnp.concatenate([jnp.where(first, rows, zero), jnp.where(first, zero, rows)], axis=0)


def flat_heads(stacked):
    half = stacked.shape[0] // 2
    return stacked[:half] + stacked[half:]


def eye128():
    return (iota((W, W), 0) == iota((W, W), 1)).astype(F32)


def same_head_ones():
    return (iota((W, W), 0) // SEG == iota((W, W), 1) // SEG).astype(F32)


def pack_kernel(switch_ref, expansion_ref, contraction_ref, out_ref, sems):
    depth = switch_ref.shape[1]
    copies = [
        pltpu.make_async_copy(switch_ref.at[0], out_ref.at[pl.ds(0, depth)], sems.at[0]),
        pltpu.make_async_copy(expansion_ref.at[0], out_ref.at[pl.ds(depth, depth)], sems.at[1]),
    ]
    for n in range(depth // W):
        copies.append(
            pltpu.make_async_copy(
                contraction_ref.at[0, :, pl.ds(n * W, W)],
                out_ref.at[pl.ds(2 * depth + n * W, W)],
                sems.at[2 + n],
            )
        )
    for copy in copies:
        copy.start()
    for copy in copies:
        copy.wait()


def columns_of(rows):
    spare = jnp.zeros((6, rows.shape[1]), rows.dtype)
    return jnp.concatenate([rows, spare], axis=0).T


def mixer_kernel(*refs):
    pair_ref, map_ref, loc_ref = refs[6:9]
    held, sems = refs[9:15], refs[15]
    copies = [
        pltpu.make_async_copy(refs[n], held[n], sems.at[n]) for n in range(len(held))
    ]
    for copy in copies:
        copy.start()
    for copy in copies:
        copy.wait()
    q_ref, k_ref, v_ref, s_ref, f_ref, b_ref = held
    bias_columns = columns_of(b_ref[...])
    rows = q_ref.shape[0]
    chunks = rows // SEG
    query = q_ref[...].astype(F32)
    key = k_ref[...].astype(F32)
    value = v_ref[...].astype(F32)
    rate = 1.0 / (1.0 + jnp.exp(-s_ref[...].astype(F32)))
    bias = jnp.where(iota((rows, W), 1) < SEG, bias_columns[:, 0:1], bias_columns[:, 1:2])
    decay = bias - DECAY / (1.0 + jnp.exp(-f_ref[...]))
    removal = key * lax.rsqrt(mm(key * key, same_head_ones()) + 1e-06)
    beta = removal * rate
    row, col = iota((rows, rows), 0), iota((rows, rows), 1)
    below = ((row // SEG == col // SEG) & (row >= col)).astype(F32)
    total = mm(below, decay)

    row, col = iota((W, W), 0), iota((W, W), 1)
    same = row // SEG == col // SEG
    strict = same & (row > col)
    inclusive = same & (row >= col)
    eye = eye128()

    part = []
    for n in range(chunks):
        at = slice(n * SEG, (n + 1) * SEG)
        cum = total[at]
        before = cum - decay[at]
        middle = cum[SEG // 2 - 1 : SEG // 2]
        closing = cum[SEG - 1 : SEG]
        up = jnp.exp(cum - middle)
        down = jnp.exp(middle - cum)
        left = jnp.exp(before - middle)
        opening = jnp.exp(middle)
        ending = jnp.exp(closing - middle)
        alpha = -removal[at] * left
        asked = query[at] * up
        beta_hat = beta[at] * down
        key_hat = key[at] * down
        scores = mm(
            jnp.concatenate([stack_heads(alpha), stack_heads(asked)], axis=0),
            jnp.concatenate([stack_heads(beta_hat), stack_heads(key_hat)], axis=0),
            ((1,), (1,)),
        )
        remove_remove = jnp.where(strict, scores[:W, :W], 0.0)
        remove_write = jnp.where(strict, scores[:W, W:], 0.0)
        read_remove = jnp.where(inclusive, scores[W:, :W], 0.0)
        read_write = jnp.where(inclusive, scores[W:, W:], 0.0)
        part.append(
            dict(
                near=remove_remove,
                write=remove_write,
                read=jnp.concatenate([read_remove, read_write], axis=1),
                read_remove=read_remove,
                alpha=stack_heads(alpha * opening),
                asked=stack_heads(asked * opening),
                value=stack_heads(value[at]),
                bar=jnp.concatenate(
                    [stack_heads(beta_hat * ending), stack_heads(key_hat * ending)], axis=0
                ),
                closing=jnp.exp(closing),
            )
        )
    inverse = [eye + jnp.where(row // 2 == col // 2, p["near"], 0.0) for p in part]
    for level in (4, 8, 16, 32, 64):
        joint = (row // level == col // level) & (row // (level // 2) != col // (level // 2))
        step = [mm(jnp.where(joint, p["near"], 0.0), x) for p, x in zip(part, inverse)]
        inverse = [x + mm(x, s) for x, s in zip(inverse, step)]
    wrote = [mm(p["write"], p["value"]) for p in part]
    solved = [
        mm(x, jnp.concatenate([p["alpha"], w], axis=1)) for x, p, w in zip(inverse, part, wrote)
    ]
    keeps, adds, reads, locals_ = [], [], [], []
    for p, s in zip(part, solved):
        absorb, carried = s[:, :W], s[:, W:]
        keeps.append(mm(absorb, p["bar"][:W], ((0,), (0,))) + eye * p["closing"])
        adds.append(
            mm(jnp.concatenate([carried, p["value"]], axis=0), p["bar"], ((0,), (0,)))
        )
        locals_.append(
            flat_heads(mm(p["read"], jnp.concatenate([carried, p["value"]], axis=0)))
        )
        reads.append(flat_heads(p["asked"] + mm(p["read_remove"], absorb)))
    map_ref[:SEG, :] = reads[0]
    loc_ref[:SEG, :] = locals_[0]
    run = jnp.concatenate([keeps[0], adds[0]], axis=0)
    for n in range(1, chunks):
        at = slice(n * SEG, (n + 1) * SEG)
        both = mm(reads[n], run, ((1,), (1,)))
        map_ref[at, :] = both[:, :W]
        loc_ref[at, :] = locals_[n] + both[:, W:]
        run = mm(run, keeps[n])
        run = jnp.concatenate([run[:W], run[W:] + adds[n]], axis=0)
    pair = jnp.concatenate([flat_heads(run[:W] - eye), flat_heads(run[W:])], axis=0).astype(BF16)
    for n in range(pair_ref.shape[0]):
        pair_ref[n] = pair


def unpack(pair):
    pair = pair.astype(F32)
    return stack_heads(pair[:SEG]), stack_heads(pair[SEG:])


def compose_kernel(pos_ref, got_ref, pair_ref, prefix_ref):
    mine = pos_ref[0]
    eye = eye128()
    change, add = unpack(got_ref[0])
    run = jnp.concatenate([eye + change, add], axis=0)
    prefix = jnp.where(mine > 0, run, jnp.concatenate([eye, jnp.zeros((W, W), F32)], axis=0))
    for n in range(1, got_ref.shape[0]):
        change, add = unpack(got_ref[n])
        run = run + mm(run, change)
        run = jnp.concatenate([run[:W], run[W:] + add], axis=0)
        prefix = jnp.where(n < mine, run, prefix)
    pair = jnp.concatenate([flat_heads(run[:W] - eye), flat_heads(run[W:])], axis=0).astype(BF16)
    for n in range(pair_ref.shape[0]):
        pair_ref[n] = pair
    prefix_ref[...] = prefix


def readout_kernel(pos_ref, got_ref, prefix_ref, map_ref, loc_ref, gain_ref, w_ref, keep_ref, send_ref):
    mine, core = pos_ref[1], pos_ref[3]
    state = jnp.where(mine > 0, unpack(got_ref[0])[1], 0.0)
    for n in range(1, got_ref.shape[0] - 1):
        change, add = unpack(got_ref[n])
        state = jnp.where(n < mine, state + mm(state, change) + add, state)
    state = mm(state, prefix_ref[:W]) + prefix_ref[W:]
    out = loc_ref[...] + mm(map_ref[...], state, ((1,), (1,)))
    ones = same_head_ones()
    centered = out - mm(out, ones) * (1.0 / SEG)
    spread = mm(centered * centered, ones) * (1.0 / SEG)
    mixed = (centered * lax.rsqrt(spread + 0.00064) * gain_ref[...]).astype(BF16)
    for n in range(keep_ref.shape[0]):
        part = jnp.dot(mixed, w_ref[:, n * 2 * W : (n + 1) * 2 * W], preferred_element_type=F32)
        first, second = part[:, :W], part[:, W:]
        keep_ref[n] = jnp.where(core == 0, first, second).astype(BF16)
        send_ref[n] = jnp.where(core == 0, second, first).astype(BF16)


def slots_of(ids_ref, experts, capacity):
    tokens = ids_ref.shape[1]
    named = columns_of(ids_ref[...].astype(F32)).astype(jnp.int32)
    names = [named[:, k : k + 1] for k in range(2)]
    hot = [(iota((tokens, experts), 1) == name).astype(F32) for name in names]
    earlier = (iota((tokens, tokens), 0) > iota((tokens, tokens), 1)).astype(BF16)
    ahead = jnp.dot(earlier, (hot[0] + hot[1]).astype(BF16), preferred_element_type=F32)
    ranks = [
        jnp.sum(hot[0] * ahead, axis=1, keepdims=True),
        jnp.sum(hot[1] * (ahead + hot[0]), axis=1, keepdims=True),
    ]
    return [name * capacity + rank.astype(jnp.int32) for name, rank in zip(names, ranks)]


def dispatch_kernel(pos_ref, parts_ref, skip_ref, gain_ref, ids_ref, hid_ref, out_ref):
    hidden = skip_ref[...].astype(F32)
    for n in range(parts_ref.shape[0]):
        hidden = hidden + parts_ref[n].astype(F32)
    hid_ref[...] = hidden
    column = pl.multiple_of((pos_ref[2] * 2 + pos_ref[3]) * W, W)
    scaled = (hidden * gain_ref[:, pl.ds(column, W)]).astype(BF16)
    tokens, places = ids_ref.shape[1], out_ref.shape[0]
    first, second = slots_of(ids_ref, 32, 32)
    lane = iota((tokens, places), 1)
    hot = ((lane == first) | (lane == second)).astype(F32).astype(BF16)
    out_ref[...] = lax.dot_general(
        hot, scaled, (((0,), (0,)), ((), ())), preferred_element_type=F32
    ).astype(BF16)


def expert_kernel(pos_ref, own_ref, other_ref, gain_ref, w0, w1, w2, w3, keep_ref, send_ref):
    core = pos_ref[3]
    ways, rows = own_ref.shape[0], own_ref.shape[1]
    blocks = []
    for n in range(ways):
        own, other = own_ref[n], other_ref[n]
        blocks.append(jnp.where(core == 0, own, other))
        blocks.append(jnp.where(core == 0, other, own))
    data = jnp.concatenate(blocks, axis=1)
    width = data.shape[1]
    squares = jnp.zeros((rows, W), F32)
    for n, block in enumerate(blocks):
        plain = block.astype(F32) * (1.0 / gain_ref[:, n * W : (n + 1) * W])
        squares = squares + plain * plain
    scale = lax.rsqrt(jnp.sum(squares, axis=1, keepdims=True) * (1.0 / width) + 1e-06)
    hidden = []
    for w_ref in (w0, w1, w2, w3):
        both = jnp.concatenate([w_ref[:width], w_ref[width : 2 * width]], axis=1)
        act = jnp.dot(data, both, preferred_element_type=F32) * scale
        gate, up = act[:, :W], act[:, W:]
        hidden.append((gate / (1.0 + jnp.exp(-gate)) * up).astype(BF16))
    hidden = jnp.concatenate(hidden, axis=1)
    for n in range(ways):
        at = 2 * width + 2 * n * W
        pieces = [
            jnp.concatenate([w_ref[at : at + W], w_ref[at + W : at + 2 * W]], axis=1)
            for w_ref in (w0, w1, w2, w3)
        ]
        part = jnp.dot(hidden, jnp.concatenate(pieces, axis=0), preferred_element_type=F32)
        first, second = part[:, :W], part[:, W:]
        keep_ref[n] = jnp.where(core == 0, first, second).astype(BF16)
        send_ref[n] = jnp.where(core == 0, second, first).astype(BF16)


def combine_kernel(ret_ref, hid_ref, ids_ref, chance_ref, within_ref, out_ref):
    tokens, places = ids_ref.shape[1], ret_ref.shape[0]
    slots = slots_of(ids_ref, 32, 32)
    lane = iota((tokens, places), 1)
    within = within_ref[...]
    shares = columns_of(chance_ref[...] * within / jnp.sum(within, axis=0, keepdims=True))
    result = hid_ref[...]
    for k in range(2):
        hot = (lane == slots[k]).astype(F32).astype(BF16)
        picked = jnp.dot(hot, ret_ref[...], preferred_element_type=F32)
        result = result + picked * shares[:, k : k + 1]
    result = result.astype(BF16)
    for n in range(out_ref.shape[0]):
        out_ref[n] = result


def assemble_kernel(pos_ref, own_ref, other_ref, out_ref):
    core = pos_ref[3]
    for n in range(own_ref.shape[0]):
        own, other = own_ref[n], other_ref[n]
        out_ref[:, 2 * n * W : (2 * n + 1) * W] = jnp.where(core == 0, own, other)
        out_ref[:, (2 * n + 1) * W : (2 * n + 2) * W] = jnp.where(core == 0, other, own)


def call(kernel, outs, *args, scalars=0, flops=2_000_000_000, far=(), scratch=(), grant=40 << 20):
    specs = [
        pl.BlockSpec(
            memory_space=pltpu.SMEM if n < scalars else pltpu.HBM if n in far else pltpu.VMEM
        )
        for n in range(len(args))
    ]
    shapes = [jax.ShapeDtypeStruct(shape, kind) for shape, kind in outs]
    result = pl.pallas_call(
        kernel,
        out_shape=shapes if len(shapes) > 1 else shapes[0],
        in_specs=specs,
        scratch_shapes=list(scratch),
        out_specs=[pl.BlockSpec(memory_space=pltpu.VMEM)] * len(shapes)
        if len(shapes) > 1
        else pl.BlockSpec(memory_space=pltpu.VMEM),
        compiler_params=pltpu.CompilerParams(vmem_limit_bytes=grant),
        cost_estimate=pl.CostEstimate(flops=flops, bytes_accessed=1_000_000, transcendentals=0),
        interpret=INTERPRET,
    )(*args)
    return result


def exchange(parts, axes):
    return lax.all_to_all(parts, axes, split_axis=0, concat_axis=0, tiled=True)


def swap_cores(data):
    return lax.ppermute(data, "c", [(0, 1), (1, 0)])


def body(
    queries,
    keys,
    values,
    step_sizes,
    forgetting,
    forgetting_bias,
    head_gain,
    skip,
    blender,
    norm_gain,
    cluster_chance,
    within_chance,
    ids,
    switch,
    expansion,
    contraction,
):
    n_z, n_x, n_y = (lax.axis_size(a) for a in ("z", "x", "y"))
    here = [lax.axis_index(a) for a in ("x", "z", "y", "c")]
    pos = jnp.stack(here).astype(jnp.int32)
    tokens, width = skip.shape

    ring = [(((y + 1) % n_y) * 2, y * 2) for y in range(n_y)]
    ring += [(((y - 1) % n_y) * 2 + 1, y * 2 + 1) for y in range(n_y)]
    weights = [
        call(
            pack_kernel,
            [((3 * width, W), BF16)],
            switch,
            expansion,
            contraction,
            far=(0, 1, 2),
            scratch=[pltpu.SemaphoreType.DMA((2 + width // W,))],
            grant=67043328,
        )
    ]
    weights.append(lax.ppermute(weights[-1], TP, ring))
    pairs, state_map, local = call(
        mixer_kernel,
        [((n_x, W, W), BF16), ((tokens, W), F32), ((tokens, W), F32)],
        queries,
        keys,
        values,
        step_sizes,
        forgetting,
        forgetting_bias.T,
        far=range(6),
        scratch=[pltpu.VMEM((tokens, W), BF16)] * 4
        + [
            pltpu.VMEM((tokens, W), F32),
            pltpu.VMEM((2, tokens), F32),
            pltpu.SemaphoreType.DMA((6,)),
        ],
        grant=67043328,
    )
    own_skip = lax.dynamic_slice_in_dim(skip, (here[2] * 2 + here[3]) * W, W, 1)
    pairs, own_skip = lax.optimization_barrier((pairs, own_skip))
    gathered = exchange(pairs, "x")
    pairs, prefix = call(
        compose_kernel, [((n_z, W, W), BF16), ((2 * W, W), F32)], pos, gathered, scalars=1
    )
    pairs, weights[1] = lax.optimization_barrier((pairs, weights[1]))
    weights.append(lax.ppermute(weights[-1], TP, ring))
    gathered = exchange(pairs, "z")
    keep, send = call(
        readout_kernel,
        [((n_y, tokens, W), BF16), ((n_y, tokens, W), BF16)],
        pos,
        gathered,
        prefix,
        state_map,
        local,
        head_gain[None],
        blender,
        scalars=1,
    )
    branch = (keep.astype(F32) + swap_cores(send).astype(F32)).astype(BF16)
    branch, weights[2] = lax.optimization_barrier((branch, weights[2]))
    parts = exchange(branch, "y")
    parts, weights[2] = lax.optimization_barrier((parts, weights[2]))
    weights.append(lax.ppermute(weights[-1], TP, ring))
    hidden, outgoing = call(
        dispatch_kernel,
        [((tokens, W), F32), ((4 * tokens, W), BF16)],
        pos,
        parts,
        own_skip,
        norm_gain[None],
        ids.T,
        scalars=1,
    )
    arrived = exchange(outgoing.reshape(n_z * n_x, -1, W), SP).reshape(4, tokens, W)
    own = exchange(jnp.concatenate([arrived, arrived], axis=0), "y")
    keep, send = call(
        expert_kernel,
        [((n_y, tokens, W), BF16), ((n_y, tokens, W), BF16)],
        pos,
        own,
        swap_cores(own),
        norm_gain[None],
        *weights,
        scalars=1,
    )
    summed = exchange((keep.astype(F32) + swap_cores(send).astype(F32)).astype(BF16), "y")
    summed = (summed[:4].astype(F32) + summed[4:].astype(F32)).astype(BF16)
    returned = exchange(summed.reshape(n_z * n_x, -1, W), SP).reshape(4 * tokens, W)
    copies = call(
        combine_kernel,
        [((n_y, tokens, W), BF16)],
        returned,
        hidden,
        ids.T,
        cluster_chance[None],
        within_chance.T,
    )
    own = exchange(copies, "y")
    return call(assemble_kernel, [((tokens, width), BF16)], pos, own, swap_cores(own), scalars=1)


def solution(mesh):
    split = Mesh(mesh.devices.reshape(8, 4, 8, 2), ("z", "x", "y", "c"))
    in_specs = (
        P(SP, TP),
        P(SP, TP),
        P(SP, TP),
        P(SP, TP),
        P(SP, TP),
        P(SP, TP),
        P(TP),
        P(SP, None),
        P(TP, None),
        P(),
        P(SP),
        P(SP, None),
        P(SP, None),
        P(SP, None, TP),
        P(SP, None, TP),
        P(SP, TP, None),
    )
    out_specs = P(SP, None)

    return jax.shard_map(body, mesh=split, in_specs=in_specs, out_specs=out_specs, check_vma=False)
```

```python
import jax
import jax.numpy as jnp
from jax import lax
from jax.experimental import pallas as pl
from jax.experimental.pallas import tpu as pltpu
from jax.sharding import Mesh
from jax.sharding import PartitionSpec as P


SP = ("z", "x")
TP = ("y", "c")
F32 = jnp.float32
BF16 = jnp.bfloat16
SEG = 64
W = 128
DECAY = 0.6065306597126334
INTERPRET = False


def mm(a, b, contract=((1,), (0,)), precision=lax.Precision.HIGHEST):
    return lax.dot_general(
        a, b, (contract, ((), ())), precision=precision, preferred_element_type=F32
    )


def iota(shape, dim):
    return lax.broadcasted_iota(jnp.int32, shape, dim)


def stack_heads(rows):
    first = iota(rows.shape, 1) < SEG
    zero = jnp.zeros_like(rows)
    return jnp.concatenate([jnp.where(first, rows, zero), jnp.where(first, zero, rows)], axis=0)


def flat_heads(stacked):
    half = stacked.shape[0] // 2
    return stacked[:half] + stacked[half:]


def eye128():
    return (iota((W, W), 0) == iota((W, W), 1)).astype(F32)


def same_head_ones():
    return (iota((W, W), 0) // SEG == iota((W, W), 1) // SEG).astype(F32)


def pack_kernel(switch_ref, expansion_ref, contraction_ref, out_ref, sems):
    depth = switch_ref.shape[1]
    copies = [
        pltpu.make_async_copy(switch_ref.at[0], out_ref.at[pl.ds(0, depth)], sems.at[0]),
        pltpu.make_async_copy(expansion_ref.at[0], out_ref.at[pl.ds(depth, depth)], sems.at[1]),
    ]
    for n in range(depth // W):
        copies.append(
            pltpu.make_async_copy(
                contraction_ref.at[0, :, pl.ds(n * W, W)],
                out_ref.at[pl.ds(2 * depth + n * W, W)],
                sems.at[2 + n],
            )
        )
    for copy in copies:
        copy.start()
    for copy in copies:
        copy.wait()


def columns_of(rows):
    spare = jnp.zeros((6, rows.shape[1]), rows.dtype)
    return jnp.concatenate([rows, spare], axis=0).T


def mixer_kernel(*refs):
    pair_ref, map_ref, loc_ref = refs[6:9]
    held, sems = refs[9:15], refs[15]
    copies = [
        pltpu.make_async_copy(refs[n], held[n], sems.at[n]) for n in range(len(held))
    ]
    for copy in copies:
        copy.start()
    for copy in copies:
        copy.wait()
    q_ref, k_ref, v_ref, s_ref, f_ref, b_ref = held
    bias_columns = columns_of(b_ref[...])
    rows = q_ref.shape[0]
    chunks = rows // SEG
    query = q_ref[...].astype(F32)
    key = k_ref[...].astype(F32)
    value = v_ref[...].astype(F32)
    rate = 1.0 / (1.0 + jnp.exp(-s_ref[...].astype(F32)))
    bias = jnp.where(iota((rows, W), 1) < SEG, bias_columns[:, 0:1], bias_columns[:, 1:2])
    decay = bias - DECAY / (1.0 + jnp.exp(-f_ref[...]))
    removal = key * lax.rsqrt(mm(key * key, same_head_ones()) + 1e-06)
    beta = removal * rate
    row, col = iota((rows, rows), 0), iota((rows, rows), 1)
    below = ((row // SEG == col // SEG) & (row >= col)).astype(F32)
    total = mm(below, decay)

    row, col = iota((W, W), 0), iota((W, W), 1)
    same = row // SEG == col // SEG
    strict = same & (row > col)
    inclusive = same & (row >= col)
    eye = eye128()

    part = []
    for n in range(chunks):
        at = slice(n * SEG, (n + 1) * SEG)
        cum = total[at]
        before = cum - decay[at]
        middle = cum[SEG // 2 - 1 : SEG // 2]
        closing = cum[SEG - 1 : SEG]
        up = jnp.exp(cum - middle)
        down = jnp.exp(middle - cum)
        left = jnp.exp(before - middle)
        opening = jnp.exp(middle)
        ending = jnp.exp(closing - middle)
        alpha = -removal[at] * left
        asked = query[at] * up
        beta_hat = beta[at] * down
        key_hat = key[at] * down
        scores = mm(
            jnp.concatenate([stack_heads(alpha), stack_heads(asked)], axis=0),
            jnp.concatenate([stack_heads(beta_hat), stack_heads(key_hat)], axis=0),
            ((1,), (1,)),
        )
        remove_remove = jnp.where(strict, scores[:W, :W], 0.0)
        remove_write = jnp.where(strict, scores[:W, W:], 0.0)
        read_remove = jnp.where(inclusive, scores[W:, :W], 0.0)
        read_write = jnp.where(inclusive, scores[W:, W:], 0.0)
        part.append(
            dict(
                near=remove_remove,
                write=remove_write,
                read=jnp.concatenate([read_remove, read_write], axis=1),
                read_remove=read_remove,
                alpha=stack_heads(alpha * opening),
                asked=stack_heads(asked * opening),
                value=stack_heads(value[at]),
                bar=jnp.concatenate(
                    [stack_heads(beta_hat * ending), stack_heads(key_hat * ending)], axis=0
                ),
                closing=jnp.exp(closing),
            )
        )
    inverse = [eye + jnp.where(row // 2 == col // 2, p["near"], 0.0) for p in part]
    for level in (4, 8, 16, 32, 64):
        joint = (row // level == col // level) & (row // (level // 2) != col // (level // 2))
        step = [mm(jnp.where(joint, p["near"], 0.0), x) for p, x in zip(part, inverse)]
        inverse = [x + mm(x, s) for x, s in zip(inverse, step)]
    wrote = [mm(p["write"], p["value"]) for p in part]
    solved = [
        mm(x, jnp.concatenate([p["alpha"], w], axis=1)) for x, p, w in zip(inverse, part, wrote)
    ]
    keeps, adds, reads, locals_ = [], [], [], []
    for p, s in zip(part, solved):
        absorb, carried = s[:, :W], s[:, W:]
        keeps.append(mm(absorb, p["bar"][:W], ((0,), (0,))) + eye * p["closing"])
        adds.append(
            mm(jnp.concatenate([carried, p["value"]], axis=0), p["bar"], ((0,), (0,)))
        )
        locals_.append(
            flat_heads(mm(p["read"], jnp.concatenate([carried, p["value"]], axis=0)))
        )
        reads.append(flat_heads(p["asked"] + mm(p["read_remove"], absorb)))
    map_ref[:SEG, :] = reads[0]
    loc_ref[:SEG, :] = locals_[0]
    run = jnp.concatenate([keeps[0], adds[0]], axis=0)
    for n in range(1, chunks):
        at = slice(n * SEG, (n + 1) * SEG)
        both = mm(reads[n], run, ((1,), (1,)))
        map_ref[at, :] = both[:, :W]
        loc_ref[at, :] = locals_[n] + both[:, W:]
        run = mm(run, keeps[n])
        run = jnp.concatenate([run[:W], run[W:] + adds[n]], axis=0)
    pair = jnp.concatenate([flat_heads(run[:W] - eye), flat_heads(run[W:])], axis=0).astype(BF16)
    for n in range(pair_ref.shape[0]):
        pair_ref[n] = pair


def unpack(pair):
    pair = pair.astype(F32)
    return stack_heads(pair[:SEG]), stack_heads(pair[SEG:])


def compose_kernel(pos_ref, got_ref, pair_ref, prefix_ref):
    mine = pos_ref[0]
    eye = eye128()
    change, add = unpack(got_ref[0])
    run = jnp.concatenate([eye + change, add], axis=0)
    prefix = jnp.where(mine > 0, run, jnp.concatenate([eye, jnp.zeros((W, W), F32)], axis=0))
    for n in range(1, got_ref.shape[0]):
        change, add = unpack(got_ref[n])
        run = run + mm(run, change)
        run = jnp.concatenate([run[:W], run[W:] + add], axis=0)
        prefix = jnp.where(n < mine, run, prefix)
    pair = jnp.concatenate([flat_heads(run[:W] - eye), flat_heads(run[W:])], axis=0).astype(BF16)
    for n in range(pair_ref.shape[0]):
        pair_ref[n] = pair
    prefix_ref[...] = prefix


def readout_kernel(pos_ref, got_ref, prefix_ref, map_ref, loc_ref, gain_ref, w_ref, keep_ref, send_ref):
    mine, core = pos_ref[1], pos_ref[3]
    state = jnp.where(mine > 0, unpack(got_ref[0])[1], 0.0)
    for n in range(1, got_ref.shape[0] - 1):
        change, add = unpack(got_ref[n])
        state = jnp.where(n < mine, state + mm(state, change) + add, state)
    state = mm(state, prefix_ref[:W]) + prefix_ref[W:]
    out = loc_ref[...] + mm(map_ref[...], state, ((1,), (1,)))
    ones = same_head_ones()
    centered = out - mm(out, ones) * (1.0 / SEG)
    spread = mm(centered * centered, ones) * (1.0 / SEG)
    mixed = (centered * lax.rsqrt(spread + 0.00064) * gain_ref[...]).astype(BF16)
    for n in range(keep_ref.shape[0]):
        part = jnp.dot(mixed, w_ref[:, n * 2 * W : (n + 1) * 2 * W], preferred_element_type=F32)
        first, second = part[:, :W], part[:, W:]
        keep_ref[n] = jnp.where(core == 0, first, second).astype(BF16)
        send_ref[n] = jnp.where(core == 0, second, first).astype(BF16)


def slots_of(ids_ref, experts, capacity):
    tokens = ids_ref.shape[1]
    named = columns_of(ids_ref[...].astype(F32)).astype(jnp.int32)
    names = [named[:, k : k + 1] for k in range(2)]
    hot = [(iota((tokens, experts), 1) == name).astype(F32) for name in names]
    earlier = (iota((tokens, tokens), 0) > iota((tokens, tokens), 1)).astype(BF16)
    ahead = jnp.dot(earlier, (hot[0] + hot[1]).astype(BF16), preferred_element_type=F32)
    ranks = [
        jnp.sum(hot[0] * ahead, axis=1, keepdims=True),
        jnp.sum(hot[1] * (ahead + hot[0]), axis=1, keepdims=True),
    ]
    return [name * capacity + rank.astype(jnp.int32) for name, rank in zip(names, ranks)]


def dispatch_kernel(pos_ref, parts_ref, skip_ref, gain_ref, ids_ref, hid_ref, out_ref):
    hidden = skip_ref[...].astype(F32)
    for n in range(parts_ref.shape[0]):
        hidden = hidden + parts_ref[n].astype(F32)
    hid_ref[...] = hidden
    column = pl.multiple_of((pos_ref[2] * 2 + pos_ref[3]) * W, W)
    scaled = (hidden * gain_ref[:, pl.ds(column, W)]).astype(BF16)
    tokens, places = ids_ref.shape[1], out_ref.shape[0] * out_ref.shape[1] // 2
    first, second = slots_of(ids_ref, 32, 32)
    lane = iota((tokens, places), 1)
    hot = ((lane == first) | (lane == second)).astype(F32).astype(BF16)
    rows = lax.dot_general(hot, scaled, (((0,), (0,)), ((), ())), preferred_element_type=F32)
    rows = rows.astype(BF16).reshape(32, 32, W)
    out_ref[:, :32, :] = rows
    out_ref[:, 32:, :] = rows


def expert_kernel(pos_ref, own_ref, other_ref, gain_ref, w0, w1, w2, w3, keep_ref, send_ref):
    core = pos_ref[3]
    sources, ways, lines, _ = own_ref.shape
    rows, width = sources * lines, gain_ref.shape[1]
    blocks = []
    for n in range(ways):
        own = own_ref[:, n].astype(F32).reshape(rows, W)
        other = other_ref[:, n].astype(F32).reshape(rows, W)
        blocks.append(jnp.where(core == 0, own, other))
        blocks.append(jnp.where(core == 0, other, own))
    data = jnp.concatenate([block.astype(BF16) for block in blocks], axis=1)
    squares = jnp.zeros((rows, W), F32)
    for n, block in enumerate(blocks):
        plain = block * (1.0 / gain_ref[:, n * W : (n + 1) * W])
        squares = squares + plain * plain
    scale = lax.rsqrt(jnp.sum(squares, axis=1, keepdims=True) * (1.0 / width) + 1e-06)
    hidden = []
    for w_ref in (w0, w1, w2, w3):
        both = jnp.concatenate([w_ref[:width], w_ref[width : 2 * width]], axis=1)
        act = jnp.dot(data, both, preferred_element_type=F32) * scale
        gate, up = act[:, :W], act[:, W:]
        hidden.append((gate / (1.0 + jnp.exp(-gate)) * up).astype(BF16))
    hidden = jnp.concatenate(hidden, axis=1)
    for n in range(ways):
        at = 2 * width + 2 * n * W
        pieces = [
            jnp.concatenate([w_ref[at : at + W], w_ref[at + W : at + 2 * W]], axis=1)
            for w_ref in (w0, w1, w2, w3)
        ]
        part = jnp.dot(hidden, jnp.concatenate(pieces, axis=0), preferred_element_type=F32)
        first, second = part[:, :W], part[:, W:]
        keep = jnp.where(core == 0, first, second).reshape(sources, lines, W)
        send = jnp.where(core == 0, second, first).reshape(sources, lines, W)
        keep_ref[:, n] = keep.astype(BF16)
        send_ref[:, n] = send.astype(BF16)


def combine_kernel(ret_ref, hid_ref, ids_ref, chance_ref, within_ref, out_ref):
    half = ret_ref.shape[1] // 2
    rows = ret_ref[:, :half].astype(F32) + ret_ref[:, half:].astype(F32)
    rows = rows.reshape(-1, W).astype(BF16)
    tokens, places = ids_ref.shape[1], rows.shape[0]
    slots = slots_of(ids_ref, 32, 32)
    lane = iota((tokens, places), 1)
    within = within_ref[...]
    shares = columns_of(chance_ref[...] * within / jnp.sum(within, axis=0, keepdims=True))
    result = hid_ref[...]
    for k in range(2):
        hot = (lane == slots[k]).astype(F32).astype(BF16)
        picked = jnp.dot(hot, rows, preferred_element_type=F32)
        result = result + picked * shares[:, k : k + 1]
    result = result.astype(BF16)
    for n in range(out_ref.shape[0]):
        out_ref[n] = result


def assemble_kernel(pos_ref, own_ref, other_ref, out_ref):
    core = pos_ref[3]
    for n in range(own_ref.shape[0]):
        own, other = own_ref[n], other_ref[n]
        out_ref[:, 2 * n * W : (2 * n + 1) * W] = jnp.where(core == 0, own, other)
        out_ref[:, (2 * n + 1) * W : (2 * n + 2) * W] = jnp.where(core == 0, other, own)


def call(kernel, outs, *args, scalars=0, flops=2_000_000_000, far=(), scratch=(), grant=40 << 20):
    specs = [
        pl.BlockSpec(
            memory_space=pltpu.SMEM if n < scalars else pltpu.HBM if n in far else pltpu.VMEM
        )
        for n in range(len(args))
    ]
    shapes = [jax.ShapeDtypeStruct(shape, kind) for shape, kind in outs]
    result = pl.pallas_call(
        kernel,
        out_shape=shapes if len(shapes) > 1 else shapes[0],
        in_specs=specs,
        scratch_shapes=list(scratch),
        out_specs=[pl.BlockSpec(memory_space=pltpu.VMEM)] * len(shapes)
        if len(shapes) > 1
        else pl.BlockSpec(memory_space=pltpu.VMEM),
        compiler_params=pltpu.CompilerParams(vmem_limit_bytes=grant),
        cost_estimate=pl.CostEstimate(flops=flops, bytes_accessed=1_000_000, transcendentals=0),
        interpret=INTERPRET,
    )(*args)
    return result


def exchange(parts, axes):
    return lax.all_to_all(parts, axes, split_axis=0, concat_axis=0, tiled=True)


def swap_cores(data):
    return lax.ppermute(data, "c", [(0, 1), (1, 0)])


def body(
    queries,
    keys,
    values,
    step_sizes,
    forgetting,
    forgetting_bias,
    head_gain,
    skip,
    blender,
    norm_gain,
    cluster_chance,
    within_chance,
    ids,
    switch,
    expansion,
    contraction,
):
    n_z, n_x, n_y = (lax.axis_size(a) for a in ("z", "x", "y"))
    here = [lax.axis_index(a) for a in ("x", "z", "y", "c")]
    pos = jnp.stack(here).astype(jnp.int32)
    tokens, width = skip.shape

    ring = [(((y + 1) % n_y) * 2, y * 2) for y in range(n_y)]
    ring += [(((y - 1) % n_y) * 2 + 1, y * 2 + 1) for y in range(n_y)]
    weights = [
        call(
            pack_kernel,
            [((3 * width, W), BF16)],
            switch,
            expansion,
            contraction,
            far=(0, 1, 2),
            scratch=[pltpu.SemaphoreType.DMA((2 + width // W,))],
            grant=67043328,
        )
    ]
    weights.append(lax.ppermute(weights[-1], TP, ring))
    pairs, state_map, local = call(
        mixer_kernel,
        [((n_x, W, W), BF16), ((tokens, W), F32), ((tokens, W), F32)],
        queries,
        keys,
        values,
        step_sizes,
        forgetting,
        forgetting_bias.T,
        far=range(6),
        scratch=[pltpu.VMEM((tokens, W), BF16)] * 4
        + [
            pltpu.VMEM((tokens, W), F32),
            pltpu.VMEM((2, tokens), F32),
            pltpu.SemaphoreType.DMA((6,)),
        ],
        grant=67043328,
    )
    own_skip = lax.dynamic_slice_in_dim(skip, (here[2] * 2 + here[3]) * W, W, 1)
    gathered = exchange(pairs, "x")
    gathered, own_skip = lax.optimization_barrier((gathered, own_skip))
    pairs, prefix = call(
        compose_kernel, [((n_z, W, W), BF16), ((2 * W, W), F32)], pos, gathered, scalars=1
    )
    pairs, weights[1] = lax.optimization_barrier((pairs, weights[1]))
    weights.append(lax.ppermute(weights[-1], TP, ring))
    gathered = exchange(pairs, "z")
    keep, send = call(
        readout_kernel,
        [((n_y, tokens, W), BF16), ((n_y, tokens, W), BF16)],
        pos,
        gathered,
        prefix,
        state_map,
        local,
        head_gain[None],
        blender,
        scalars=1,
    )
    branch = (keep.astype(F32) + swap_cores(send).astype(F32)).astype(BF16)
    branch, weights[2] = lax.optimization_barrier((branch, weights[2]))
    parts = exchange(branch, "y")
    parts, weights[2] = lax.optimization_barrier((parts, weights[2]))
    weights.append(lax.ppermute(weights[-1], TP, ring))
    hidden, outgoing = call(
        dispatch_kernel,
        [((tokens, W), F32), ((n_z * n_x, 64, W), BF16)],
        pos,
        parts,
        own_skip,
        norm_gain[None],
        ids.T,
        scalars=1,
    )
    own = exchange(outgoing.reshape(n_z * n_x * n_y, 8, W), ("z", "x", "y"))
    own = own.reshape(n_z * n_x, n_y, 8, W)
    keep, send = call(
        expert_kernel,
        [((n_z * n_x, n_y, 8, W), BF16), ((n_z * n_x, n_y, 8, W), BF16)],
        pos,
        own,
        swap_cores(own),
        norm_gain[None],
        *weights,
        scalars=1,
    )
    summed = (keep.astype(F32) + swap_cores(send).astype(F32)).astype(BF16)
    returned = exchange(summed.reshape(n_z * n_x * n_y, 8, W), ("z", "x", "y"))
    returned = returned.reshape(n_z * n_x, n_y, 8, W)
    copies = call(
        combine_kernel,
        [((n_y, tokens, W), BF16)],
        returned,
        hidden,
        ids.T,
        cluster_chance[None],
        within_chance.T,
    )
    own = exchange(copies, "y")
    return call(assemble_kernel, [((tokens, width), BF16)], pos, own, swap_cores(own), scalars=1)


def solution(mesh):
    split = Mesh(mesh.devices.reshape(8, 4, 8, 2), ("z", "x", "y", "c"))
    in_specs = (
        P(SP, TP),
        P(SP, TP),
        P(SP, TP),
        P(SP, TP),
        P(SP, TP),
        P(SP, TP),
        P(TP),
        P(SP, None),
        P(TP, None),
        P(),
        P(SP),
        P(SP, None),
        P(SP, None),
        P(SP, None, TP),
        P(SP, None, TP),
        P(SP, TP, None),
    )
    out_specs = P(SP, None)

    return jax.shard_map(body, mesh=split, in_specs=in_specs, out_specs=out_specs, check_vma=False)
```

```python
import jax
import jax.numpy as jnp
from jax import lax
from jax.experimental import pallas as pl
from jax.experimental.pallas import tpu as pltpu
from jax.sharding import Mesh
from jax.sharding import PartitionSpec as P


SP = ("z", "x")
TP = ("y", "c")
F32 = jnp.float32
BF16 = jnp.bfloat16
SEG = 64
W = 128
DECAY = 0.6065306597126334
INTERPRET = False


def dot(a, b, contract=((1,), (0,))):
    return lax.dot_general(a, b, (contract, ((), ())), preferred_element_type=F32)


def halves(a):
    high = a.astype(BF16)
    return high, (a - high.astype(F32)).astype(BF16)


def mm(a, b, contract=((1,), (0,))):
    (a_high, a_low), (b_high, b_low) = halves(a), halves(b)
    return dot(a_high, b_high, contract) + (
        dot(a_high, b_low, contract) + dot(a_low, b_high, contract)
    )


def mm_exact(a, b, contract=((1,), (0,))):
    high, low = halves(a)
    return dot(high, b, contract) + dot(low, b, contract)


def iota(shape, dim):
    return lax.broadcasted_iota(jnp.int32, shape, dim)


def stack_heads(rows):
    first = iota(rows.shape, 1) < SEG
    zero = jnp.zeros_like(rows)
    return jnp.concatenate([jnp.where(first, rows, zero), jnp.where(first, zero, rows)], axis=0)


def flat_heads(stacked):
    half = stacked.shape[0] // 2
    return stacked[:half] + stacked[half:]


def eye128():
    return (iota((W, W), 0) == iota((W, W), 1)).astype(F32)


def same_head_ones():
    return (iota((W, W), 0) // SEG == iota((W, W), 1) // SEG).astype(F32).astype(BF16)


def pack_kernel(switch_ref, expansion_ref, contraction_ref, out_ref, sems):
    depth = switch_ref.shape[1]
    copies = [
        pltpu.make_async_copy(switch_ref.at[0], out_ref.at[pl.ds(0, depth)], sems.at[0]),
        pltpu.make_async_copy(expansion_ref.at[0], out_ref.at[pl.ds(depth, depth)], sems.at[1]),
    ]
    for n in range(depth // W):
        copies.append(
            pltpu.make_async_copy(
                contraction_ref.at[0, :, pl.ds(n * W, W)],
                out_ref.at[pl.ds(2 * depth + n * W, W)],
                sems.at[2 + n],
            )
        )
    for copy in copies:
        copy.start()
    for copy in copies:
        copy.wait()


def columns_of(rows):
    spare = jnp.zeros((6, rows.shape[1]), rows.dtype)
    return jnp.concatenate([rows, spare], axis=0).T


def mixer_kernel(*refs):
    pair_ref, map_ref, loc_ref = refs[6:9]
    held, sems = refs[9:15], refs[15]
    copies = [
        pltpu.make_async_copy(refs[n], held[n], sems.at[n]) for n in range(len(held))
    ]
    for copy in copies:
        copy.start()
    for copy in copies:
        copy.wait()
    q_ref, k_ref, v_ref, s_ref, f_ref, b_ref = held
    bias_columns = columns_of(b_ref[...])
    rows = q_ref.shape[0]
    chunks = rows // SEG
    query = q_ref[...].astype(F32)
    key = k_ref[...].astype(F32)
    value = v_ref[...].astype(F32)
    rate = 1.0 / (1.0 + jnp.exp(-s_ref[...].astype(F32)))
    bias = jnp.where(iota((rows, W), 1) < SEG, bias_columns[:, 0:1], bias_columns[:, 1:2])
    decay = bias - DECAY / (1.0 + jnp.exp(-f_ref[...]))
    removal = key * lax.rsqrt(mm_exact(key * key, same_head_ones()) + 1e-06)
    beta = removal * rate
    row, col = iota((rows, rows), 0), iota((rows, rows), 1)
    below = ((row // SEG == col // SEG) & (row >= col)).astype(F32).astype(BF16)
    high, low = halves(decay)
    rest = (decay - high.astype(F32) - low.astype(F32)).astype(BF16)
    total = dot(below, high) + (dot(below, low) + dot(below, rest))

    row, col = iota((W, W), 0), iota((W, W), 1)
    same = row // SEG == col // SEG
    strict = same & (row > col)
    inclusive = same & (row >= col)
    eye = eye128()

    part = []
    for n in range(chunks):
        at = slice(n * SEG, (n + 1) * SEG)
        cum = total[at]
        before = cum - decay[at]
        middle = cum[SEG // 2 - 1 : SEG // 2]
        closing = cum[SEG - 1 : SEG]
        up = jnp.exp(cum - middle)
        down = jnp.exp(middle - cum)
        left = jnp.exp(before - middle)
        opening = jnp.exp(middle)
        ending = jnp.exp(closing - middle)
        alpha = -removal[at] * left
        asked = query[at] * up
        beta_hat = beta[at] * down
        key_hat = key[at] * down
        scores = mm(
            jnp.concatenate([stack_heads(alpha), stack_heads(asked)], axis=0),
            jnp.concatenate([stack_heads(beta_hat), stack_heads(key_hat)], axis=0),
            ((1,), (1,)),
        )
        remove_remove = jnp.where(strict, scores[:W, :W], 0.0)
        remove_write = jnp.where(strict, scores[:W, W:], 0.0)
        read_remove = jnp.where(inclusive, scores[W:, :W], 0.0)
        read_write = jnp.where(inclusive, scores[W:, W:], 0.0)
        part.append(
            dict(
                near=remove_remove,
                write=remove_write,
                read=jnp.concatenate([read_remove, read_write], axis=1),
                read_remove=read_remove,
                alpha=stack_heads(alpha * opening),
                asked=stack_heads(asked * opening),
                value=stack_heads(value[at]),
                bar=jnp.concatenate(
                    [stack_heads(beta_hat * ending), stack_heads(key_hat * ending)], axis=0
                ),
                closing=jnp.exp(closing),
            )
        )
    inverse = [eye + jnp.where(row // 2 == col // 2, p["near"], 0.0) for p in part]
    for level in (4, 8, 16, 32, 64):
        joint = (row // level == col // level) & (row // (level // 2) != col // (level // 2))
        step = [mm(jnp.where(joint, p["near"], 0.0), x) for p, x in zip(part, inverse)]
        inverse = [x + mm(x, s) for x, s in zip(inverse, step)]
    wrote = [mm(p["write"], p["value"]) for p in part]
    solved = [
        mm(x, jnp.concatenate([p["alpha"], w], axis=1)) for x, p, w in zip(inverse, part, wrote)
    ]
    keeps, adds, reads, locals_ = [], [], [], []
    for p, s in zip(part, solved):
        absorb, carried = s[:, :W], s[:, W:]
        keeps.append(mm(absorb, p["bar"][:W], ((0,), (0,))) + eye * p["closing"])
        adds.append(
            mm(jnp.concatenate([carried, p["value"]], axis=0), p["bar"], ((0,), (0,)))
        )
        locals_.append(
            flat_heads(mm(p["read"], jnp.concatenate([carried, p["value"]], axis=0)))
        )
        reads.append(flat_heads(p["asked"] + mm(p["read_remove"], absorb)))
    map_ref[:SEG, :] = reads[0]
    loc_ref[:SEG, :] = locals_[0]
    run = jnp.concatenate([keeps[0], adds[0]], axis=0)
    for n in range(1, chunks):
        at = slice(n * SEG, (n + 1) * SEG)
        both = mm(reads[n], run, ((1,), (1,)))
        map_ref[at, :] = both[:, :W]
        loc_ref[at, :] = locals_[n] + both[:, W:]
        run = mm(run, keeps[n])
        run = jnp.concatenate([run[:W], run[W:] + adds[n]], axis=0)
    pair = jnp.concatenate([flat_heads(run[:W] - eye), flat_heads(run[W:])], axis=0).astype(BF16)
    for n in range(pair_ref.shape[0]):
        pair_ref[n] = pair


def unpack(pair):
    pair = pair.astype(F32)
    return stack_heads(pair[:SEG]), stack_heads(pair[SEG:])


def times(state, change):
    return state + mm_exact(state, change.astype(BF16))


def compose_kernel(pos_ref, got_ref, pair_ref, prefix_ref):
    mine = pos_ref[0]
    eye = eye128()
    change, add = unpack(got_ref[0])
    run = jnp.concatenate([eye + change, add], axis=0)
    prefix = jnp.where(mine > 0, run, jnp.concatenate([eye, jnp.zeros((W, W), F32)], axis=0))
    for n in range(1, got_ref.shape[0]):
        change, add = unpack(got_ref[n])
        run = times(run, change)
        run = jnp.concatenate([run[:W], run[W:] + add], axis=0)
        prefix = jnp.where(n < mine, run, prefix)
    pair = jnp.concatenate([flat_heads(run[:W] - eye), flat_heads(run[W:])], axis=0).astype(BF16)
    for n in range(pair_ref.shape[0]):
        pair_ref[n] = pair
    prefix_ref[...] = prefix


def readout_kernel(pos_ref, got_ref, prefix_ref, map_ref, loc_ref, gain_ref, w_ref, keep_ref, send_ref):
    mine, core = pos_ref[1], pos_ref[3]
    state = jnp.where(mine > 0, unpack(got_ref[0])[1], 0.0)
    for n in range(1, got_ref.shape[0] - 1):
        change, add = unpack(got_ref[n])
        state = jnp.where(n < mine, times(state, change) + add, state)
    state = mm(state, prefix_ref[:W]) + prefix_ref[W:]
    out = loc_ref[...] + mm(map_ref[...], state, ((1,), (1,)))
    ones = same_head_ones()
    centered = out - mm_exact(out, ones) * (1.0 / SEG)
    spread = mm_exact(centered * centered, ones) * (1.0 / SEG)
    mixed = (centered * lax.rsqrt(spread + 0.00064) * gain_ref[...]).astype(BF16)
    for n in range(keep_ref.shape[0]):
        part = jnp.dot(mixed, w_ref[:, n * 2 * W : (n + 1) * 2 * W], preferred_element_type=F32)
        first, second = part[:, :W], part[:, W:]
        keep_ref[n] = jnp.where(core == 0, first, second).astype(BF16)
        send_ref[n] = jnp.where(core == 0, second, first).astype(BF16)


def route_kernel(table_ref, hot_ref, high_ref, low_ref):
    experts, capacity = 32, 32
    tokens, places = table_ref.shape[1], hot_ref.shape[0]
    names = [table_ref[k : k + 1, :] for k in range(2)]
    hot = [(iota((experts, tokens), 0).astype(F32) == name).astype(F32) for name in names]
    earlier = (iota((tokens, tokens), 0) < iota((tokens, tokens), 1)).astype(F32).astype(BF16)
    ahead = dot((hot[0] + hot[1]).astype(BF16), earlier)
    ranks = [
        jnp.sum(hot[0] * ahead, axis=0, keepdims=True),
        jnp.sum(hot[1] * (ahead + hot[0]), axis=0, keepdims=True),
    ]
    slots = [name * capacity + rank for name, rank in zip(names, ranks)]
    place = iota((places, tokens), 0).astype(F32)
    hot_ref[...] = ((place == slots[0]) | (place == slots[1])).astype(F32).astype(BF16)
    shares = columns_of(table_ref[2:4, :])
    found = columns_of(jnp.concatenate(slots, axis=0))
    place = iota((tokens, places), 1).astype(F32)
    weight = jnp.zeros((tokens, places), F32)
    for k in range(2):
        weight = weight + jnp.where(place == found[:, k : k + 1], shares[:, k : k + 1], 0.0)
    high_ref[...], low_ref[...] = halves(weight)


def dispatch_kernel(pos_ref, parts_ref, skip_ref, gain_ref, hot_ref, hid_ref, out_ref):
    hidden = skip_ref[...].astype(F32)
    for n in range(parts_ref.shape[0]):
        hidden = hidden + parts_ref[n].astype(F32)
    hid_ref[...] = hidden
    column = pl.multiple_of((pos_ref[2] * 2 + pos_ref[3]) * W, W)
    scaled = (hidden * gain_ref[:, pl.ds(column, W)]).astype(BF16)
    rows = dot(hot_ref[...], scaled).astype(BF16).reshape(32, 32, W)
    out_ref[:, :32, :] = rows
    out_ref[:, 32:, :] = rows


def expert_kernel(pos_ref, own_ref, other_ref, gain_ref, w0, w1, w2, w3, keep_ref, send_ref):
    core = pos_ref[3]
    sources, ways, lines, _ = own_ref.shape
    rows, width = sources * lines, gain_ref.shape[1]
    blocks = []
    for n in range(ways):
        own = own_ref[:, n].astype(F32).reshape(rows, W)
        other = other_ref[:, n].astype(F32).reshape(rows, W)
        blocks.append(jnp.where(core == 0, own, other))
        blocks.append(jnp.where(core == 0, other, own))
    data = jnp.concatenate([block.astype(BF16) for block in blocks], axis=1)
    squares = jnp.zeros((rows, W), F32)
    for n, block in enumerate(blocks):
        plain = block * (1.0 / gain_ref[:, n * W : (n + 1) * W])
        squares = squares + plain * plain
    scale = lax.rsqrt(jnp.sum(squares, axis=1, keepdims=True) * (1.0 / width) + 1e-06)
    hidden = []
    for w_ref in (w0, w1, w2, w3):
        both = jnp.concatenate([w_ref[:width], w_ref[width : 2 * width]], axis=1)
        act = jnp.dot(data, both, preferred_element_type=F32) * scale
        gate, up = act[:, :W], act[:, W:]
        hidden.append((gate / (1.0 + jnp.exp(-gate)) * up).astype(BF16))
    hidden = jnp.concatenate(hidden, axis=1)
    for n in range(ways):
        at = 2 * width + 2 * n * W
        pieces = [
            jnp.concatenate([w_ref[at : at + W], w_ref[at + W : at + 2 * W]], axis=1)
            for w_ref in (w0, w1, w2, w3)
        ]
        part = jnp.dot(hidden, jnp.concatenate(pieces, axis=0), preferred_element_type=F32)
        first, second = part[:, :W], part[:, W:]
        keep = jnp.where(core == 0, first, second).reshape(sources, lines, W)
        send = jnp.where(core == 0, second, first).reshape(sources, lines, W)
        keep_ref[:, n] = keep.astype(BF16)
        send_ref[:, n] = send.astype(BF16)


def combine_kernel(ret_ref, hid_ref, high_ref, low_ref, out_ref):
    half = ret_ref.shape[1] // 2
    rows = ret_ref[:, :half].astype(F32) + ret_ref[:, half:].astype(F32)
    rows = rows.reshape(-1, W).astype(BF16)
    result = hid_ref[...] + (dot(high_ref[...], rows) + dot(low_ref[...], rows))
    result = result.astype(BF16)
    for n in range(out_ref.shape[0]):
        out_ref[n] = result


def columns_out(first, blocks_ref, out_ref, sems):
    copies = []
    for n in range(blocks_ref.shape[0]):
        column = pl.multiple_of((2 * n + first) * W, W)
        copies.append(
            pltpu.make_async_copy(blocks_ref.at[n], out_ref.at[:, pl.ds(column, W)], sems.at[n])
        )
    for copy in copies:
        copy.start()
    for copy in copies:
        copy.wait()


def own_out_kernel(pos_ref, own_ref, out_ref, sems):
    columns_out(pos_ref[3], own_ref, out_ref, sems)


def other_out_kernel(pos_ref, other_ref, half_ref, out_ref, sems):
    columns_out(1 - pos_ref[3], other_ref, out_ref, sems)


def output_call(kernel, shape, pos, blocks, *half):
    near = [pl.BlockSpec(memory_space=pltpu.SMEM), pl.BlockSpec(memory_space=pltpu.VMEM)]
    return pl.pallas_call(
        kernel,
        out_shape=jax.ShapeDtypeStruct(shape, BF16),
        in_specs=near + [pl.BlockSpec(memory_space=pl.ANY)] * len(half),
        out_specs=pl.BlockSpec(memory_space=pl.ANY),
        scratch_shapes=[pltpu.SemaphoreType.DMA((blocks.shape[0],))],
        input_output_aliases={2: 0} if half else {},
        compiler_params=pltpu.CompilerParams(vmem_limit_bytes=8 << 20),
        cost_estimate=pl.CostEstimate(
            flops=1_000_000_000, bytes_accessed=1_000_000, transcendentals=0
        ),
        interpret=INTERPRET,
    )(pos, blocks, *half)


def call(kernel, outs, *args, scalars=0, flops=2_000_000_000, far=(), scratch=(), grant=40 << 20):
    specs = [
        pl.BlockSpec(
            memory_space=pltpu.SMEM if n < scalars else pltpu.HBM if n in far else pltpu.VMEM
        )
        for n in range(len(args))
    ]
    shapes = [jax.ShapeDtypeStruct(shape, kind) for shape, kind in outs]
    result = pl.pallas_call(
        kernel,
        out_shape=shapes if len(shapes) > 1 else shapes[0],
        in_specs=specs,
        scratch_shapes=list(scratch),
        out_specs=[pl.BlockSpec(memory_space=pltpu.VMEM)] * len(shapes)
        if len(shapes) > 1
        else pl.BlockSpec(memory_space=pltpu.VMEM),
        compiler_params=pltpu.CompilerParams(vmem_limit_bytes=grant),
        cost_estimate=pl.CostEstimate(flops=flops, bytes_accessed=1_000_000, transcendentals=0),
        interpret=INTERPRET,
    )(*args)
    return result


def exchange(parts, axes):
    return lax.all_to_all(parts, axes, split_axis=0, concat_axis=0, tiled=True)


def swap_cores(data):
    return lax.ppermute(data, "c", [(0, 1), (1, 0)])


def body(
    queries,
    keys,
    values,
    step_sizes,
    forgetting,
    forgetting_bias,
    head_gain,
    skip,
    blender,
    norm_gain,
    cluster_chance,
    within_chance,
    ids,
    switch,
    expansion,
    contraction,
):
    n_z, n_x, n_y = (lax.axis_size(a) for a in ("z", "x", "y"))
    here = [lax.axis_index(a) for a in ("x", "z", "y", "c")]
    pos = jnp.stack(here).astype(jnp.int32)
    tokens, width = skip.shape

    ring = [(((y + 1) % n_y) * 2, y * 2) for y in range(n_y)]
    ring += [(((y - 1) % n_y) * 2 + 1, y * 2 + 1) for y in range(n_y)]
    weights = [
        call(
            pack_kernel,
            [((3 * width, W), BF16)],
            switch,
            expansion,
            contraction,
            far=(0, 1, 2),
            scratch=[pltpu.SemaphoreType.DMA((2 + width // W,))],
            grant=67043328,
        )
    ]
    weights.append(lax.ppermute(weights[-1], TP, ring))
    pairs, state_map, local = call(
        mixer_kernel,
        [((n_x, W, W), BF16), ((tokens, W), F32), ((tokens, W), F32)],
        queries,
        keys,
        values,
        step_sizes,
        forgetting,
        forgetting_bias.T,
        far=range(6),
        scratch=[pltpu.VMEM((tokens, W), BF16)] * 4
        + [
            pltpu.VMEM((tokens, W), F32),
            pltpu.VMEM((2, tokens), F32),
            pltpu.SemaphoreType.DMA((6,)),
        ],
        grant=67043328,
    )
    own_skip = lax.dynamic_slice_in_dim(skip, (here[2] * 2 + here[3]) * W, W, 1)
    gathered = exchange(pairs, "x")
    shares = within_chance.T
    shares = cluster_chance[None] * shares / jnp.sum(shares, axis=0, keepdims=True)
    hot, high, low = call(
        route_kernel,
        [((4 * tokens, tokens), BF16)] + [((tokens, 4 * tokens), BF16)] * 2,
        jnp.concatenate([ids.T.astype(F32), shares], axis=0),
    )
    gathered, own_skip, hot, high, low = lax.optimization_barrier(
        (gathered, own_skip, hot, high, low)
    )
    pairs, prefix = call(
        compose_kernel, [((n_z, W, W), BF16), ((2 * W, W), F32)], pos, gathered, scalars=1
    )
    pairs, weights[1] = lax.optimization_barrier((pairs, weights[1]))
    weights.append(lax.ppermute(weights[-1], TP, ring))
    gathered = exchange(pairs, "z")
    keep, send = call(
        readout_kernel,
        [((n_y, tokens, W), BF16), ((n_y, tokens, W), BF16)],
        pos,
        gathered,
        prefix,
        state_map,
        local,
        head_gain[None],
        blender,
        scalars=1,
    )
    branch = (keep.astype(F32) + swap_cores(send).astype(F32)).astype(BF16)
    branch, weights[2] = lax.optimization_barrier((branch, weights[2]))
    parts = exchange(branch, "y")
    parts, weights[2] = lax.optimization_barrier((parts, weights[2]))
    weights.append(lax.ppermute(weights[-1], TP, ring))
    hidden, outgoing = call(
        dispatch_kernel,
        [((tokens, W), F32), ((n_z * n_x, 64, W), BF16)],
        pos,
        parts,
        own_skip,
        norm_gain[None],
        hot,
        scalars=1,
    )
    own = exchange(outgoing.reshape(n_z * n_x * n_y, 8, W), ("z", "x", "y"))
    own = own.reshape(n_z * n_x, n_y, 8, W)
    keep, send = call(
        expert_kernel,
        [((n_z * n_x, n_y, 8, W), BF16), ((n_z * n_x, n_y, 8, W), BF16)],
        pos,
        own,
        swap_cores(own),
        norm_gain[None],
        *weights,
        scalars=1,
    )
    summed = (keep.astype(F32) + swap_cores(send).astype(F32)).astype(BF16)
    returned = exchange(summed.reshape(n_z * n_x * n_y, 8, W), ("z", "x", "y"))
    returned = returned.reshape(n_z * n_x, n_y, 8, W)
    copies = call(combine_kernel, [((n_y, tokens, W), BF16)], returned, hidden, high, low)
    own = exchange(copies, "y")
    other = swap_cores(own)
    half = output_call(own_out_kernel, (tokens, width), pos, own)
    return output_call(other_out_kernel, (tokens, width), pos, other, half)


def solution(mesh):
    split = Mesh(mesh.devices.reshape(8, 4, 8, 2), ("z", "x", "y", "c"))
    in_specs = (
        P(SP, TP),
        P(SP, TP),
        P(SP, TP),
        P(SP, TP),
        P(SP, TP),
        P(SP, TP),
        P(TP),
        P(SP, None),
        P(TP, None),
        P(),
        P(SP),
        P(SP, None),
        P(SP, None),
        P(SP, None, TP),
        P(SP, None, TP),
        P(SP, TP, None),
    )
    out_specs = P(SP, None)

    return jax.shard_map(body, mesh=split, in_specs=in_specs, out_specs=out_specs, check_vma=False)
```

```python
import jax
import jax.numpy as jnp
from jax import lax
from jax.experimental import pallas as pl
from jax.experimental.pallas import tpu as pltpu
from jax.sharding import Mesh
from jax.sharding import PartitionSpec as P


SP = ("z", "x")
TP = ("y", "c")
F32 = jnp.float32
BF16 = jnp.bfloat16
SEG = 64
W = 128
DECAY = 0.6065306597126334
INTERPRET = False


def dot(a, b, contract=((1,), (0,))):
    return lax.dot_general(a, b, (contract, ((), ())), preferred_element_type=F32)


def halves(a):
    high = a.astype(BF16)
    return high, (a - high.astype(F32)).astype(BF16)


def mm(a, b, contract=((1,), (0,))):
    (a_high, a_low), (b_high, b_low) = halves(a), halves(b)
    return dot(a_high, b_high, contract) + (
        dot(a_high, b_low, contract) + dot(a_low, b_high, contract)
    )


def mm_exact(a, b, contract=((1,), (0,))):
    high, low = halves(a)
    return dot(high, b, contract) + dot(low, b, contract)


def iota(shape, dim):
    return lax.broadcasted_iota(jnp.int32, shape, dim)


def stack_heads(rows):
    first = iota(rows.shape, 1) < SEG
    zero = jnp.zeros_like(rows)
    return jnp.concatenate([jnp.where(first, rows, zero), jnp.where(first, zero, rows)], axis=0)


def flat_heads(stacked):
    half = stacked.shape[0] // 2
    return stacked[:half] + stacked[half:]


def eye128():
    return (iota((W, W), 0) == iota((W, W), 1)).astype(F32)


def same_head_ones():
    return (iota((W, W), 0) // SEG == iota((W, W), 1) // SEG).astype(F32).astype(BF16)


def pack_kernel(switch_ref, expansion_ref, contraction_ref, out_ref, sems):
    depth = switch_ref.shape[1]
    copies = [
        pltpu.make_async_copy(switch_ref.at[0], out_ref.at[pl.ds(0, depth)], sems.at[0]),
        pltpu.make_async_copy(expansion_ref.at[0], out_ref.at[pl.ds(depth, depth)], sems.at[1]),
    ]
    for n in range(depth // W):
        copies.append(
            pltpu.make_async_copy(
                contraction_ref.at[0, :, pl.ds(n * W, W)],
                out_ref.at[pl.ds(2 * depth + n * W, W)],
                sems.at[2 + n],
            )
        )
    for copy in copies:
        copy.start()
    for copy in copies:
        copy.wait()


def columns_of(rows):
    spare = jnp.zeros((6, rows.shape[1]), rows.dtype)
    return jnp.concatenate([rows, spare], axis=0).T


def mixer_kernel(*refs):
    pair_ref, map_ref, loc_ref = refs[6:9]
    held, sems = refs[9:15], refs[15]
    copies = [
        pltpu.make_async_copy(refs[n], held[n], sems.at[n]) for n in range(len(held))
    ]
    for copy in copies:
        copy.start()
    for copy in copies:
        copy.wait()
    q_ref, k_ref, v_ref, s_ref, f_ref, b_ref = held
    bias_columns = columns_of(b_ref[...])
    rows = q_ref.shape[0]
    chunks = rows // SEG
    query = q_ref[...].astype(F32)
    key = k_ref[...].astype(F32)
    value = v_ref[...].astype(F32)
    rate = 1.0 / (1.0 + jnp.exp(-s_ref[...].astype(F32)))
    bias = jnp.where(iota((rows, W), 1) < SEG, bias_columns[:, 0:1], bias_columns[:, 1:2])
    decay = bias - DECAY / (1.0 + jnp.exp(-f_ref[...]))
    removal = key * lax.rsqrt(mm_exact(key * key, same_head_ones()) + 1e-06)
    beta = removal * rate
    row, col = iota((rows, rows), 0), iota((rows, rows), 1)
    below = ((row // SEG == col // SEG) & (row >= col)).astype(F32).astype(BF16)
    high, low = halves(decay)
    rest = (decay - high.astype(F32) - low.astype(F32)).astype(BF16)
    total = dot(below, high) + (dot(below, low) + dot(below, rest))

    row, col = iota((W, W), 0), iota((W, W), 1)
    same = row // SEG == col // SEG
    strict = same & (row > col)
    inclusive = same & (row >= col)
    eye = eye128()

    part = []
    for n in range(chunks):
        at = slice(n * SEG, (n + 1) * SEG)
        cum = total[at]
        before = cum - decay[at]
        middle = cum[SEG // 2 - 1 : SEG // 2]
        closing = cum[SEG - 1 : SEG]
        up = jnp.exp(cum - middle)
        down = jnp.exp(middle - cum)
        left = jnp.exp(before - middle)
        opening = jnp.exp(middle)
        ending = jnp.exp(closing - middle)
        alpha = -removal[at] * left
        asked = query[at] * up
        beta_hat = beta[at] * down
        key_hat = key[at] * down
        scores = mm(
            jnp.concatenate([stack_heads(alpha), stack_heads(asked)], axis=0),
            jnp.concatenate([stack_heads(beta_hat), stack_heads(key_hat)], axis=0),
            ((1,), (1,)),
        )
        remove_remove = jnp.where(strict, scores[:W, :W], 0.0)
        remove_write = jnp.where(strict, scores[:W, W:], 0.0)
        read_remove = jnp.where(inclusive, scores[W:, :W], 0.0)
        read_write = jnp.where(inclusive, scores[W:, W:], 0.0)
        part.append(
            dict(
                near=remove_remove,
                write=remove_write,
                read=jnp.concatenate([read_remove, read_write], axis=1),
                read_remove=read_remove,
                alpha=stack_heads(alpha * opening),
                asked=stack_heads(asked * opening),
                value=stack_heads(value[at]),
                bar=jnp.concatenate(
                    [stack_heads(beta_hat * ending), stack_heads(key_hat * ending)], axis=0
                ),
                closing=jnp.exp(closing),
            )
        )
    inverse = [eye + jnp.where(row // 2 == col // 2, p["near"], 0.0) for p in part]
    for level in (4, 8, 16, 32, 64):
        joint = (row // level == col // level) & (row // (level // 2) != col // (level // 2))
        step = [mm(jnp.where(joint, p["near"], 0.0), x) for p, x in zip(part, inverse)]
        inverse = [x + mm(x, s) for x, s in zip(inverse, step)]
    wrote = [mm(p["write"], p["value"]) for p in part]
    solved = [
        mm(x, jnp.concatenate([p["alpha"], w], axis=1)) for x, p, w in zip(inverse, part, wrote)
    ]
    keeps, adds, reads, locals_ = [], [], [], []
    for p, s in zip(part, solved):
        absorb, carried = s[:, :W], s[:, W:]
        keeps.append(mm(absorb, p["bar"][:W], ((0,), (0,))) + eye * p["closing"])
        adds.append(
            mm(jnp.concatenate([carried, p["value"]], axis=0), p["bar"], ((0,), (0,)))
        )
        locals_.append(
            flat_heads(mm(p["read"], jnp.concatenate([carried, p["value"]], axis=0)))
        )
        reads.append(flat_heads(p["asked"] + mm(p["read_remove"], absorb)))
    map_ref[:SEG, :] = reads[0]
    loc_ref[:SEG, :] = locals_[0]
    run = jnp.concatenate([keeps[0], adds[0]], axis=0)
    for n in range(1, chunks):
        at = slice(n * SEG, (n + 1) * SEG)
        both = mm(reads[n], run, ((1,), (1,)))
        map_ref[at, :] = both[:, :W]
        loc_ref[at, :] = locals_[n] + both[:, W:]
        run = mm(run, keeps[n])
        run = jnp.concatenate([run[:W], run[W:] + adds[n]], axis=0)
    pair = jnp.concatenate([flat_heads(run[:W] - eye), flat_heads(run[W:])], axis=0).astype(BF16)
    for n in range(pair_ref.shape[0]):
        pair_ref[n] = pair


def unpack(pair):
    pair = pair.astype(F32)
    return stack_heads(pair[:SEG]), stack_heads(pair[SEG:])


def times(state, change):
    return state + mm_exact(state, change.astype(BF16))


def compose_kernel(pos_ref, got_ref, pair_ref, prefix_ref):
    mine = pos_ref[0]
    eye = eye128()
    change, add = unpack(got_ref[0])
    run = jnp.concatenate([eye + change, add], axis=0)
    prefix = jnp.where(mine > 0, run, jnp.concatenate([eye, jnp.zeros((W, W), F32)], axis=0))
    for n in range(1, got_ref.shape[0]):
        change, add = unpack(got_ref[n])
        run = times(run, change)
        run = jnp.concatenate([run[:W], run[W:] + add], axis=0)
        prefix = jnp.where(n < mine, run, prefix)
    pair = jnp.concatenate([flat_heads(run[:W] - eye), flat_heads(run[W:])], axis=0).astype(BF16)
    for n in range(pair_ref.shape[0]):
        pair_ref[n] = pair
    prefix_ref[...] = prefix


def readout_kernel(pos_ref, got_ref, prefix_ref, map_ref, loc_ref, gain_ref, w_ref, keep_ref, send_ref):
    mine, core = pos_ref[1], pos_ref[3]
    state = jnp.where(mine > 0, unpack(got_ref[0])[1], 0.0)
    for n in range(1, got_ref.shape[0] - 1):
        change, add = unpack(got_ref[n])
        state = jnp.where(n < mine, times(state, change) + add, state)
    state = mm(state, prefix_ref[:W]) + prefix_ref[W:]
    out = loc_ref[...] + mm(map_ref[...], state, ((1,), (1,)))
    ones = same_head_ones()
    centered = out - mm_exact(out, ones) * (1.0 / SEG)
    spread = mm_exact(centered * centered, ones) * (1.0 / SEG)
    mixed = (centered * lax.rsqrt(spread + 0.00064) * gain_ref[...]).astype(BF16)
    for n in range(keep_ref.shape[0]):
        part = jnp.dot(mixed, w_ref[:, n * 2 * W : (n + 1) * 2 * W], preferred_element_type=F32)
        first, second = part[:, :W], part[:, W:]
        keep_ref[n] = jnp.where(core == 0, first, second).astype(BF16)
        send_ref[n] = jnp.where(core == 0, second, first).astype(BF16)


def route_kernel(names_ref, hot_ref, slots_ref):
    experts, capacity = 32, 32
    tokens, places = names_ref.shape[1], hot_ref.shape[0]
    names = [names_ref[k : k + 1, :] for k in range(2)]
    hot = [(iota((experts, tokens), 0) == name).astype(F32) for name in names]
    earlier = (iota((tokens, tokens), 0) < iota((tokens, tokens), 1)).astype(F32).astype(BF16)
    ahead = dot((hot[0] + hot[1]).astype(BF16), earlier)
    ranks = [
        jnp.sum(hot[0] * ahead, axis=0, keepdims=True),
        jnp.sum(hot[1] * (ahead + hot[0]), axis=0, keepdims=True),
    ]
    slots = [(name * capacity).astype(F32) + rank for name, rank in zip(names, ranks)]
    place = iota((places, tokens), 0).astype(F32)
    hot_ref[...] = ((place == slots[0]) | (place == slots[1])).astype(F32).astype(BF16)
    slots_ref[...] = jnp.concatenate(slots, axis=0)


def weigh_kernel(slots_ref, chance_ref, within_ref, high_ref, low_ref):
    tokens, places = high_ref.shape
    within = within_ref[...]
    shares = columns_of(chance_ref[...] * within / jnp.sum(within, axis=0, keepdims=True))
    found = columns_of(slots_ref[...])
    place = iota((tokens, places), 1).astype(F32)
    weight = jnp.zeros((tokens, places), F32)
    for k in range(2):
        weight = weight + jnp.where(place == found[:, k : k + 1], shares[:, k : k + 1], 0.0)
    high_ref[...], low_ref[...] = halves(weight)


def dispatch_kernel(pos_ref, parts_ref, skip_ref, gain_ref, hot_ref, hid_ref, out_ref):
    column = pl.multiple_of((pos_ref[2] * 2 + pos_ref[3]) * W, W)
    hidden = skip_ref[...].astype(F32)
    for n in range(parts_ref.shape[0]):
        hidden = hidden + parts_ref[n].astype(F32)
    hid_ref[...] = hidden
    scaled = (hidden * gain_ref[:, pl.ds(column, W)]).astype(BF16)
    rows = dot(hot_ref[...], scaled).astype(BF16).reshape(32, 32, W)
    out_ref[:, :32, :] = rows
    out_ref[:, 32:, :] = rows


def expert_kernel(pos_ref, own_ref, other_ref, gain_ref, w0, w1, w2, w3, keep_ref, send_ref):
    core = pos_ref[3]
    sources, ways, lines, _ = own_ref.shape
    rows, width = sources * lines, gain_ref.shape[1]
    blocks = []
    for n in range(ways):
        own = own_ref[:, n].astype(F32).reshape(rows, W)
        other = other_ref[:, n].astype(F32).reshape(rows, W)
        blocks.append(jnp.where(core == 0, own, other))
        blocks.append(jnp.where(core == 0, other, own))
    data = jnp.concatenate([block.astype(BF16) for block in blocks], axis=1)
    squares = jnp.zeros((rows, W), F32)
    for n, block in enumerate(blocks):
        plain = block * (1.0 / gain_ref[:, n * W : (n + 1) * W])
        squares = squares + plain * plain
    scale = lax.rsqrt(jnp.sum(squares, axis=1, keepdims=True) * (1.0 / width) + 1e-06)
    hidden = []
    for w_ref in (w0, w1, w2, w3):
        both = jnp.concatenate([w_ref[:width], w_ref[width : 2 * width]], axis=1)
        act = jnp.dot(data, both, preferred_element_type=F32) * scale
        gate, up = act[:, :W], act[:, W:]
        hidden.append((gate / (1.0 + jnp.exp(-gate)) * up).astype(BF16))
    hidden = jnp.concatenate(hidden, axis=1)
    for n in range(ways):
        at = 2 * width + 2 * n * W
        pieces = [
            jnp.concatenate([w_ref[at : at + W], w_ref[at + W : at + 2 * W]], axis=1)
            for w_ref in (w0, w1, w2, w3)
        ]
        part = jnp.dot(hidden, jnp.concatenate(pieces, axis=0), preferred_element_type=F32)
        first, second = part[:, :W], part[:, W:]
        keep = jnp.where(core == 0, first, second).reshape(sources, lines, W)
        send = jnp.where(core == 0, second, first).reshape(sources, lines, W)
        keep_ref[:, n] = keep.astype(BF16)
        send_ref[:, n] = send.astype(BF16)


def combine_kernel(ret_ref, hid_ref, high_ref, low_ref, out_ref):
    half = ret_ref.shape[1] // 2
    rows = ret_ref[:, :half].astype(F32) + ret_ref[:, half:].astype(F32)
    rows = rows.reshape(-1, W).astype(BF16)
    result = hid_ref[...] + (dot(high_ref[...], rows) + dot(low_ref[...], rows))
    result = result.astype(BF16)
    for n in range(out_ref.shape[0]):
        out_ref[n] = result


def columns_out(first, blocks_ref, out_ref, sems):
    copies = []
    for n in range(blocks_ref.shape[0]):
        column = pl.multiple_of((2 * n + first) * W, W)
        copies.append(
            pltpu.make_async_copy(blocks_ref.at[n], out_ref.at[:, pl.ds(column, W)], sems.at[n])
        )
    for copy in copies:
        copy.start()
    for copy in copies:
        copy.wait()


def own_out_kernel(pos_ref, own_ref, out_ref, sems):
    columns_out(pos_ref[3], own_ref, out_ref, sems)


def other_out_kernel(pos_ref, other_ref, half_ref, out_ref, sems):
    columns_out(1 - pos_ref[3], other_ref, out_ref, sems)


def output_call(kernel, shape, pos, blocks, *half):
    near = [pl.BlockSpec(memory_space=pltpu.SMEM), pl.BlockSpec(memory_space=pltpu.VMEM)]
    return pl.pallas_call(
        kernel,
        out_shape=jax.ShapeDtypeStruct(shape, BF16),
        in_specs=near + [pl.BlockSpec(memory_space=pl.ANY)] * len(half),
        out_specs=pl.BlockSpec(memory_space=pl.ANY),
        scratch_shapes=[pltpu.SemaphoreType.DMA((blocks.shape[0],))],
        input_output_aliases={2: 0} if half else {},
        compiler_params=pltpu.CompilerParams(vmem_limit_bytes=8 << 20),
        cost_estimate=pl.CostEstimate(
            flops=1_000_000_000, bytes_accessed=1_000_000, transcendentals=0
        ),
        interpret=INTERPRET,
    )(pos, blocks, *half)


def call(kernel, outs, *args, scalars=0, flops=2_000_000_000, far=(), scratch=(), grant=40 << 20):
    specs = [
        pl.BlockSpec(
            memory_space=pltpu.SMEM if n < scalars else pltpu.HBM if n in far else pltpu.VMEM
        )
        for n in range(len(args))
    ]
    shapes = [jax.ShapeDtypeStruct(shape, kind) for shape, kind in outs]
    result = pl.pallas_call(
        kernel,
        out_shape=shapes if len(shapes) > 1 else shapes[0],
        in_specs=specs,
        scratch_shapes=list(scratch),
        out_specs=[pl.BlockSpec(memory_space=pltpu.VMEM)] * len(shapes)
        if len(shapes) > 1
        else pl.BlockSpec(memory_space=pltpu.VMEM),
        compiler_params=pltpu.CompilerParams(vmem_limit_bytes=grant),
        cost_estimate=pl.CostEstimate(flops=flops, bytes_accessed=1_000_000, transcendentals=0),
        interpret=INTERPRET,
    )(*args)
    return result


def exchange(parts, axes):
    return lax.all_to_all(parts, axes, split_axis=0, concat_axis=0, tiled=True)


def swap_cores(data):
    return lax.ppermute(data, "c", [(0, 1), (1, 0)])


def body(
    queries,
    keys,
    values,
    step_sizes,
    forgetting,
    forgetting_bias,
    head_gain,
    skip,
    blender,
    norm_gain,
    cluster_chance,
    within_chance,
    ids,
    switch,
    expansion,
    contraction,
):
    n_z, n_x, n_y = (lax.axis_size(a) for a in ("z", "x", "y"))
    here = [lax.axis_index(a) for a in ("x", "z", "y", "c")]
    pos = jnp.stack(here).astype(jnp.int32)
    tokens, width = skip.shape

    ring = [(((y + 1) % n_y) * 2, y * 2) for y in range(n_y)]
    ring += [(((y - 1) % n_y) * 2 + 1, y * 2 + 1) for y in range(n_y)]
    back = [(target, source) for source, target in ring]
    weights = [
        call(
            pack_kernel,
            [((3 * width, W), BF16)],
            switch,
            expansion,
            contraction,
            far=(0, 1, 2),
            scratch=[pltpu.SemaphoreType.DMA((2 + width // W,))],
            grant=67043328,
        )
    ]
    weights.append(lax.ppermute(weights[-1], TP, ring))
    pairs, state_map, local = call(
        mixer_kernel,
        [((n_x, W, W), BF16), ((tokens, W), F32), ((tokens, W), F32)],
        queries,
        keys,
        values,
        step_sizes,
        forgetting,
        forgetting_bias.T,
        far=range(6),
        scratch=[pltpu.VMEM((tokens, W), BF16)] * 4
        + [
            pltpu.VMEM((tokens, W), F32),
            pltpu.VMEM((2, tokens), F32),
            pltpu.SemaphoreType.DMA((6,)),
        ],
        grant=67043328,
    )
    gathered = exchange(pairs, "x")
    weights.append(lax.ppermute(weights[0], TP, back))
    hot, slots = call(route_kernel, [((4 * tokens, tokens), BF16), ((2, tokens), F32)], ids.T)
    gathered, hot = lax.optimization_barrier((gathered, hot))
    pairs, prefix = call(
        compose_kernel, [((n_z, W, W), BF16), ((2 * W, W), F32)], pos, gathered, scalars=1
    )
    gathered = exchange(pairs, "z")
    keep, send = call(
        readout_kernel,
        [((n_y, tokens, W), BF16), ((n_y, tokens, W), BF16)],
        pos,
        gathered,
        prefix,
        state_map,
        local,
        head_gain[None],
        blender,
        scalars=1,
    )
    own_skip = lax.dynamic_slice_in_dim(skip, (here[2] * 2 + here[3]) * W, W, 1)
    send, own_skip = lax.optimization_barrier((swap_cores(send), own_skip))
    branch = (keep.astype(F32) + send.astype(F32)).astype(BF16)
    branch, weights[1], weights[2] = lax.optimization_barrier((branch, weights[1], weights[2]))
    parts = exchange(branch, "y")
    parts, weights[1] = lax.optimization_barrier((parts, weights[1]))
    weights.append(lax.ppermute(weights[1], TP, ring))
    hidden, outgoing = call(
        dispatch_kernel,
        [((tokens, W), F32), ((n_z * n_x, 64, W), BF16)],
        pos,
        parts,
        own_skip,
        norm_gain[None],
        hot,
        scalars=1,
    )
    own = exchange(outgoing.reshape(n_z * n_x * n_y, 8, W), ("z", "x", "y"))
    own = own.reshape(n_z * n_x, n_y, 8, W)
    keep, send = call(
        expert_kernel,
        [((n_z * n_x, n_y, 8, W), BF16), ((n_z * n_x, n_y, 8, W), BF16)],
        pos,
        own,
        swap_cores(own),
        norm_gain[None],
        *weights,
        scalars=1,
    )
    high, low = call(
        weigh_kernel,
        [((tokens, 4 * tokens), BF16)] * 2,
        slots,
        cluster_chance[None],
        within_chance.T,
    )
    send, high, low = lax.optimization_barrier((swap_cores(send), high, low))
    summed = (keep.astype(F32) + send.astype(F32)).astype(BF16)
    returned = exchange(summed.reshape(n_z * n_x * n_y, 8, W), ("z", "x", "y"))
    returned = returned.reshape(n_z * n_x, n_y, 8, W)
    copies = call(combine_kernel, [((n_y, tokens, W), BF16)], returned, hidden, high, low)
    own = exchange(copies, "y")
    other = swap_cores(own)
    half = output_call(own_out_kernel, (tokens, width), pos, own)
    return output_call(other_out_kernel, (tokens, width), pos, other, half)


def solution(mesh):
    split = Mesh(mesh.devices.reshape(8, 4, 8, 2), ("z", "x", "y", "c"))
    in_specs = (
        P(SP, TP),
        P(SP, TP),
        P(SP, TP),
        P(SP, TP),
        P(SP, TP),
        P(SP, TP),
        P(TP),
        P(SP, None),
        P(TP, None),
        P(),
        P(SP),
        P(SP, None),
        P(SP, None),
        P(SP, None, TP),
        P(SP, None, TP),
        P(SP, TP, None),
    )
    out_specs = P(SP, None)

    return jax.shard_map(body, mesh=split, in_specs=in_specs, out_specs=out_specs, check_vma=False)
```

```python
import jax
import jax.numpy as jnp
from jax import lax
from jax.experimental import pallas as pl
from jax.experimental.pallas import tpu as pltpu
from jax.sharding import Mesh
from jax.sharding import PartitionSpec as P


SP = ("z", "x")
TP = ("y", "c")
F32 = jnp.float32
BF16 = jnp.bfloat16
SEG = 64
W = 128
DECAY = 0.6065306597126334
INTERPRET = False


def dot(a, b, contract=((1,), (0,))):
    return lax.dot_general(a, b, (contract, ((), ())), preferred_element_type=F32)


def halves(a):
    high = a.astype(BF16)
    return high, (a - high.astype(F32)).astype(BF16)


def mm(a, b, contract=((1,), (0,))):
    (a_high, a_low), (b_high, b_low) = halves(a), halves(b)
    return dot(a_high, b_high, contract) + (
        dot(a_high, b_low, contract) + dot(a_low, b_high, contract)
    )


def mm_exact(a, b, contract=((1,), (0,))):
    high, low = halves(a)
    return dot(high, b, contract) + dot(low, b, contract)


def iota(shape, dim):
    return lax.broadcasted_iota(jnp.int32, shape, dim)


def stack_heads(rows):
    first = iota(rows.shape, 1) < SEG
    zero = jnp.zeros_like(rows)
    return jnp.concatenate([jnp.where(first, rows, zero), jnp.where(first, zero, rows)], axis=0)


def flat_heads(stacked):
    half = stacked.shape[0] // 2
    return stacked[:half] + stacked[half:]


def eye128():
    return (iota((W, W), 0) == iota((W, W), 1)).astype(F32)


def same_head_ones():
    return (iota((W, W), 0) // SEG == iota((W, W), 1) // SEG).astype(F32).astype(BF16)


def pack_kernel(switch_ref, expansion_ref, contraction_ref, out_ref, sems):
    depth = switch_ref.shape[1]
    copies = [
        pltpu.make_async_copy(switch_ref.at[0], out_ref.at[pl.ds(0, depth)], sems.at[0]),
        pltpu.make_async_copy(expansion_ref.at[0], out_ref.at[pl.ds(depth, depth)], sems.at[1]),
    ]
    for n in range(depth // W):
        copies.append(
            pltpu.make_async_copy(
                contraction_ref.at[0, :, pl.ds(n * W, W)],
                out_ref.at[pl.ds(2 * depth + n * W, W)],
                sems.at[2 + n],
            )
        )
    for copy in copies:
        copy.start()
    for copy in copies:
        copy.wait()


def columns_of(rows):
    spare = jnp.zeros((6, rows.shape[1]), rows.dtype)
    return jnp.concatenate([rows, spare], axis=0).T


def mixer_kernel(*refs):
    pair_ref, map_ref, loc_ref = refs[6:9]
    held, sems = refs[9:15], refs[15]
    copies = [
        pltpu.make_async_copy(refs[n], held[n], sems.at[n]) for n in range(len(held))
    ]
    for copy in copies:
        copy.start()
    for copy in copies:
        copy.wait()
    q_ref, k_ref, v_ref, s_ref, f_ref, b_ref = held
    bias_columns = columns_of(b_ref[...])
    rows = q_ref.shape[0]
    chunks = rows // SEG
    query = q_ref[...].astype(F32)
    key = k_ref[...].astype(F32)
    value = v_ref[...].astype(F32)
    rate = 1.0 / (1.0 + jnp.exp(-s_ref[...].astype(F32)))
    bias = jnp.where(iota((rows, W), 1) < SEG, bias_columns[:, 0:1], bias_columns[:, 1:2])
    decay = bias - DECAY / (1.0 + jnp.exp(-f_ref[...]))
    removal = key * lax.rsqrt(mm_exact(key * key, same_head_ones()) + 1e-06)
    beta = removal * rate
    row, col = iota((rows, rows), 0), iota((rows, rows), 1)
    below = ((row // SEG == col // SEG) & (row >= col)).astype(F32).astype(BF16)
    high, low = halves(decay)
    rest = (decay - high.astype(F32) - low.astype(F32)).astype(BF16)
    total = dot(below, high) + (dot(below, low) + dot(below, rest))

    row, col = iota((W, W), 0), iota((W, W), 1)
    same = row // SEG == col // SEG
    strict = same & (row > col)
    inclusive = same & (row >= col)
    eye = eye128()

    part = []
    for n in range(chunks):
        at = slice(n * SEG, (n + 1) * SEG)
        cum = total[at]
        before = cum - decay[at]
        middle = cum[SEG // 2 - 1 : SEG // 2]
        closing = cum[SEG - 1 : SEG]
        up = jnp.exp(cum - middle)
        down = jnp.exp(middle - cum)
        left = jnp.exp(before - middle)
        opening = jnp.exp(middle)
        ending = jnp.exp(closing - middle)
        alpha = -removal[at] * left
        asked = query[at] * up
        beta_hat = beta[at] * down
        key_hat = key[at] * down
        scores = mm(
            jnp.concatenate([stack_heads(alpha), stack_heads(asked)], axis=0),
            jnp.concatenate([stack_heads(beta_hat), stack_heads(key_hat)], axis=0),
            ((1,), (1,)),
        )
        remove_remove = jnp.where(strict, scores[:W, :W], 0.0)
        remove_write = jnp.where(strict, scores[:W, W:], 0.0)
        read_remove = jnp.where(inclusive, scores[W:, :W], 0.0)
        read_write = jnp.where(inclusive, scores[W:, W:], 0.0)
        part.append(
            dict(
                near=remove_remove,
                write=remove_write,
                read=jnp.concatenate([read_remove, read_write], axis=1),
                read_remove=read_remove,
                alpha=stack_heads(alpha * opening),
                asked=stack_heads(asked * opening),
                value=stack_heads(value[at]),
                bar=jnp.concatenate(
                    [stack_heads(beta_hat * ending), stack_heads(key_hat * ending)], axis=0
                ),
                closing=jnp.exp(closing),
            )
        )
    inverse = [eye + jnp.where(row // 2 == col // 2, p["near"], 0.0) for p in part]
    for level in (4, 8, 16, 32, 64):
        joint = (row // level == col // level) & (row // (level // 2) != col // (level // 2))
        step = [mm(jnp.where(joint, p["near"], 0.0), x) for p, x in zip(part, inverse)]
        inverse = [x + mm(x, s) for x, s in zip(inverse, step)]
    wrote = [mm(p["write"], p["value"]) for p in part]
    solved = [
        mm(x, jnp.concatenate([p["alpha"], w], axis=1)) for x, p, w in zip(inverse, part, wrote)
    ]
    keeps, adds, reads, locals_ = [], [], [], []
    for p, s in zip(part, solved):
        absorb, carried = s[:, :W], s[:, W:]
        keeps.append(mm(absorb, p["bar"][:W], ((0,), (0,))) + eye * p["closing"])
        adds.append(
            mm(jnp.concatenate([carried, p["value"]], axis=0), p["bar"], ((0,), (0,)))
        )
        locals_.append(
            flat_heads(mm(p["read"], jnp.concatenate([carried, p["value"]], axis=0)))
        )
        reads.append(flat_heads(p["asked"] + mm(p["read_remove"], absorb)))
    map_ref[:SEG, :] = reads[0]
    loc_ref[:SEG, :] = locals_[0]
    run = jnp.concatenate([keeps[0], adds[0]], axis=0)
    for n in range(1, chunks):
        at = slice(n * SEG, (n + 1) * SEG)
        both = mm(reads[n], run, ((1,), (1,)))
        map_ref[at, :] = both[:, :W]
        loc_ref[at, :] = locals_[n] + both[:, W:]
        run = mm(run, keeps[n])
        run = jnp.concatenate([run[:W], run[W:] + adds[n]], axis=0)
    pair = jnp.concatenate([flat_heads(run[:W] - eye), flat_heads(run[W:])], axis=0).astype(BF16)
    for n in range(pair_ref.shape[0]):
        pair_ref[n] = pair


def unpack(pair):
    pair = pair.astype(F32)
    return stack_heads(pair[:SEG]), stack_heads(pair[SEG:])


def times(state, change):
    return state + mm_exact(state, change.astype(BF16))


def compose_kernel(pos_ref, got_ref, pair_ref, prefix_ref):
    mine = pos_ref[0]
    eye = eye128()
    change, add = unpack(got_ref[0])
    run = jnp.concatenate([eye + change, add], axis=0)
    prefix = jnp.where(mine > 0, run, jnp.concatenate([eye, jnp.zeros((W, W), F32)], axis=0))
    for n in range(1, got_ref.shape[0]):
        change, add = unpack(got_ref[n])
        run = times(run, change)
        run = jnp.concatenate([run[:W], run[W:] + add], axis=0)
        prefix = jnp.where(n < mine, run, prefix)
    pair = jnp.concatenate([flat_heads(run[:W] - eye), flat_heads(run[W:])], axis=0).astype(BF16)
    for n in range(pair_ref.shape[0]):
        pair_ref[n] = pair
    prefix_ref[...] = prefix


def readout_kernel(pos_ref, got_ref, prefix_ref, map_ref, loc_ref, gain_ref, w_ref, send_ref, mixed_ref):
    mine, core = pos_ref[1], pos_ref[3]
    state = jnp.where(mine > 0, unpack(got_ref[0])[1], 0.0)
    for n in range(1, got_ref.shape[0] - 1):
        change, add = unpack(got_ref[n])
        state = jnp.where(n < mine, times(state, change) + add, state)
    state = mm(state, prefix_ref[:W]) + prefix_ref[W:]
    out = loc_ref[...] + mm(map_ref[...], state, ((1,), (1,)))
    ones = same_head_ones()
    centered = out - mm_exact(out, ones) * (1.0 / SEG)
    spread = mm_exact(centered * centered, ones) * (1.0 / SEG)
    mixed = (centered * lax.rsqrt(spread + 0.00064) * gain_ref[...]).astype(BF16)
    mixed_ref[...] = mixed
    branch_columns(1 - core, mixed, w_ref, send_ref)


def branch_columns(core, mixed, w_ref, out_ref):
    for n in range(0, out_ref.shape[0], 2):
        sides = [w_ref[:, pl.ds(pl.multiple_of((2 * m + core) * W, W), W)] for m in (n, n + 1)]
        part = dot(mixed, jnp.concatenate(sides, axis=1)).astype(BF16)
        out_ref[n] = part[:, :W]
        out_ref[n + 1] = part[:, W:]


def branch_keep_kernel(pos_ref, mixed_ref, w_ref, keep_ref):
    branch_columns(pos_ref[3], mixed_ref[...], w_ref, keep_ref)


def route_kernel(names_ref, hot_ref, slots_ref):
    experts = 32
    tokens, places = names_ref.shape[1], hot_ref.shape[0]
    names = [names_ref[k : k + 1, :] for k in range(2)]
    hot = [(iota((experts, tokens), 0) == name).astype(F32) for name in names]
    earlier = (iota((tokens, tokens), 0) < iota((tokens, tokens), 1)).astype(F32).astype(BF16)
    ahead = dot((hot[0] + hot[1]).astype(BF16), earlier)
    ranks = [
        jnp.sum(hot[0] * ahead, axis=0, keepdims=True),
        jnp.sum(hot[1] * (ahead + hot[0]), axis=0, keepdims=True),
    ]
    ranks = [rank.astype(jnp.int32) for rank in ranks]
    slots = [
        ((name >> 2) << 7) + ((rank >> 3) << 5) + ((name & 3) << 3) + (rank & 7)
        for name, rank in zip(names, ranks)
    ]
    slots = [slot.astype(F32) for slot in slots]
    place = iota((places, tokens), 0).astype(F32)
    hot_ref[...] = ((place == slots[0]) | (place == slots[1])).astype(F32).astype(BF16)
    slots_ref[...] = jnp.concatenate(slots, axis=0)


def weigh_kernel(slots_ref, chance_ref, within_ref, high_ref, low_ref):
    tokens, places = high_ref.shape
    within = within_ref[...]
    shares = columns_of(chance_ref[...] * within / jnp.sum(within, axis=0, keepdims=True))
    found = columns_of(slots_ref[...])
    place = iota((tokens, places), 1).astype(F32)
    weight = jnp.zeros((tokens, places), F32)
    for k in range(2):
        weight = weight + jnp.where(place == found[:, k : k + 1], shares[:, k : k + 1], 0.0)
    high_ref[...], low_ref[...] = halves(weight)


def dispatch_kernel(pos_ref, parts_ref, skip_ref, gain_ref, hot_ref, hid_ref, out_ref):
    column = pl.multiple_of((pos_ref[2] * 2 + pos_ref[3]) * W, W)
    hidden = skip_ref[...].astype(F32)
    for n in range(parts_ref.shape[0]):
        hidden = hidden + parts_ref[n].astype(F32)
    hid_ref[...] = hidden
    scaled = (hidden * gain_ref[:, pl.ds(column, W)]).astype(BF16)
    groups = out_ref.shape[1] // 2
    rows = dot(hot_ref[...], scaled)
    rows = rows.reshape(out_ref.shape[0], groups, *out_ref.shape[2:]).astype(BF16)
    out_ref[:, :groups] = rows
    out_ref[:, groups:] = rows


def block_at(n, core):
    return pl.multiple_of((2 * n + core) * W, W)


def columns_product(core, data_ref, gain_ref, weight_refs):
    ways, width = data_ref.shape[1], gain_ref.shape[1]
    blocks = [data_ref[:, n].astype(F32).reshape(-1, W) for n in range(ways)]
    squares = jnp.zeros(blocks[0].shape, F32)
    for n, block in enumerate(blocks):
        plain = block * (1.0 / gain_ref[:, pl.ds(block_at(n, core), W)])
        squares = squares + plain * plain
    data = jnp.concatenate([block.astype(BF16) for block in blocks], axis=1)
    acts = []
    for w_ref in weight_refs:
        sides = [
            jnp.concatenate(
                [w_ref[pl.ds(at + block_at(n, core), W), :] for n in range(ways)], axis=0
            )
            for at in (0, width)
        ]
        acts.append(dot(data, jnp.concatenate(sides, axis=1)))
    return squares, acts


def down_columns(core, hidden, width, weight_refs, out_ref):
    for n in range(0, out_ref.shape[1], 2):
        sides = [
            jnp.concatenate(
                [w_ref[pl.ds(2 * width + block_at(m, core), W), :] for w_ref in weight_refs], axis=0
            )
            for m in (n, n + 1)
        ]
        part = dot(hidden, jnp.concatenate(sides, axis=1))
        shape = (out_ref.shape[0], *out_ref.shape[2:])
        out_ref[:, n] = part[:, :W].reshape(shape).astype(BF16)
        out_ref[:, n + 1] = part[:, W:].reshape(shape).astype(BF16)


def expert_own_kernel(pos_ref, own_ref, gain_ref, w0, w1, w2, w3, act_ref, square_ref):
    square_ref[...], acts = columns_product(pos_ref[3], own_ref, gain_ref, (w0, w1, w2, w3))
    for n, act in enumerate(acts):
        act_ref[n] = act


def expert_kernel(
    pos_ref, other_ref, gain_ref, act_ref, square_ref, w0, w1, w2, w3, send_ref, hidden_ref
):
    core, width = pos_ref[3], gain_ref.shape[1]
    squares, acts = columns_product(1 - core, other_ref, gain_ref, (w0, w1, w2, w3))
    total = jnp.sum(squares + square_ref[...], axis=1, keepdims=True)
    scale = lax.rsqrt(total * (1.0 / width) + 1e-06)
    hidden = []
    for n, act in enumerate(acts):
        act = (act + act_ref[n]) * scale
        gate, up = act[:, :W], act[:, W:]
        hidden.append((gate / (1.0 + jnp.exp(-gate)) * up).astype(BF16))
    hidden = jnp.concatenate(hidden, axis=1)
    hidden_ref[...] = hidden
    down_columns(1 - core, hidden, width, (w0, w1, w2, w3), send_ref)


def expert_keep_kernel(pos_ref, hidden_ref, w0, w1, w2, w3, keep_ref):
    width = w0.shape[0] // 3
    down_columns(pos_ref[3], hidden_ref[...], width, (w0, w1, w2, w3), keep_ref)


def combine_kernel(ret_ref, hid_ref, high_ref, low_ref, out_ref):
    half = ret_ref.shape[1] // 2
    rows = ret_ref[:, :half].astype(F32) + ret_ref[:, half:].astype(F32)
    rows = rows.reshape(-1, W).astype(BF16)
    result = hid_ref[...] + (dot(high_ref[...], rows) + dot(low_ref[...], rows))
    result = result.astype(BF16)
    for n in range(out_ref.shape[0]):
        out_ref[n] = result


def columns_out(first, blocks_ref, out_ref, sems):
    copies = []
    for n in range(blocks_ref.shape[0]):
        column = pl.multiple_of((2 * n + first) * W, W)
        copies.append(
            pltpu.make_async_copy(blocks_ref.at[n], out_ref.at[:, pl.ds(column, W)], sems.at[n])
        )
    for copy in copies:
        copy.start()
    for copy in copies:
        copy.wait()


def own_out_kernel(pos_ref, own_ref, out_ref, sems):
    columns_out(pos_ref[3], own_ref, out_ref, sems)


def other_out_kernel(pos_ref, other_ref, half_ref, out_ref, sems):
    columns_out(1 - pos_ref[3], other_ref, out_ref, sems)


def output_call(kernel, shape, pos, blocks, *half):
    near = [pl.BlockSpec(memory_space=pltpu.SMEM), pl.BlockSpec(memory_space=pltpu.VMEM)]
    return pl.pallas_call(
        kernel,
        out_shape=jax.ShapeDtypeStruct(shape, BF16),
        in_specs=near + [pl.BlockSpec(memory_space=pl.ANY)] * len(half),
        out_specs=pl.BlockSpec(memory_space=pl.ANY),
        scratch_shapes=[pltpu.SemaphoreType.DMA((blocks.shape[0],))],
        input_output_aliases={2: 0} if half else {},
        compiler_params=pltpu.CompilerParams(vmem_limit_bytes=8 << 20),
        cost_estimate=pl.CostEstimate(
            flops=1_000_000_000, bytes_accessed=1_000_000, transcendentals=0
        ),
        interpret=INTERPRET,
    )(pos, blocks, *half)


def call(kernel, outs, *args, scalars=0, flops=2_000_000_000, far=(), scratch=(), grant=40 << 20):
    specs = [
        pl.BlockSpec(
            memory_space=pltpu.SMEM if n < scalars else pltpu.HBM if n in far else pltpu.VMEM
        )
        for n in range(len(args))
    ]
    shapes = [jax.ShapeDtypeStruct(shape, kind) for shape, kind in outs]
    result = pl.pallas_call(
        kernel,
        out_shape=shapes if len(shapes) > 1 else shapes[0],
        in_specs=specs,
        scratch_shapes=list(scratch),
        out_specs=[pl.BlockSpec(memory_space=pltpu.VMEM)] * len(shapes)
        if len(shapes) > 1
        else pl.BlockSpec(memory_space=pltpu.VMEM),
        compiler_params=pltpu.CompilerParams(vmem_limit_bytes=grant),
        cost_estimate=pl.CostEstimate(flops=flops, bytes_accessed=1_000_000, transcendentals=0),
        interpret=INTERPRET,
    )(*args)
    return result


def exchange(parts, axes):
    return lax.all_to_all(parts, axes, split_axis=0, concat_axis=0, tiled=True)


def swap_cores(data):
    return lax.ppermute(data, "c", [(0, 1), (1, 0)])


def body(
    queries,
    keys,
    values,
    step_sizes,
    forgetting,
    forgetting_bias,
    head_gain,
    skip,
    blender,
    norm_gain,
    cluster_chance,
    within_chance,
    ids,
    switch,
    expansion,
    contraction,
):
    n_z, n_x, n_y = (lax.axis_size(a) for a in ("z", "x", "y"))
    here = [lax.axis_index(a) for a in ("x", "z", "y", "c")]
    pos = jnp.stack(here).astype(jnp.int32)
    tokens, width = skip.shape

    ring = [(((y + 1) % n_y) * 2, y * 2) for y in range(n_y)]
    ring += [(((y - 1) % n_y) * 2 + 1, y * 2 + 1) for y in range(n_y)]
    back = [(target, source) for source, target in ring]
    weights = [
        call(
            pack_kernel,
            [((3 * width, W), BF16)],
            switch,
            expansion,
            contraction,
            far=(0, 1, 2),
            scratch=[pltpu.SemaphoreType.DMA((2 + width // W,))],
            grant=67043328,
        )
    ]
    weights.append(lax.ppermute(weights[-1], TP, ring))
    pairs, state_map, local = call(
        mixer_kernel,
        [((n_x, W, W), BF16), ((tokens, W), F32), ((tokens, W), F32)],
        queries,
        keys,
        values,
        step_sizes,
        forgetting,
        forgetting_bias.T,
        far=range(6),
        scratch=[pltpu.VMEM((tokens, W), BF16)] * 4
        + [
            pltpu.VMEM((tokens, W), F32),
            pltpu.VMEM((2, tokens), F32),
            pltpu.SemaphoreType.DMA((6,)),
        ],
        grant=67043328,
    )
    gathered = exchange(pairs, "x")
    weights.append(lax.ppermute(weights[0], TP, back))
    hot, slots = call(route_kernel, [((4 * tokens, tokens), BF16), ((2, tokens), F32)], ids.T)
    gathered, hot = lax.optimization_barrier((gathered, hot))
    pairs, prefix = call(
        compose_kernel, [((n_z, W, W), BF16), ((2 * W, W), F32)], pos, gathered, scalars=1
    )
    gathered = exchange(pairs, "z")
    send, mixed = call(
        readout_kernel,
        [((n_y, tokens, W), BF16), ((tokens, W), BF16)],
        pos,
        gathered,
        prefix,
        state_map,
        local,
        head_gain[None],
        blender,
        scalars=1,
    )
    own_skip = lax.dynamic_slice_in_dim(skip, (here[2] * 2 + here[3]) * W, W, 1)
    keep = call(branch_keep_kernel, [((n_y, tokens, W), BF16)], pos, mixed, blender, scalars=1)
    send, own_skip, keep = lax.optimization_barrier((swap_cores(send), own_skip, keep))
    branch = (keep.astype(F32) + send.astype(F32)).astype(BF16)
    branch, weights[1], weights[2] = lax.optimization_barrier((branch, weights[1], weights[2]))
    parts = exchange(branch, "y")
    parts, weights[1] = lax.optimization_barrier((parts, weights[1]))
    weights.append(lax.ppermute(weights[1], TP, ring))
    hidden, outgoing = call(
        dispatch_kernel,
        [((tokens, W), F32), ((n_z, n_y, n_x, 8, W), BF16)],
        pos,
        parts,
        own_skip,
        norm_gain[None],
        hot,
        scalars=1,
    )
    own = exchange(outgoing.reshape(n_z * n_x * n_y, 8, W), ("z", "y", "x"))
    own = own.reshape(n_z, n_y, n_x, 8, W)
    gains = norm_gain[None]
    acts, squares = call(
        expert_own_kernel,
        [((4, tokens, 2 * W), F32), ((tokens, W), F32)],
        pos,
        own,
        gains,
        *weights,
        scalars=1,
    )
    high, low = call(
        weigh_kernel,
        [((tokens, 4 * tokens), BF16)] * 2,
        slots,
        cluster_chance[None],
        within_chance.T,
    )
    other, acts = lax.optimization_barrier((swap_cores(own), acts))
    send, units = call(
        expert_kernel,
        [((n_z, n_y, n_x, 8, W), BF16), ((tokens, 4 * W), BF16)],
        pos,
        other,
        gains,
        acts,
        squares,
        *weights,
        scalars=1,
    )
    keep = call(
        expert_keep_kernel, [((n_z, n_y, n_x, 8, W), BF16)], pos, units, *weights, scalars=1
    )
    send, keep, high, low = lax.optimization_barrier((swap_cores(send), keep, high, low))
    summed = (keep.astype(F32) + send.astype(F32)).astype(BF16)
    returned = exchange(summed.reshape(n_z * n_x * n_y, 8, W), ("z", "y", "x"))
    returned = returned.reshape(n_z, n_y, n_x, 8, W)
    copies = call(combine_kernel, [((n_y, tokens, W), BF16)], returned, hidden, high, low)
    own = exchange(copies, "y")
    other = swap_cores(own)
    half = output_call(own_out_kernel, (tokens, width), pos, own)
    return output_call(other_out_kernel, (tokens, width), pos, other, half)


def solution(mesh):
    split = Mesh(mesh.devices.reshape(8, 4, 8, 2), ("z", "x", "y", "c"))
    in_specs = (
        P(SP, TP),
        P(SP, TP),
        P(SP, TP),
        P(SP, TP),
        P(SP, TP),
        P(SP, TP),
        P(TP),
        P(SP, None),
        P(TP, None),
        P(),
        P(SP),
        P(SP, None),
        P(SP, None),
        P(SP, None, TP),
        P(SP, None, TP),
        P(SP, TP, None),
    )
    out_specs = P(SP, None)

    return jax.shard_map(body, mesh=split, in_specs=in_specs, out_specs=out_specs, check_vma=False)
```

```python
import jax
import jax.numpy as jnp
from jax import lax
from jax.experimental import pallas as pl
from jax.experimental.pallas import tpu as pltpu
from jax.sharding import Mesh
from jax.sharding import PartitionSpec as P


SP = ("z", "x")
TP = ("y", "c")
F32 = jnp.float32
BF16 = jnp.bfloat16
SEG = 64
W = 128
DECAY = 0.6065306597126334
INTERPRET = False


def dot(a, b, contract=((1,), (0,))):
    return lax.dot_general(a, b, (contract, ((), ())), preferred_element_type=F32)


def halves(a):
    high = a.astype(BF16)
    return high, (a - high.astype(F32)).astype(BF16)


def mm(a, b, contract=((1,), (0,))):
    (a_high, a_low), (b_high, b_low) = halves(a), halves(b)
    return dot(a_high, b_high, contract) + (
        dot(a_high, b_low, contract) + dot(a_low, b_high, contract)
    )


def mm_exact(a, b, contract=((1,), (0,))):
    high, low = halves(a)
    return dot(high, b, contract) + dot(low, b, contract)


def iota(shape, dim):
    return lax.broadcasted_iota(jnp.int32, shape, dim)


def stack_heads(rows):
    first = iota(rows.shape, 1) < SEG
    zero = jnp.zeros_like(rows)
    return jnp.concatenate([jnp.where(first, rows, zero), jnp.where(first, zero, rows)], axis=0)


def flat_heads(stacked):
    half = stacked.shape[0] // 2
    return stacked[:half] + stacked[half:]


def eye128():
    return (iota((W, W), 0) == iota((W, W), 1)).astype(F32)


def same_head_ones():
    return (iota((W, W), 0) // SEG == iota((W, W), 1) // SEG).astype(F32).astype(BF16)


def pack_kernel(switch_ref, expansion_ref, contraction_ref, out_ref, held, sems):
    depth = switch_ref.shape[1]
    copies = [
        pltpu.make_async_copy(switch_ref.at[0], held.at[pl.ds(0, depth)], sems.at[0]),
        pltpu.make_async_copy(expansion_ref.at[0], held.at[pl.ds(depth, depth)], sems.at[1]),
    ]
    for n in range(depth // W):
        copies.append(
            pltpu.make_async_copy(
                contraction_ref.at[0, :, pl.ds(n * W, W)],
                held.at[pl.ds(2 * depth + n * W, W)],
                sems.at[2 + n],
            )
        )
    onward = [
        pltpu.make_async_copy(
            held.at[pl.ds(n * depth, depth)],
            out_ref.at[pl.ds(n * depth, depth)],
            sems.at[len(copies) + n],
        )
        for n in range(3)
    ]
    for copy in copies:
        copy.start()
    for n in range(2):
        copies[n].wait()
        onward[n].start()
    for copy in copies[2:]:
        copy.wait()
    onward[2].start()
    for copy in onward:
        copy.wait()


def hold_kernel(far_ref, near_ref, sem):
    copy = pltpu.make_async_copy(far_ref, near_ref, sem)
    copy.start()
    copy.wait()


def hold(data):
    return pl.pallas_call(
        hold_kernel,
        name="hold",
        out_shape=jax.ShapeDtypeStruct(data.shape, data.dtype),
        in_specs=[pl.BlockSpec(memory_space=pl.ANY)],
        out_specs=pl.BlockSpec(memory_space=pltpu.VMEM),
        scratch_shapes=[pltpu.SemaphoreType.DMA(())],
        compiler_params=pltpu.CompilerParams(vmem_limit_bytes=8 << 20),
        cost_estimate=pl.CostEstimate(
            flops=1_000_000_000, bytes_accessed=1_000_000, transcendentals=0
        ),
        interpret=INTERPRET,
    )(data)


def columns_of(rows):
    spare = jnp.zeros((6, rows.shape[1]), rows.dtype)
    return jnp.concatenate([rows, spare], axis=0).T


def mixer_kernel(*refs):
    pair_ref, map_ref, loc_ref = refs[6:9]
    held, sems = refs[9:15], refs[15]
    copies = [
        pltpu.make_async_copy(refs[n], held[n], sems.at[n]) for n in range(len(held))
    ]
    for copy in copies:
        copy.start()
    for copy in copies:
        copy.wait()
    q_ref, k_ref, v_ref, s_ref, f_ref, b_ref = held
    bias_columns = columns_of(b_ref[...])
    rows = q_ref.shape[0]
    chunks = rows // SEG
    query = q_ref[...].astype(F32)
    key = k_ref[...].astype(F32)
    value = v_ref[...].astype(F32)
    rate = 1.0 / (1.0 + jnp.exp(-s_ref[...].astype(F32)))
    bias = jnp.where(iota((rows, W), 1) < SEG, bias_columns[:, 0:1], bias_columns[:, 1:2])
    decay = bias - DECAY / (1.0 + jnp.exp(-f_ref[...]))
    removal = key * lax.rsqrt(mm_exact(key * key, same_head_ones()) + 1e-06)
    beta = removal * rate
    row, col = iota((rows, rows), 0), iota((rows, rows), 1)
    below = ((row // SEG == col // SEG) & (row >= col)).astype(F32).astype(BF16)
    high, low = halves(decay)
    rest = (decay - high.astype(F32) - low.astype(F32)).astype(BF16)
    total = dot(below, high) + (dot(below, low) + dot(below, rest))

    row, col = iota((W, W), 0), iota((W, W), 1)
    same = row // SEG == col // SEG
    strict = same & (row > col)
    inclusive = same & (row >= col)
    eye = eye128()

    part = []
    for n in range(chunks):
        at = slice(n * SEG, (n + 1) * SEG)
        cum = total[at]
        before = cum - decay[at]
        middle = cum[SEG // 2 - 1 : SEG // 2]
        closing = cum[SEG - 1 : SEG]
        up = jnp.exp(cum - middle)
        down = jnp.exp(middle - cum)
        left = jnp.exp(before - middle)
        opening = jnp.exp(middle)
        ending = jnp.exp(closing - middle)
        alpha = -removal[at] * left
        asked = query[at] * up
        beta_hat = beta[at] * down
        key_hat = key[at] * down
        scores = mm(
            jnp.concatenate([stack_heads(alpha), stack_heads(asked)], axis=0),
            jnp.concatenate([stack_heads(beta_hat), stack_heads(key_hat)], axis=0),
            ((1,), (1,)),
        )
        remove_remove = jnp.where(strict, scores[:W, :W], 0.0)
        remove_write = jnp.where(strict, scores[:W, W:], 0.0)
        read_remove = jnp.where(inclusive, scores[W:, :W], 0.0)
        read_write = jnp.where(inclusive, scores[W:, W:], 0.0)
        part.append(
            dict(
                near=remove_remove,
                write=remove_write,
                read=jnp.concatenate([read_remove, read_write], axis=1),
                read_remove=read_remove,
                alpha=stack_heads(alpha * opening),
                asked=stack_heads(asked * opening),
                value=stack_heads(value[at]),
                bar=jnp.concatenate(
                    [stack_heads(beta_hat * ending), stack_heads(key_hat * ending)], axis=0
                ),
                closing=jnp.exp(closing),
            )
        )
    inverse = [eye + jnp.where(row // 2 == col // 2, p["near"], 0.0) for p in part]
    for level in (4, 8, 16, 32, 64):
        joint = (row // level == col // level) & (row // (level // 2) != col // (level // 2))
        step = [mm(jnp.where(joint, p["near"], 0.0), x) for p, x in zip(part, inverse)]
        inverse = [x + mm(x, s) for x, s in zip(inverse, step)]
    wrote = [mm(p["write"], p["value"]) for p in part]
    solved = [
        mm(x, jnp.concatenate([p["alpha"], w], axis=1)) for x, p, w in zip(inverse, part, wrote)
    ]
    keeps, adds, reads, locals_ = [], [], [], []
    for p, s in zip(part, solved):
        absorb, carried = s[:, :W], s[:, W:]
        keeps.append(mm(absorb, p["bar"][:W], ((0,), (0,))) + eye * p["closing"])
        adds.append(
            mm(jnp.concatenate([carried, p["value"]], axis=0), p["bar"], ((0,), (0,)))
        )
        locals_.append(
            flat_heads(mm(p["read"], jnp.concatenate([carried, p["value"]], axis=0)))
        )
        reads.append(flat_heads(p["asked"] + mm(p["read_remove"], absorb)))
    map_ref[:SEG, :] = reads[0]
    loc_ref[:SEG, :] = locals_[0]
    run = jnp.concatenate([keeps[0], adds[0]], axis=0)
    for n in range(1, chunks):
        at = slice(n * SEG, (n + 1) * SEG)
        both = mm(reads[n], run, ((1,), (1,)))
        map_ref[at, :] = both[:, :W]
        loc_ref[at, :] = locals_[n] + both[:, W:]
        run = mm(run, keeps[n])
        run = jnp.concatenate([run[:W], run[W:] + adds[n]], axis=0)
    pair = jnp.concatenate([flat_heads(run[:W] - eye), flat_heads(run[W:])], axis=0).astype(BF16)
    for n in range(pair_ref.shape[0]):
        pair_ref[n] = pair


def unpack(pair):
    pair = pair.astype(F32)
    return stack_heads(pair[:SEG]), stack_heads(pair[SEG:])


def times(state, change):
    return state + mm_exact(state, change.astype(BF16))


def compose_kernel(pos_ref, got_ref, pair_ref, prefix_ref):
    mine = pos_ref[0]
    eye = eye128()
    change, add = unpack(got_ref[0])
    run = jnp.concatenate([eye + change, add], axis=0)
    prefix = jnp.where(mine > 0, run, jnp.concatenate([eye, jnp.zeros((W, W), F32)], axis=0))
    for n in range(1, got_ref.shape[0]):
        change, add = unpack(got_ref[n])
        run = times(run, change)
        run = jnp.concatenate([run[:W], run[W:] + add], axis=0)
        prefix = jnp.where(n < mine, run, prefix)
    pair = jnp.concatenate([flat_heads(run[:W] - eye), flat_heads(run[W:])], axis=0).astype(BF16)
    for n in range(pair_ref.shape[0]):
        pair_ref[n] = pair
    prefix_ref[...] = prefix


def readout_kernel(pos_ref, got_ref, prefix_ref, map_ref, loc_ref, gain_ref, w_ref, send_ref, mixed_ref):
    mine, core = pos_ref[1], pos_ref[3]
    state = jnp.where(mine > 0, unpack(got_ref[0])[1], 0.0)
    for n in range(1, got_ref.shape[0] - 1):
        change, add = unpack(got_ref[n])
        state = jnp.where(n < mine, times(state, change) + add, state)
    state = mm(state, prefix_ref[:W]) + prefix_ref[W:]
    out = loc_ref[...] + mm(map_ref[...], state, ((1,), (1,)))
    ones = same_head_ones()
    centered = out - mm_exact(out, ones) * (1.0 / SEG)
    spread = mm_exact(centered * centered, ones) * (1.0 / SEG)
    mixed = (centered * lax.rsqrt(spread + 0.00064) * gain_ref[...]).astype(BF16)
    mixed_ref[...] = mixed
    branch_columns(1 - core, mixed, w_ref, send_ref)


def branch_columns(core, mixed, w_ref, out_ref):
    for n in range(0, out_ref.shape[0], 2):
        sides = [w_ref[:, pl.ds(pl.multiple_of((2 * m + core) * W, W), W)] for m in (n, n + 1)]
        part = dot(mixed, jnp.concatenate(sides, axis=1)).astype(BF16)
        out_ref[n] = part[:, :W]
        out_ref[n + 1] = part[:, W:]


def branch_keep_kernel(pos_ref, mixed_ref, w_ref, keep_ref):
    branch_columns(pos_ref[3], mixed_ref[...], w_ref, keep_ref)


def route_kernel(names_ref, hot_ref, slots_ref):
    experts = 32
    tokens, places = names_ref.shape[1], hot_ref.shape[0]
    names = [names_ref[k : k + 1, :] for k in range(2)]
    hot = [(iota((experts, tokens), 0) == name).astype(F32) for name in names]
    earlier = (iota((tokens, tokens), 0) < iota((tokens, tokens), 1)).astype(F32).astype(BF16)
    ahead = dot((hot[0] + hot[1]).astype(BF16), earlier)
    ranks = [
        jnp.sum(hot[0] * ahead, axis=0, keepdims=True),
        jnp.sum(hot[1] * (ahead + hot[0]), axis=0, keepdims=True),
    ]
    ranks = [rank.astype(jnp.int32) for rank in ranks]
    slots = [
        ((name >> 2) << 7) + ((rank >> 3) << 5) + ((name & 3) << 3) + (rank & 7)
        for name, rank in zip(names, ranks)
    ]
    slots = [slot.astype(F32) for slot in slots]
    place = iota((places, tokens), 0).astype(F32)
    hot_ref[...] = ((place == slots[0]) | (place == slots[1])).astype(F32).astype(BF16)
    slots_ref[...] = jnp.concatenate(slots, axis=0)


def weigh_kernel(slots_ref, chance_ref, within_ref, high_ref, low_ref):
    tokens, places = high_ref.shape
    within = within_ref[...]
    shares = columns_of(chance_ref[...] * within / jnp.sum(within, axis=0, keepdims=True))
    found = columns_of(slots_ref[...])
    place = iota((tokens, places), 1).astype(F32)
    weight = jnp.zeros((tokens, places), F32)
    for k in range(2):
        weight = weight + jnp.where(place == found[:, k : k + 1], shares[:, k : k + 1], 0.0)
    high_ref[...], low_ref[...] = halves(weight)


def dispatch_kernel(pos_ref, parts_ref, skip_ref, gain_ref, hot_ref, hid_ref, out_ref):
    column = pl.multiple_of((pos_ref[2] * 2 + pos_ref[3]) * W, W)
    hidden = skip_ref[:, pl.ds(column, W)].astype(F32)
    for n in range(parts_ref.shape[0]):
        hidden = hidden + parts_ref[n].astype(F32)
    hid_ref[...] = hidden
    scaled = (hidden * gain_ref[:, pl.ds(column, W)]).astype(BF16)
    groups = out_ref.shape[1] // 2
    rows = dot(hot_ref[...], scaled)
    rows = rows.reshape(out_ref.shape[0], groups, *out_ref.shape[2:]).astype(BF16)
    out_ref[:, :groups] = rows
    out_ref[:, groups:] = rows


def block_at(n, core):
    return pl.multiple_of((2 * n + core) * W, W)


def columns_product(core, data_ref, gain_ref, weight_refs):
    ways, width = data_ref.shape[1], gain_ref.shape[1]
    blocks = [data_ref[:, n].astype(F32).reshape(-1, W) for n in range(ways)]
    squares = jnp.zeros(blocks[0].shape, F32)
    for n, block in enumerate(blocks):
        plain = block * (1.0 / gain_ref[:, pl.ds(block_at(n, core), W)])
        squares = squares + plain * plain
    data = jnp.concatenate([block.astype(BF16) for block in blocks], axis=1)
    acts = []
    for w_ref in weight_refs:
        sides = [
            jnp.concatenate(
                [w_ref[pl.ds(at + block_at(n, core), W), :] for n in range(ways)], axis=0
            )
            for at in (0, width)
        ]
        acts.append(dot(data, jnp.concatenate(sides, axis=1)))
    return squares, acts


def down_columns(core, hidden, width, weight_refs, out_ref):
    for n in range(0, out_ref.shape[1], 2):
        sides = [
            jnp.concatenate(
                [w_ref[pl.ds(2 * width + block_at(m, core), W), :] for w_ref in weight_refs], axis=0
            )
            for m in (n, n + 1)
        ]
        part = dot(hidden, jnp.concatenate(sides, axis=1))
        shape = (out_ref.shape[0], *out_ref.shape[2:])
        out_ref[:, n] = part[:, :W].reshape(shape).astype(BF16)
        out_ref[:, n + 1] = part[:, W:].reshape(shape).astype(BF16)


def expert_own_kernel(pos_ref, own_ref, gain_ref, w0, w1, w2, w3, act_ref, square_ref):
    square_ref[...], acts = columns_product(pos_ref[3], own_ref, gain_ref, (w0, w1, w2, w3))
    for n, act in enumerate(acts):
        act_ref[n] = act


def expert_kernel(
    pos_ref, other_ref, gain_ref, act_ref, square_ref, w0, w1, w2, w3, send_ref, hidden_ref
):
    core, width = pos_ref[3], gain_ref.shape[1]
    squares, acts = columns_product(1 - core, other_ref, gain_ref, (w0, w1, w2, w3))
    total = jnp.sum(squares + square_ref[...], axis=1, keepdims=True)
    scale = lax.rsqrt(total * (1.0 / width) + 1e-06)
    hidden = []
    for n, act in enumerate(acts):
        act = (act + act_ref[n]) * scale
        gate, up = act[:, :W], act[:, W:]
        hidden.append((gate / (1.0 + jnp.exp(-gate)) * up).astype(BF16))
    hidden = jnp.concatenate(hidden, axis=1)
    hidden_ref[...] = hidden
    down_columns(1 - core, hidden, width, (w0, w1, w2, w3), send_ref)


def expert_keep_kernel(pos_ref, hidden_ref, w0, w1, w2, w3, keep_ref):
    width = w0.shape[0] // 3
    down_columns(pos_ref[3], hidden_ref[...], width, (w0, w1, w2, w3), keep_ref)


def combine_kernel(ret_ref, hid_ref, high_ref, low_ref, out_ref):
    half = ret_ref.shape[1] // 2
    rows = ret_ref[:, :half].astype(F32) + ret_ref[:, half:].astype(F32)
    rows = rows.reshape(-1, W).astype(BF16)
    result = hid_ref[...] + (dot(high_ref[...], rows) + dot(low_ref[...], rows))
    result = result.astype(BF16)
    for n in range(out_ref.shape[0]):
        out_ref[n] = result


def columns_out(first, blocks_ref, out_ref, sems):
    copies = []
    for n in range(blocks_ref.shape[0]):
        column = pl.multiple_of((2 * n + first) * W, W)
        copies.append(
            pltpu.make_async_copy(blocks_ref.at[n], out_ref.at[:, pl.ds(column, W)], sems.at[n])
        )
    for copy in copies:
        copy.start()
    for copy in copies:
        copy.wait()


def own_out_kernel(pos_ref, own_ref, out_ref, sems):
    columns_out(pos_ref[3], own_ref, out_ref, sems)


def other_out_kernel(pos_ref, other_ref, half_ref, out_ref, sems):
    columns_out(1 - pos_ref[3], other_ref, out_ref, sems)


def output_call(kernel, shape, pos, blocks, *half):
    near = [pl.BlockSpec(memory_space=pltpu.SMEM), pl.BlockSpec(memory_space=pltpu.VMEM)]
    return pl.pallas_call(
        kernel,
        out_shape=jax.ShapeDtypeStruct(shape, BF16),
        in_specs=near + [pl.BlockSpec(memory_space=pl.ANY)] * len(half),
        out_specs=pl.BlockSpec(memory_space=pl.ANY),
        scratch_shapes=[pltpu.SemaphoreType.DMA((blocks.shape[0],))],
        input_output_aliases={2: 0} if half else {},
        compiler_params=pltpu.CompilerParams(vmem_limit_bytes=8 << 20),
        cost_estimate=pl.CostEstimate(
            flops=1_000_000_000, bytes_accessed=1_000_000, transcendentals=0
        ),
        interpret=INTERPRET,
    )(pos, blocks, *half)


def call(kernel, outs, *args, scalars=0, flops=2_000_000_000, far=(), scratch=(), grant=40 << 20):
    specs = [
        pl.BlockSpec(
            memory_space=pltpu.SMEM if n < scalars else pltpu.HBM if n in far else pltpu.VMEM
        )
        for n in range(len(args))
    ]
    shapes = [jax.ShapeDtypeStruct(shape, kind) for shape, kind in outs]
    result = pl.pallas_call(
        kernel,
        out_shape=shapes if len(shapes) > 1 else shapes[0],
        in_specs=specs,
        scratch_shapes=list(scratch),
        out_specs=[pl.BlockSpec(memory_space=pltpu.VMEM)] * len(shapes)
        if len(shapes) > 1
        else pl.BlockSpec(memory_space=pltpu.VMEM),
        compiler_params=pltpu.CompilerParams(vmem_limit_bytes=grant),
        cost_estimate=pl.CostEstimate(flops=flops, bytes_accessed=1_000_000, transcendentals=0),
        interpret=INTERPRET,
    )(*args)
    return result


def exchange(parts, axes):
    return lax.all_to_all(parts, axes, split_axis=0, concat_axis=0, tiled=True)


def swap_cores(data):
    return lax.ppermute(data, "c", [(0, 1), (1, 0)])


def body(
    queries,
    keys,
    values,
    step_sizes,
    forgetting,
    forgetting_bias,
    head_gain,
    skip,
    blender,
    norm_gain,
    cluster_chance,
    within_chance,
    ids,
    switch,
    expansion,
    contraction,
):
    n_z, n_x, n_y = (lax.axis_size(a) for a in ("z", "x", "y"))
    here = [lax.axis_index(a) for a in ("x", "z", "y", "c")]
    pos = jnp.stack(here).astype(jnp.int32)
    tokens, width = skip.shape

    ring = [(((y + 1) % n_y) * 2, y * 2) for y in range(n_y)]
    ring += [(((y - 1) % n_y) * 2 + 1, y * 2 + 1) for y in range(n_y)]
    back = [(target, source) for source, target in ring]
    packed = pl.pallas_call(
        pack_kernel,
        name="pack",
        out_shape=jax.ShapeDtypeStruct((3 * width, W), BF16),
        in_specs=[pl.BlockSpec(memory_space=pltpu.HBM)] * 3,
        out_specs=pl.BlockSpec(memory_space=pltpu.HBM),
        scratch_shapes=[
            pltpu.VMEM((3 * width, W), BF16),
            pltpu.SemaphoreType.DMA((5 + width // W,)),
        ],
        compiler_params=pltpu.CompilerParams(vmem_limit_bytes=67043328),
        interpret=INTERPRET,
    )(switch, expansion, contraction)
    weights = [packed]
    weights.append(lax.ppermute(weights[-1], TP, ring))
    pairs, state_map, local = call(
        mixer_kernel,
        [((n_x, W, W), BF16), ((tokens, W), F32), ((tokens, W), F32)],
        queries,
        keys,
        values,
        step_sizes,
        forgetting,
        forgetting_bias.T,
        far=range(6),
        scratch=[pltpu.VMEM((tokens, W), BF16)] * 4
        + [
            pltpu.VMEM((tokens, W), F32),
            pltpu.VMEM((2, tokens), F32),
            pltpu.SemaphoreType.DMA((6,)),
        ],
        grant=67043328,
    )
    gathered = exchange(pairs, "x")
    weights.append(lax.ppermute(weights[0], TP, back))
    hot, slots = call(route_kernel, [((4 * tokens, tokens), BF16), ((2, tokens), F32)], ids.T)
    gathered, hot = lax.optimization_barrier((gathered, hot))
    pairs, prefix = call(
        compose_kernel, [((n_z, W, W), BF16), ((2 * W, W), F32)], pos, gathered, scalars=1
    )
    gathered = exchange(pairs, "z")
    gathered, weights[1] = lax.optimization_barrier((gathered, weights[1]))
    weights.append(lax.ppermute(weights[1], TP, ring))
    send, mixed = call(
        readout_kernel,
        [((n_y, tokens, W), BF16), ((tokens, W), BF16)],
        pos,
        gathered,
        prefix,
        state_map,
        local,
        head_gain[None],
        blender,
        scalars=1,
    )
    keep = call(branch_keep_kernel, [((n_y, tokens, W), BF16)], pos, mixed, blender, scalars=1)
    near = hold(weights[1])
    send, keep, near = lax.optimization_barrier((swap_cores(send), keep, near))
    branch = (keep.astype(F32) + send.astype(F32)).astype(BF16)
    parts = exchange(branch, "y")
    hidden, outgoing = call(
        dispatch_kernel,
        [((tokens, W), F32), ((n_z, n_y, n_x, 8, W), BF16)],
        pos,
        parts,
        skip,
        norm_gain[None],
        hot,
        scalars=1,
    )
    own = exchange(outgoing.reshape(n_z * n_x * n_y, 8, W), ("z", "y", "x"))
    own = own.reshape(n_z, n_y, n_x, 8, W)
    gains = norm_gain[None]
    weights[1] = near
    acts, squares = call(
        expert_own_kernel,
        [((4, tokens, 2 * W), F32), ((tokens, W), F32)],
        pos,
        own,
        gains,
        *weights,
        scalars=1,
    )
    high, low = call(
        weigh_kernel,
        [((tokens, 4 * tokens), BF16)] * 2,
        slots,
        cluster_chance[None],
        within_chance.T,
    )
    other, acts = lax.optimization_barrier((swap_cores(own), acts))
    send, units = call(
        expert_kernel,
        [((n_z, n_y, n_x, 8, W), BF16), ((tokens, 4 * W), BF16)],
        pos,
        other,
        gains,
        acts,
        squares,
        *weights,
        scalars=1,
    )
    keep = call(
        expert_keep_kernel, [((n_z, n_y, n_x, 8, W), BF16)], pos, units, *weights, scalars=1
    )
    send, keep, high, low = lax.optimization_barrier((swap_cores(send), keep, high, low))
    summed = (keep.astype(F32) + send.astype(F32)).astype(BF16)
    returned = exchange(summed.reshape(n_z * n_x * n_y, 8, W), ("z", "y", "x"))
    returned = returned.reshape(n_z, n_y, n_x, 8, W)
    copies = call(combine_kernel, [((n_y, tokens, W), BF16)], returned, hidden, high, low)
    own = exchange(copies, "y")
    other = swap_cores(own)
    half = output_call(own_out_kernel, (tokens, width), pos, own)
    return output_call(other_out_kernel, (tokens, width), pos, other, half)


def solution(mesh):
    split = Mesh(mesh.devices.reshape(8, 4, 8, 2), ("z", "x", "y", "c"))
    in_specs = (
        P(SP, TP),
        P(SP, TP),
        P(SP, TP),
        P(SP, TP),
        P(SP, TP),
        P(SP, TP),
        P(TP),
        P(SP, None),
        P(TP, None),
        P(),
        P(SP),
        P(SP, None),
        P(SP, None),
        P(SP, None, TP),
        P(SP, None, TP),
        P(SP, TP, None),
    )
    out_specs = P(SP, None)

    return jax.shard_map(body, mesh=split, in_specs=in_specs, out_specs=out_specs, check_vma=False)
```

```python
import jax
import jax.numpy as jnp
from jax import lax
from jax.experimental import pallas as pl
from jax.experimental.pallas import tpu as pltpu
from jax.sharding import Mesh
from jax.sharding import PartitionSpec as P


SP = ("z", "x")
TP = ("y", "c")
F32 = jnp.float32
BF16 = jnp.bfloat16
SEG = 64
W = 128
DECAY = 0.6065306597126334
INTERPRET = False


def dot(a, b, contract=((1,), (0,))):
    return lax.dot_general(a, b, (contract, ((), ())), preferred_element_type=F32)


def halves(a):
    high = a.astype(BF16)
    return high, (a - high.astype(F32)).astype(BF16)


def mm(a, b, contract=((1,), (0,))):
    (a_high, a_low), (b_high, b_low) = halves(a), halves(b)
    return dot(a_high, b_high, contract) + (
        dot(a_high, b_low, contract) + dot(a_low, b_high, contract)
    )


def mm_exact(a, b, contract=((1,), (0,))):
    high, low = halves(a)
    return dot(high, b, contract) + dot(low, b, contract)


def iota(shape, dim):
    return lax.broadcasted_iota(jnp.int32, shape, dim)


def stack_heads(rows):
    first = iota(rows.shape, 1) < SEG
    zero = jnp.zeros_like(rows)
    return jnp.concatenate([jnp.where(first, rows, zero), jnp.where(first, zero, rows)], axis=0)


def flat_heads(stacked):
    half = stacked.shape[0] // 2
    return stacked[:half] + stacked[half:]


def eye128():
    return (iota((W, W), 0) == iota((W, W), 1)).astype(F32)


def same_head_ones():
    return (iota((W, W), 0) // SEG == iota((W, W), 1) // SEG).astype(F32).astype(BF16)


def pack_kernel(switch_ref, expansion_ref, contraction_ref, out_ref, held, sems):
    depth = switch_ref.shape[1]
    copies = [
        pltpu.make_async_copy(switch_ref.at[0], held.at[pl.ds(0, depth)], sems.at[0]),
        pltpu.make_async_copy(expansion_ref.at[0], held.at[pl.ds(depth, depth)], sems.at[1]),
    ]
    for n in range(depth // W):
        copies.append(
            pltpu.make_async_copy(
                contraction_ref.at[0, :, pl.ds(n * W, W)],
                held.at[pl.ds(2 * depth + n * W, W)],
                sems.at[2 + n],
            )
        )
    onward = [
        pltpu.make_async_copy(
            held.at[pl.ds(n * depth, depth)],
            out_ref.at[pl.ds(n * depth, depth)],
            sems.at[len(copies) + n],
        )
        for n in range(3)
    ]
    for copy in copies:
        copy.start()
    for n in range(2):
        copies[n].wait()
        onward[n].start()
    for copy in copies[2:]:
        copy.wait()
    onward[2].start()
    for copy in onward:
        copy.wait()


def hold_kernel(far_ref, near_ref, sem):
    copy = pltpu.make_async_copy(far_ref, near_ref, sem)
    copy.start()
    copy.wait()


def hold(data):
    return pl.pallas_call(
        hold_kernel,
        name="hold",
        out_shape=jax.ShapeDtypeStruct(data.shape, data.dtype),
        in_specs=[pl.BlockSpec(memory_space=pl.ANY)],
        out_specs=pl.BlockSpec(memory_space=pltpu.VMEM),
        scratch_shapes=[pltpu.SemaphoreType.DMA(())],
        compiler_params=pltpu.CompilerParams(vmem_limit_bytes=8 << 20),
        cost_estimate=pl.CostEstimate(
            flops=1_000_000_000, bytes_accessed=1_000_000, transcendentals=0
        ),
        interpret=INTERPRET,
    )(data)


def columns_of(rows):
    spare = jnp.zeros((6, rows.shape[1]), rows.dtype)
    return jnp.concatenate([rows, spare], axis=0).T


def mixer_kernel(*refs):
    pair_ref, map_ref, loc_ref = refs[6:9]
    held, sems = refs[9:15], refs[15]
    copies = [
        pltpu.make_async_copy(refs[n], held[n], sems.at[n]) for n in range(len(held))
    ]
    for copy in copies:
        copy.start()
    for copy in copies:
        copy.wait()
    q_ref, k_ref, v_ref, s_ref, f_ref, b_ref = held
    bias_columns = columns_of(b_ref[...])
    rows = q_ref.shape[0]
    chunks = rows // SEG
    query = q_ref[...].astype(F32)
    key = k_ref[...].astype(F32)
    value = v_ref[...].astype(F32)
    rate = 1.0 / (1.0 + jnp.exp(-s_ref[...].astype(F32)))
    bias = jnp.where(iota((rows, W), 1) < SEG, bias_columns[:, 0:1], bias_columns[:, 1:2])
    decay = bias - DECAY / (1.0 + jnp.exp(-f_ref[...]))
    removal = key * lax.rsqrt(mm_exact(key * key, same_head_ones()) + 1e-06)
    beta = removal * rate
    row, col = iota((rows, rows), 0), iota((rows, rows), 1)
    below = ((row // SEG == col // SEG) & (row >= col)).astype(F32).astype(BF16)
    high, low = halves(decay)
    rest = (decay - high.astype(F32) - low.astype(F32)).astype(BF16)
    total = dot(below, high) + (dot(below, low) + dot(below, rest))

    row, col = iota((W, W), 0), iota((W, W), 1)
    same = row // SEG == col // SEG
    strict = same & (row > col)
    inclusive = same & (row >= col)
    eye = eye128()

    part = []
    for n in range(chunks):
        at = slice(n * SEG, (n + 1) * SEG)
        cum = total[at]
        before = cum - decay[at]
        middle = cum[SEG // 2 - 1 : SEG // 2]
        closing = cum[SEG - 1 : SEG]
        up = jnp.exp(cum - middle)
        down = jnp.exp(middle - cum)
        left = jnp.exp(before - middle)
        opening = jnp.exp(middle)
        ending = jnp.exp(closing - middle)
        alpha = -removal[at] * left
        asked = query[at] * up
        beta_hat = beta[at] * down
        key_hat = key[at] * down
        scores = mm(
            jnp.concatenate([stack_heads(alpha), stack_heads(asked)], axis=0),
            jnp.concatenate([stack_heads(beta_hat), stack_heads(key_hat)], axis=0),
            ((1,), (1,)),
        )
        remove_remove = jnp.where(strict, scores[:W, :W], 0.0)
        remove_write = jnp.where(strict, scores[:W, W:], 0.0)
        read_remove = jnp.where(inclusive, scores[W:, :W], 0.0)
        read_write = jnp.where(inclusive, scores[W:, W:], 0.0)
        part.append(
            dict(
                near=remove_remove,
                write=remove_write,
                read=jnp.concatenate([read_remove, read_write], axis=1),
                read_remove=read_remove,
                alpha=stack_heads(alpha * opening),
                asked=stack_heads(asked * opening),
                value=stack_heads(value[at]),
                bar=jnp.concatenate(
                    [stack_heads(beta_hat * ending), stack_heads(key_hat * ending)], axis=0
                ),
                closing=jnp.exp(closing),
            )
        )
    inverse = [eye + jnp.where(row // 2 == col // 2, p["near"], 0.0) for p in part]
    for level in (4, 8, 16, 32, 64):
        joint = (row // level == col // level) & (row // (level // 2) != col // (level // 2))
        step = [mm(jnp.where(joint, p["near"], 0.0), x) for p, x in zip(part, inverse)]
        inverse = [x + mm(x, s) for x, s in zip(inverse, step)]
    wrote = [mm(p["write"], p["value"]) for p in part]
    solved = [
        mm(x, jnp.concatenate([p["alpha"], w], axis=1)) for x, p, w in zip(inverse, part, wrote)
    ]
    keeps, adds, reads, locals_ = [], [], [], []
    for p, s in zip(part, solved):
        absorb, carried = s[:, :W], s[:, W:]
        keeps.append(mm(absorb, p["bar"][:W], ((0,), (0,))) + eye * p["closing"])
        adds.append(
            mm(jnp.concatenate([carried, p["value"]], axis=0), p["bar"], ((0,), (0,)))
        )
        locals_.append(
            flat_heads(mm(p["read"], jnp.concatenate([carried, p["value"]], axis=0)))
        )
        reads.append(flat_heads(p["asked"] + mm(p["read_remove"], absorb)))
    map_ref[:SEG, :] = reads[0]
    loc_ref[:SEG, :] = locals_[0]
    run = jnp.concatenate([keeps[0], adds[0]], axis=0)
    for n in range(1, chunks):
        at = slice(n * SEG, (n + 1) * SEG)
        both = mm(reads[n], run, ((1,), (1,)))
        map_ref[at, :] = both[:, :W]
        loc_ref[at, :] = locals_[n] + both[:, W:]
        run = mm(run, keeps[n])
        run = jnp.concatenate([run[:W], run[W:] + adds[n]], axis=0)
    pair = jnp.concatenate([flat_heads(run[:W] - eye), flat_heads(run[W:])], axis=0).astype(BF16)
    for n in range(pair_ref.shape[0]):
        pair_ref[n] = pair


def unpack(pair):
    pair = pair.astype(F32)
    return stack_heads(pair[:SEG]), stack_heads(pair[SEG:])


def times(state, change):
    return state + mm_exact(state, change.astype(BF16))


def compose_kernel(pos_ref, got_ref, pair_ref, prefix_ref):
    mine = pos_ref[0]
    eye = eye128()
    change, add = unpack(got_ref[0])
    run = jnp.concatenate([eye + change, add], axis=0)
    prefix = jnp.where(mine > 0, run, jnp.concatenate([eye, jnp.zeros((W, W), F32)], axis=0))
    for n in range(1, got_ref.shape[0]):
        change, add = unpack(got_ref[n])
        run = times(run, change)
        run = jnp.concatenate([run[:W], run[W:] + add], axis=0)
        prefix = jnp.where(n < mine, run, prefix)
    pair = jnp.concatenate([flat_heads(run[:W] - eye), flat_heads(run[W:])], axis=0).astype(BF16)
    for n in range(pair_ref.shape[0]):
        pair_ref[n] = pair
    prefix_ref[...] = prefix


def readout_kernel(pos_ref, got_ref, prefix_ref, map_ref, loc_ref, gain_ref, w_ref, names_ref, send_ref, mixed_ref, hot_ref, slots_ref):
    mine, core = pos_ref[1], pos_ref[3]
    route_kernel(names_ref, hot_ref, slots_ref)
    state = jnp.where(mine > 0, unpack(got_ref[0])[1], 0.0)
    for n in range(1, got_ref.shape[0] - 1):
        change, add = unpack(got_ref[n])
        state = jnp.where(n < mine, times(state, change) + add, state)
    state = mm(state, prefix_ref[:W]) + prefix_ref[W:]
    out = loc_ref[...] + mm(map_ref[...], state, ((1,), (1,)))
    ones = same_head_ones()
    centered = out - mm_exact(out, ones) * (1.0 / SEG)
    spread = mm_exact(centered * centered, ones) * (1.0 / SEG)
    mixed = (centered * lax.rsqrt(spread + 0.00064) * gain_ref[...]).astype(BF16)
    mixed_ref[...] = mixed
    branch_columns(1 - core, mixed, w_ref, send_ref)


def branch_columns(core, mixed, w_ref, out_ref):
    for n in range(0, out_ref.shape[0], 2):
        sides = [w_ref[:, pl.ds(pl.multiple_of((2 * m + core) * W, W), W)] for m in (n, n + 1)]
        part = dot(mixed, jnp.concatenate(sides, axis=1)).astype(BF16)
        out_ref[n] = part[:, :W]
        out_ref[n + 1] = part[:, W:]


def branch_keep_kernel(pos_ref, mixed_ref, w_ref, keep_ref):
    branch_columns(pos_ref[3], mixed_ref[...], w_ref, keep_ref)


def route_kernel(names_ref, hot_ref, slots_ref):
    experts = 32
    tokens, places = names_ref.shape[1], hot_ref.shape[0]
    names = [names_ref[k : k + 1, :] for k in range(2)]
    hot = [(iota((experts, tokens), 0) == name).astype(F32) for name in names]
    earlier = (iota((tokens, tokens), 0) < iota((tokens, tokens), 1)).astype(F32).astype(BF16)
    ahead = dot((hot[0] + hot[1]).astype(BF16), earlier)
    ranks = [
        jnp.sum(hot[0] * ahead, axis=0, keepdims=True),
        jnp.sum(hot[1] * (ahead + hot[0]), axis=0, keepdims=True),
    ]
    ranks = [rank.astype(jnp.int32) for rank in ranks]
    slots = [
        ((name >> 2) << 7) + ((rank >> 3) << 5) + ((name & 3) << 3) + (rank & 7)
        for name, rank in zip(names, ranks)
    ]
    slots = [slot.astype(F32) for slot in slots]
    place = iota((places, tokens), 0).astype(F32)
    hot_ref[...] = ((place == slots[0]) | (place == slots[1])).astype(F32).astype(BF16)
    slots_ref[...] = jnp.concatenate(slots, axis=0)


def weigh_kernel(slots_ref, chance_ref, within_ref, high_ref, low_ref):
    tokens, places = high_ref.shape
    within = within_ref[...]
    shares = columns_of(chance_ref[...] * within / jnp.sum(within, axis=0, keepdims=True))
    found = columns_of(slots_ref[...])
    place = iota((tokens, places), 1).astype(F32)
    weight = jnp.zeros((tokens, places), F32)
    for k in range(2):
        weight = weight + jnp.where(place == found[:, k : k + 1], shares[:, k : k + 1], 0.0)
    high_ref[...], low_ref[...] = halves(weight)


def dispatch_kernel(pos_ref, parts_ref, skip_ref, gain_ref, hot_ref, hid_ref, out_ref):
    column = pl.multiple_of((pos_ref[2] * 2 + pos_ref[3]) * W, W)
    hidden = skip_ref[:, pl.ds(column, W)].astype(F32)
    for n in range(parts_ref.shape[0]):
        hidden = hidden + parts_ref[n].astype(F32)
    hid_ref[...] = hidden
    scaled = (hidden * gain_ref[:, pl.ds(column, W)]).astype(BF16)
    groups = out_ref.shape[1] // 2
    rows = dot(hot_ref[...], scaled)
    rows = rows.reshape(out_ref.shape[0], groups, *out_ref.shape[2:]).astype(BF16)
    out_ref[:, :groups] = rows
    out_ref[:, groups:] = rows


def block_at(n, core):
    return pl.multiple_of((2 * n + core) * W, W)


def columns_product(core, data_ref, gain_ref, weight_refs):
    ways, width = data_ref.shape[1], gain_ref.shape[1]
    blocks = [data_ref[:, n].astype(F32).reshape(-1, W) for n in range(ways)]
    squares = jnp.zeros(blocks[0].shape, F32)
    for n, block in enumerate(blocks):
        plain = block * (1.0 / gain_ref[:, pl.ds(block_at(n, core), W)])
        squares = squares + plain * plain
    data = jnp.concatenate([block.astype(BF16) for block in blocks], axis=1)
    acts = []
    for w_ref in weight_refs:
        sides = [
            jnp.concatenate(
                [w_ref[pl.ds(at + block_at(n, core), W), :] for n in range(ways)], axis=0
            )
            for at in (0, width)
        ]
        acts.append(dot(data, jnp.concatenate(sides, axis=1)))
    return squares, acts


def down_columns(core, hidden, width, weight_refs, out_ref):
    for n in range(0, out_ref.shape[1], 2):
        sides = [
            jnp.concatenate(
                [w_ref[pl.ds(2 * width + block_at(m, core), W), :] for w_ref in weight_refs], axis=0
            )
            for m in (n, n + 1)
        ]
        part = dot(hidden, jnp.concatenate(sides, axis=1))
        shape = (out_ref.shape[0], *out_ref.shape[2:])
        out_ref[:, n] = part[:, :W].reshape(shape).astype(BF16)
        out_ref[:, n + 1] = part[:, W:].reshape(shape).astype(BF16)


def expert_own_kernel(pos_ref, own_ref, gain_ref, w0, w1, w2, w3, act_ref, square_ref):
    square_ref[...], acts = columns_product(pos_ref[3], own_ref, gain_ref, (w0, w1, w2, w3))
    for n, act in enumerate(acts):
        act_ref[n] = act


def expert_kernel(
    pos_ref, other_ref, gain_ref, act_ref, square_ref, w0, w1, w2, w3, send_ref, hidden_ref
):
    core, width = pos_ref[3], gain_ref.shape[1]
    squares, acts = columns_product(1 - core, other_ref, gain_ref, (w0, w1, w2, w3))
    total = jnp.sum(squares + square_ref[...], axis=1, keepdims=True)
    scale = lax.rsqrt(total * (1.0 / width) + 1e-06)
    hidden = []
    for n, act in enumerate(acts):
        act = (act + act_ref[n]) * scale
        gate, up = act[:, :W], act[:, W:]
        hidden.append((gate / (1.0 + jnp.exp(-gate)) * up).astype(BF16))
    hidden = jnp.concatenate(hidden, axis=1)
    hidden_ref[...] = hidden
    down_columns(1 - core, hidden, width, (w0, w1, w2, w3), send_ref)


def expert_keep_kernel(pos_ref, hidden_ref, w0, w1, w2, w3, keep_ref):
    width = w0.shape[0] // 3
    down_columns(pos_ref[3], hidden_ref[...], width, (w0, w1, w2, w3), keep_ref)


def combine_kernel(ret_ref, hid_ref, high_ref, low_ref, out_ref):
    half = ret_ref.shape[1] // 2
    rows = ret_ref[:, :half].astype(F32) + ret_ref[:, half:].astype(F32)
    rows = rows.reshape(-1, W).astype(BF16)
    result = hid_ref[...] + (dot(high_ref[...], rows) + dot(low_ref[...], rows))
    result = result.astype(BF16)
    for n in range(out_ref.shape[0]):
        out_ref[n] = result


def columns_out(first, blocks_ref, out_ref, sems):
    copies = []
    for n in range(blocks_ref.shape[0]):
        column = pl.multiple_of((2 * n + first) * W, W)
        copies.append(
            pltpu.make_async_copy(blocks_ref.at[n], out_ref.at[:, pl.ds(column, W)], sems.at[n])
        )
    for copy in copies:
        copy.start()
    for copy in copies:
        copy.wait()


def own_out_kernel(pos_ref, own_ref, out_ref, sems):
    columns_out(pos_ref[3], own_ref, out_ref, sems)


def other_out_kernel(pos_ref, other_ref, half_ref, out_ref, sems):
    columns_out(1 - pos_ref[3], other_ref, out_ref, sems)


def output_call(kernel, shape, pos, blocks, *half):
    near = [pl.BlockSpec(memory_space=pltpu.SMEM), pl.BlockSpec(memory_space=pltpu.VMEM)]
    return pl.pallas_call(
        kernel,
        out_shape=jax.ShapeDtypeStruct(shape, BF16),
        in_specs=near + [pl.BlockSpec(memory_space=pl.ANY)] * len(half),
        out_specs=pl.BlockSpec(memory_space=pl.ANY),
        scratch_shapes=[pltpu.SemaphoreType.DMA((blocks.shape[0],))],
        input_output_aliases={2: 0} if half else {},
        compiler_params=pltpu.CompilerParams(vmem_limit_bytes=8 << 20),
        cost_estimate=pl.CostEstimate(
            flops=1_000_000_000, bytes_accessed=1_000_000, transcendentals=0
        ),
        interpret=INTERPRET,
    )(pos, blocks, *half)


def call(kernel, outs, *args, scalars=0, flops=2_000_000_000, far=(), scratch=(), grant=40 << 20):
    specs = [
        pl.BlockSpec(
            memory_space=pltpu.SMEM if n < scalars else pltpu.HBM if n in far else pltpu.VMEM
        )
        for n in range(len(args))
    ]
    shapes = [jax.ShapeDtypeStruct(shape, kind) for shape, kind in outs]
    result = pl.pallas_call(
        kernel,
        out_shape=shapes if len(shapes) > 1 else shapes[0],
        in_specs=specs,
        scratch_shapes=list(scratch),
        out_specs=[pl.BlockSpec(memory_space=pltpu.VMEM)] * len(shapes)
        if len(shapes) > 1
        else pl.BlockSpec(memory_space=pltpu.VMEM),
        compiler_params=pltpu.CompilerParams(vmem_limit_bytes=grant),
        cost_estimate=pl.CostEstimate(flops=flops, bytes_accessed=1_000_000, transcendentals=0),
        interpret=INTERPRET,
    )(*args)
    return result


def exchange(parts, axes):
    return lax.all_to_all(parts, axes, split_axis=0, concat_axis=0, tiled=True)


def swap_cores(data):
    return lax.ppermute(data, "c", [(0, 1), (1, 0)])


def body(
    queries,
    keys,
    values,
    step_sizes,
    forgetting,
    forgetting_bias,
    head_gain,
    skip,
    blender,
    norm_gain,
    cluster_chance,
    within_chance,
    ids,
    switch,
    expansion,
    contraction,
):
    n_z, n_x, n_y = (lax.axis_size(a) for a in ("z", "x", "y"))
    here = [lax.axis_index(a) for a in ("x", "z", "y", "c")]
    pos = jnp.stack(here).astype(jnp.int32)
    tokens, width = skip.shape

    ring = [(((y + 1) % n_y) * 2, y * 2) for y in range(n_y)]
    ring += [(((y - 1) % n_y) * 2 + 1, y * 2 + 1) for y in range(n_y)]
    back = [(target, source) for source, target in ring]
    packed = pl.pallas_call(
        pack_kernel,
        name="pack",
        out_shape=jax.ShapeDtypeStruct((3 * width, W), BF16),
        in_specs=[pl.BlockSpec(memory_space=pltpu.HBM)] * 3,
        out_specs=pl.BlockSpec(memory_space=pltpu.HBM),
        scratch_shapes=[
            pltpu.VMEM((3 * width, W), BF16),
            pltpu.SemaphoreType.DMA((5 + width // W,)),
        ],
        compiler_params=pltpu.CompilerParams(vmem_limit_bytes=67043328),
        interpret=INTERPRET,
    )(switch, expansion, contraction)
    weights = [packed]
    weights.append(lax.ppermute(weights[-1], TP, ring))
    pairs, state_map, local = call(
        mixer_kernel,
        [((n_x, W, W), BF16), ((tokens, W), F32), ((tokens, W), F32)],
        queries,
        keys,
        values,
        step_sizes,
        forgetting,
        forgetting_bias.T,
        far=range(6),
        scratch=[pltpu.VMEM((tokens, W), BF16)] * 4
        + [
            pltpu.VMEM((tokens, W), F32),
            pltpu.VMEM((2, tokens), F32),
            pltpu.SemaphoreType.DMA((6,)),
        ],
        grant=67043328,
    )
    gathered = exchange(pairs, "x")
    weights.append(lax.ppermute(weights[0], TP, back))
    pairs, prefix = call(
        compose_kernel, [((n_z, W, W), BF16), ((2 * W, W), F32)], pos, gathered, scalars=1
    )
    gathered = exchange(pairs, "z")
    gathered, weights[1] = lax.optimization_barrier((gathered, weights[1]))
    weights.append(lax.ppermute(weights[1], TP, ring))
    send, mixed, hot, slots = call(
        readout_kernel,
        [
            ((n_y, tokens, W), BF16),
            ((tokens, W), BF16),
            ((4 * tokens, tokens), BF16),
            ((2, tokens), F32),
        ],
        pos,
        gathered,
        prefix,
        state_map,
        local,
        head_gain[None],
        blender,
        ids.T,
        scalars=1,
    )
    keep = call(branch_keep_kernel, [((n_y, tokens, W), BF16)], pos, mixed, blender, scalars=1)
    near = hold(weights[1])
    send, keep, near = lax.optimization_barrier((swap_cores(send), keep, near))
    branch = (keep.astype(F32) + send.astype(F32)).astype(BF16)
    parts = exchange(branch, "y")
    hidden, outgoing = call(
        dispatch_kernel,
        [((tokens, W), F32), ((n_z, n_y, n_x, 8, W), BF16)],
        pos,
        parts,
        skip,
        norm_gain[None],
        hot,
        scalars=1,
    )
    own = exchange(outgoing.reshape(n_z * n_x * n_y, 8, W), ("z", "y", "x"))
    own = own.reshape(n_z, n_y, n_x, 8, W)
    gains = norm_gain[None]
    weights[1] = near
    acts, squares = call(
        expert_own_kernel,
        [((4, tokens, 2 * W), F32), ((tokens, W), F32)],
        pos,
        own,
        gains,
        *weights,
        scalars=1,
    )
    high, low = call(
        weigh_kernel,
        [((tokens, 4 * tokens), BF16)] * 2,
        slots,
        cluster_chance[None],
        within_chance.T,
    )
    other, acts = lax.optimization_barrier((swap_cores(own), acts))
    send, units = call(
        expert_kernel,
        [((n_z, n_y, n_x, 8, W), BF16), ((tokens, 4 * W), BF16)],
        pos,
        other,
        gains,
        acts,
        squares,
        *weights,
        scalars=1,
    )
    keep = call(
        expert_keep_kernel, [((n_z, n_y, n_x, 8, W), BF16)], pos, units, *weights, scalars=1
    )
    send, keep, high, low = lax.optimization_barrier((swap_cores(send), keep, high, low))
    summed = (keep.astype(F32) + send.astype(F32)).astype(BF16)
    returned = exchange(summed.reshape(n_z * n_x * n_y, 8, W), ("z", "y", "x"))
    returned = returned.reshape(n_z, n_y, n_x, 8, W)
    copies = call(combine_kernel, [((n_y, tokens, W), BF16)], returned, hidden, high, low)
    own = exchange(copies, "y")
    other = swap_cores(own)
    half = output_call(own_out_kernel, (tokens, width), pos, own)
    return output_call(other_out_kernel, (tokens, width), pos, other, half)


def solution(mesh):
    split = Mesh(mesh.devices.reshape(8, 4, 8, 2), ("z", "x", "y", "c"))
    in_specs = (
        P(SP, TP),
        P(SP, TP),
        P(SP, TP),
        P(SP, TP),
        P(SP, TP),
        P(SP, TP),
        P(TP),
        P(SP, None),
        P(TP, None),
        P(),
        P(SP),
        P(SP, None),
        P(SP, None),
        P(SP, None, TP),
        P(SP, None, TP),
        P(SP, TP, None),
    )
    out_specs = P(SP, None)

    return jax.shard_map(body, mesh=split, in_specs=in_specs, out_specs=out_specs, check_vma=False)
```

```python
import jax
import jax.numpy as jnp
from jax import lax
from jax.experimental import pallas as pl
from jax.experimental.pallas import tpu as pltpu
from jax.sharding import Mesh
from jax.sharding import PartitionSpec as P


SP = ("z", "x")
TP = ("y", "c")
F32 = jnp.float32
BF16 = jnp.bfloat16
SEG = 64
W = 128
DECAY = 0.6065306597126334
INTERPRET = False


def dot(a, b, contract=((1,), (0,))):
    return lax.dot_general(a, b, (contract, ((), ())), preferred_element_type=F32)


def halves(a):
    high = a.astype(BF16)
    return high, (a - high.astype(F32)).astype(BF16)


def mm(a, b, contract=((1,), (0,))):
    (a_high, a_low), (b_high, b_low) = halves(a), halves(b)
    return dot(a_high, b_high, contract) + (
        dot(a_high, b_low, contract) + dot(a_low, b_high, contract)
    )


def mm_one(a, b, contract=((1,), (0,))):
    return dot(a.astype(BF16), b.astype(BF16), contract)


def mm_exact(a, b, contract=((1,), (0,))):
    high, low = halves(a)
    return dot(high, b, contract) + dot(low, b, contract)


def iota(shape, dim):
    return lax.broadcasted_iota(jnp.int32, shape, dim)


def stack_heads(rows):
    first = iota(rows.shape, 1) < SEG
    zero = jnp.zeros_like(rows)
    return jnp.concatenate([jnp.where(first, rows, zero), jnp.where(first, zero, rows)], axis=0)


def flat_heads(stacked):
    half = stacked.shape[0] // 2
    return stacked[:half] + stacked[half:]


def eye128():
    return (iota((W, W), 0) == iota((W, W), 1)).astype(F32)


def same_head_ones():
    return (iota((W, W), 0) // SEG == iota((W, W), 1) // SEG).astype(F32).astype(BF16)


def pack_kernel(switch_ref, expansion_ref, contraction_ref, out_ref, held, sems):
    depth = switch_ref.shape[1]
    copies = [
        pltpu.make_async_copy(switch_ref.at[0], held.at[pl.ds(0, depth)], sems.at[0]),
        pltpu.make_async_copy(expansion_ref.at[0], held.at[pl.ds(depth, depth)], sems.at[1]),
    ]
    for n in range(depth // W):
        copies.append(
            pltpu.make_async_copy(
                contraction_ref.at[0, :, pl.ds(n * W, W)],
                held.at[pl.ds(2 * depth + n * W, W)],
                sems.at[2 + n],
            )
        )
    onward = [
        pltpu.make_async_copy(
            held.at[pl.ds(n * depth, depth)],
            out_ref.at[pl.ds(n * depth, depth)],
            sems.at[len(copies) + n],
        )
        for n in range(3)
    ]
    for copy in copies:
        copy.start()
    for n in range(2):
        copies[n].wait()
        onward[n].start()
    for copy in copies[2:]:
        copy.wait()
    onward[2].start()
    for copy in onward:
        copy.wait()


def hold_kernel(far_ref, near_ref, sem):
    copy = pltpu.make_async_copy(far_ref, near_ref, sem)
    copy.start()
    copy.wait()


def hold(data):
    return pl.pallas_call(
        hold_kernel,
        name="hold",
        out_shape=jax.ShapeDtypeStruct(data.shape, data.dtype),
        in_specs=[pl.BlockSpec(memory_space=pl.ANY)],
        out_specs=pl.BlockSpec(memory_space=pltpu.VMEM),
        scratch_shapes=[pltpu.SemaphoreType.DMA(())],
        compiler_params=pltpu.CompilerParams(vmem_limit_bytes=8 << 20),
        cost_estimate=pl.CostEstimate(
            flops=1_000_000_000, bytes_accessed=1_000_000, transcendentals=0
        ),
        interpret=INTERPRET,
    )(data)


def columns_of(rows):
    spare = jnp.zeros((6, rows.shape[1]), rows.dtype)
    return jnp.concatenate([rows, spare], axis=0).T


def mixer_kernel(*refs):
    pair_ref, map_ref, loc_ref = refs[6:9]
    held, sems = refs[9:15], refs[15]
    copies = [
        pltpu.make_async_copy(refs[n], held[n], sems.at[n]) for n in range(len(held))
    ]
    for copy in copies:
        copy.start()
    for copy in copies:
        copy.wait()
    q_ref, k_ref, v_ref, s_ref, f_ref, b_ref = held
    bias_columns = columns_of(b_ref[...])
    rows = q_ref.shape[0]
    chunks = rows // SEG
    query = q_ref[...].astype(F32)
    key = k_ref[...].astype(F32)
    value = v_ref[...].astype(F32)
    rate = 1.0 / (1.0 + jnp.exp(-s_ref[...].astype(F32)))
    bias = jnp.where(iota((rows, W), 1) < SEG, bias_columns[:, 0:1], bias_columns[:, 1:2])
    decay = bias - DECAY / (1.0 + jnp.exp(-f_ref[...]))
    removal = key * lax.rsqrt(mm_exact(key * key, same_head_ones()) + 1e-06)
    beta = removal * rate
    row, col = iota((rows, rows), 0), iota((rows, rows), 1)
    below = ((row // SEG == col // SEG) & (row >= col)).astype(F32).astype(BF16)
    high, low = halves(decay)
    rest = (decay - high.astype(F32) - low.astype(F32)).astype(BF16)
    total = dot(below, high) + (dot(below, low) + dot(below, rest))

    row, col = iota((W, W), 0), iota((W, W), 1)
    same = row // SEG == col // SEG
    strict = same & (row > col)
    inclusive = same & (row >= col)
    eye = eye128()

    part = []
    for n in range(chunks):
        at = slice(n * SEG, (n + 1) * SEG)
        cum = total[at]
        before = cum - decay[at]
        middle = cum[SEG // 2 - 1 : SEG // 2]
        closing = cum[SEG - 1 : SEG]
        up = jnp.exp(cum - middle)
        down = jnp.exp(middle - cum)
        left = jnp.exp(before - middle)
        opening = jnp.exp(middle)
        ending = jnp.exp(closing - middle)
        alpha = -removal[at] * left
        asked = query[at] * up
        beta_hat = beta[at] * down
        key_hat = key[at] * down
        scores = mm(
            jnp.concatenate([stack_heads(alpha), stack_heads(asked)], axis=0),
            jnp.concatenate([stack_heads(beta_hat), stack_heads(key_hat)], axis=0),
            ((1,), (1,)),
        )
        remove_remove = jnp.where(strict, scores[:W, :W], 0.0)
        remove_write = jnp.where(strict, scores[:W, W:], 0.0)
        read_remove = jnp.where(inclusive, scores[W:, :W], 0.0)
        read_write = jnp.where(inclusive, scores[W:, W:], 0.0)
        part.append(
            dict(
                near=remove_remove,
                write=remove_write,
                read=jnp.concatenate([read_remove, read_write], axis=1),
                read_remove=read_remove,
                alpha=stack_heads(alpha * opening),
                asked=stack_heads(asked * opening),
                value=stack_heads(value[at]),
                bar=jnp.concatenate(
                    [stack_heads(beta_hat * ending), stack_heads(key_hat * ending)], axis=0
                ),
                closing=jnp.exp(closing),
            )
        )
    inverse = [eye + jnp.where(row // 2 == col // 2, p["near"], 0.0) for p in part]
    for level in (4, 8, 16, 32, 64):
        joint = (row // level == col // level) & (row // (level // 2) != col // (level // 2))
        step = [mm(jnp.where(joint, p["near"], 0.0), x) for p, x in zip(part, inverse)]
        inverse = [x + mm(x, s) for x, s in zip(inverse, step)]
    wrote = [mm(p["write"], p["value"]) for p in part]
    solved = [
        mm(x, jnp.concatenate([p["alpha"], w], axis=1)) for x, p, w in zip(inverse, part, wrote)
    ]
    keeps, adds, reads, locals_ = [], [], [], []
    for p, s in zip(part, solved):
        absorb, carried = s[:, :W], s[:, W:]
        keeps.append(mm(absorb, p["bar"][:W], ((0,), (0,))) + eye * p["closing"])
        adds.append(
            mm(jnp.concatenate([carried, p["value"]], axis=0), p["bar"], ((0,), (0,)))
        )
        locals_.append(
            flat_heads(mm_one(p["read"], jnp.concatenate([carried, p["value"]], axis=0)))
        )
        reads.append(flat_heads(p["asked"] + mm_one(p["read_remove"], absorb)))
    map_ref[:SEG, :] = reads[0]
    loc_ref[:SEG, :] = locals_[0]
    run = jnp.concatenate([keeps[0], adds[0]], axis=0)
    for n in range(1, chunks):
        at = slice(n * SEG, (n + 1) * SEG)
        both = mm_one(reads[n], run, ((1,), (1,)))
        map_ref[at, :] = both[:, :W]
        loc_ref[at, :] = locals_[n] + both[:, W:]
        run = mm(run, keeps[n])
        run = jnp.concatenate([run[:W], run[W:] + adds[n]], axis=0)
    pair = jnp.concatenate([flat_heads(run[:W] - eye), flat_heads(run[W:])], axis=0).astype(BF16)
    for n in range(pair_ref.shape[0]):
        pair_ref[n] = pair


def unpack(pair):
    pair = pair.astype(F32)
    return stack_heads(pair[:SEG]), stack_heads(pair[SEG:])


def times(state, change):
    return state + mm_exact(state, change.astype(BF16))


def compose_kernel(pos_ref, got_ref, pair_ref, prefix_ref):
    mine = pos_ref[0]
    eye = eye128()
    change, add = unpack(got_ref[0])
    run = jnp.concatenate([eye + change, add], axis=0)
    prefix = jnp.where(mine > 0, run, jnp.concatenate([eye, jnp.zeros((W, W), F32)], axis=0))
    for n in range(1, got_ref.shape[0]):
        change, add = unpack(got_ref[n])
        run = times(run, change)
        run = jnp.concatenate([run[:W], run[W:] + add], axis=0)
        prefix = jnp.where(n < mine, run, prefix)
    pair = jnp.concatenate([flat_heads(run[:W] - eye), flat_heads(run[W:])], axis=0).astype(BF16)
    for n in range(pair_ref.shape[0]):
        pair_ref[n] = pair
    prefix_ref[...] = prefix


def readout_kernel(pos_ref, got_ref, prefix_ref, map_ref, loc_ref, gain_ref, w_ref, names_ref, send_ref, mixed_ref, hot_ref, slots_ref):
    mine, core = pos_ref[1], pos_ref[3]
    route_kernel(names_ref, hot_ref, slots_ref)
    state = jnp.where(mine > 0, unpack(got_ref[0])[1], 0.0)
    for n in range(1, got_ref.shape[0] - 1):
        change, add = unpack(got_ref[n])
        state = jnp.where(n < mine, times(state, change) + add, state)
    state = mm(state, prefix_ref[:W]) + prefix_ref[W:]
    out = loc_ref[...] + mm(map_ref[...], state, ((1,), (1,)))
    ones = same_head_ones()
    centered = out - mm_exact(out, ones) * (1.0 / SEG)
    spread = mm_exact(centered * centered, ones) * (1.0 / SEG)
    mixed = (centered * lax.rsqrt(spread + 0.00064) * gain_ref[...]).astype(BF16)
    mixed_ref[...] = mixed
    branch_columns(1 - core, mixed, w_ref, send_ref)


def branch_columns(core, mixed, w_ref, out_ref):
    for n in range(0, out_ref.shape[0], 2):
        sides = [w_ref[:, pl.ds(pl.multiple_of((2 * m + core) * W, W), W)] for m in (n, n + 1)]
        part = dot(mixed, jnp.concatenate(sides, axis=1)).astype(BF16)
        out_ref[n] = part[:, :W]
        out_ref[n + 1] = part[:, W:]


def branch_keep_kernel(pos_ref, mixed_ref, w_ref, keep_ref):
    branch_columns(pos_ref[3], mixed_ref[...], w_ref, keep_ref)


def route_kernel(names_ref, hot_ref, slots_ref):
    experts = 32
    tokens, places = names_ref.shape[1], hot_ref.shape[0]
    names = [names_ref[k : k + 1, :] for k in range(2)]
    hot = [(iota((experts, tokens), 0) == name).astype(F32) for name in names]
    earlier = (iota((tokens, tokens), 0) < iota((tokens, tokens), 1)).astype(F32).astype(BF16)
    ahead = dot((hot[0] + hot[1]).astype(BF16), earlier)
    ranks = [
        jnp.sum(hot[0] * ahead, axis=0, keepdims=True),
        jnp.sum(hot[1] * (ahead + hot[0]), axis=0, keepdims=True),
    ]
    ranks = [rank.astype(jnp.int32) for rank in ranks]
    slots = [
        ((name >> 2) << 7) + ((rank >> 3) << 5) + ((name & 3) << 3) + (rank & 7)
        for name, rank in zip(names, ranks)
    ]
    slots = [slot.astype(F32) for slot in slots]
    place = iota((places, tokens), 0).astype(F32)
    hot_ref[...] = ((place == slots[0]) | (place == slots[1])).astype(F32).astype(BF16)
    slots_ref[...] = jnp.concatenate(slots, axis=0)


def weigh_kernel(slots_ref, chance_ref, within_ref, high_ref, low_ref):
    tokens, places = high_ref.shape
    within = within_ref[...]
    shares = columns_of(chance_ref[...] * within / jnp.sum(within, axis=0, keepdims=True))
    found = columns_of(slots_ref[...])
    place = iota((tokens, places), 1).astype(F32)
    weight = jnp.zeros((tokens, places), F32)
    for k in range(2):
        weight = weight + jnp.where(place == found[:, k : k + 1], shares[:, k : k + 1], 0.0)
    high_ref[...], low_ref[...] = halves(weight)


def dispatch_kernel(pos_ref, parts_ref, skip_ref, gain_ref, hot_ref, hid_ref, out_ref):
    column = pl.multiple_of((pos_ref[2] * 2 + pos_ref[3]) * W, W)
    hidden = skip_ref[:, pl.ds(column, W)].astype(F32)
    for n in range(parts_ref.shape[0]):
        hidden = hidden + parts_ref[n].astype(F32)
    hid_ref[...] = hidden
    scaled = (hidden * gain_ref[:, pl.ds(column, W)]).astype(BF16)
    groups = out_ref.shape[1] // 2
    rows = dot(hot_ref[...], scaled)
    rows = rows.reshape(out_ref.shape[0], groups, *out_ref.shape[2:]).astype(BF16)
    out_ref[:, :groups] = rows
    out_ref[:, groups:] = rows


def block_at(n, core):
    return pl.multiple_of((2 * n + core) * W, W)


def columns_product(core, data_ref, gain_ref, weight_refs):
    ways, width = data_ref.shape[1], gain_ref.shape[1]
    blocks = [data_ref[:, n].astype(F32).reshape(-1, W) for n in range(ways)]
    squares = jnp.zeros(blocks[0].shape, F32)
    for n, block in enumerate(blocks):
        plain = block * (1.0 / gain_ref[:, pl.ds(block_at(n, core), W)])
        squares = squares + plain * plain
    data = jnp.concatenate([block.astype(BF16) for block in blocks], axis=1)
    acts = []
    for w_ref in weight_refs:
        sides = [
            jnp.concatenate(
                [w_ref[pl.ds(at + block_at(n, core), W), :] for n in range(ways)], axis=0
            )
            for at in (0, width)
        ]
        acts.append(dot(data, jnp.concatenate(sides, axis=1)))
    return squares, acts


def down_columns(core, hidden, width, weight_refs, out_ref):
    for n in range(0, out_ref.shape[1], 2):
        sides = [
            jnp.concatenate(
                [w_ref[pl.ds(2 * width + block_at(m, core), W), :] for w_ref in weight_refs], axis=0
            )
            for m in (n, n + 1)
        ]
        part = dot(hidden, jnp.concatenate(sides, axis=1))
        shape = (out_ref.shape[0], *out_ref.shape[2:])
        out_ref[:, n] = part[:, :W].reshape(shape).astype(BF16)
        out_ref[:, n + 1] = part[:, W:].reshape(shape).astype(BF16)


def expert_own_kernel(pos_ref, own_ref, gain_ref, w0, w1, w2, w3, act_ref, square_ref):
    square_ref[...], acts = columns_product(pos_ref[3], own_ref, gain_ref, (w0, w1, w2, w3))
    for n, act in enumerate(acts):
        act_ref[n] = act


def expert_kernel(
    pos_ref, other_ref, gain_ref, act_ref, square_ref, w0, w1, w2, w3, send_ref, hidden_ref
):
    core, width = pos_ref[3], gain_ref.shape[1]
    squares, acts = columns_product(1 - core, other_ref, gain_ref, (w0, w1, w2, w3))
    total = jnp.sum(squares + square_ref[...], axis=1, keepdims=True)
    scale = lax.rsqrt(total * (1.0 / width) + 1e-06)
    hidden = []
    for n, act in enumerate(acts):
        act = (act + act_ref[n]) * scale
        gate, up = act[:, :W], act[:, W:]
        hidden.append((gate / (1.0 + jnp.exp(-gate)) * up).astype(BF16))
    hidden = jnp.concatenate(hidden, axis=1)
    hidden_ref[...] = hidden
    down_columns(1 - core, hidden, width, (w0, w1, w2, w3), send_ref)


def expert_keep_kernel(pos_ref, hidden_ref, w0, w1, w2, w3, keep_ref):
    width = w0.shape[0] // 3
    down_columns(pos_ref[3], hidden_ref[...], width, (w0, w1, w2, w3), keep_ref)


def combine_kernel(ret_ref, hid_ref, high_ref, low_ref, out_ref):
    half = ret_ref.shape[1] // 2
    rows = ret_ref[:, :half].astype(F32) + ret_ref[:, half:].astype(F32)
    rows = rows.reshape(-1, W).astype(BF16)
    result = hid_ref[...] + (dot(high_ref[...], rows) + dot(low_ref[...], rows))
    result = result.astype(BF16)
    for n in range(out_ref.shape[0]):
        out_ref[n] = result


def columns_out(first, blocks_ref, out_ref, sems):
    copies = []
    for n in range(blocks_ref.shape[0]):
        column = pl.multiple_of((2 * n + first) * W, W)
        copies.append(
            pltpu.make_async_copy(blocks_ref.at[n], out_ref.at[:, pl.ds(column, W)], sems.at[n])
        )
    for copy in copies:
        copy.start()
    for copy in copies:
        copy.wait()


def own_out_kernel(pos_ref, own_ref, out_ref, sems):
    columns_out(pos_ref[3], own_ref, out_ref, sems)


def other_out_kernel(pos_ref, other_ref, half_ref, out_ref, sems):
    columns_out(1 - pos_ref[3], other_ref, out_ref, sems)


def output_call(kernel, shape, pos, blocks, *half):
    near = [pl.BlockSpec(memory_space=pltpu.SMEM), pl.BlockSpec(memory_space=pltpu.VMEM)]
    return pl.pallas_call(
        kernel,
        out_shape=jax.ShapeDtypeStruct(shape, BF16),
        in_specs=near + [pl.BlockSpec(memory_space=pl.ANY)] * len(half),
        out_specs=pl.BlockSpec(memory_space=pl.ANY),
        scratch_shapes=[pltpu.SemaphoreType.DMA((blocks.shape[0],))],
        input_output_aliases={2: 0} if half else {},
        compiler_params=pltpu.CompilerParams(vmem_limit_bytes=8 << 20),
        cost_estimate=pl.CostEstimate(
            flops=1_000_000_000, bytes_accessed=1_000_000, transcendentals=0
        ),
        interpret=INTERPRET,
    )(pos, blocks, *half)


def call(kernel, outs, *args, scalars=0, flops=2_000_000_000, far=(), scratch=(), grant=40 << 20):
    specs = [
        pl.BlockSpec(
            memory_space=pltpu.SMEM if n < scalars else pltpu.HBM if n in far else pltpu.VMEM
        )
        for n in range(len(args))
    ]
    shapes = [jax.ShapeDtypeStruct(shape, kind) for shape, kind in outs]
    result = pl.pallas_call(
        kernel,
        out_shape=shapes if len(shapes) > 1 else shapes[0],
        in_specs=specs,
        scratch_shapes=list(scratch),
        out_specs=[pl.BlockSpec(memory_space=pltpu.VMEM)] * len(shapes)
        if len(shapes) > 1
        else pl.BlockSpec(memory_space=pltpu.VMEM),
        compiler_params=pltpu.CompilerParams(vmem_limit_bytes=grant),
        cost_estimate=pl.CostEstimate(flops=flops, bytes_accessed=1_000_000, transcendentals=0),
        interpret=INTERPRET,
    )(*args)
    return result


def exchange(parts, axes):
    return lax.all_to_all(parts, axes, split_axis=0, concat_axis=0, tiled=True)


def swap_cores(data):
    return lax.ppermute(data, "c", [(0, 1), (1, 0)])


def body(
    queries,
    keys,
    values,
    step_sizes,
    forgetting,
    forgetting_bias,
    head_gain,
    skip,
    blender,
    norm_gain,
    cluster_chance,
    within_chance,
    ids,
    switch,
    expansion,
    contraction,
):
    n_z, n_x, n_y = (lax.axis_size(a) for a in ("z", "x", "y"))
    here = [lax.axis_index(a) for a in ("x", "z", "y", "c")]
    pos = jnp.stack(here).astype(jnp.int32)
    tokens, width = skip.shape

    ring = [(((y + 1) % n_y) * 2, y * 2) for y in range(n_y)]
    ring += [(((y - 1) % n_y) * 2 + 1, y * 2 + 1) for y in range(n_y)]
    back = [(target, source) for source, target in ring]
    packed = pl.pallas_call(
        pack_kernel,
        name="pack",
        out_shape=jax.ShapeDtypeStruct((3 * width, W), BF16),
        in_specs=[pl.BlockSpec(memory_space=pltpu.HBM)] * 3,
        out_specs=pl.BlockSpec(memory_space=pltpu.HBM),
        scratch_shapes=[
            pltpu.VMEM((3 * width, W), BF16),
            pltpu.SemaphoreType.DMA((5 + width // W,)),
        ],
        compiler_params=pltpu.CompilerParams(vmem_limit_bytes=67043328),
        interpret=INTERPRET,
    )(switch, expansion, contraction)
    weights = [packed]
    weights.append(lax.ppermute(weights[-1], TP, ring))
    pairs, state_map, local = call(
        mixer_kernel,
        [((n_x, W, W), BF16), ((tokens, W), F32), ((tokens, W), F32)],
        queries,
        keys,
        values,
        step_sizes,
        forgetting,
        forgetting_bias.T,
        far=range(6),
        scratch=[pltpu.VMEM((tokens, W), BF16)] * 4
        + [
            pltpu.VMEM((tokens, W), F32),
            pltpu.VMEM((2, tokens), F32),
            pltpu.SemaphoreType.DMA((6,)),
        ],
        grant=67043328,
    )
    gathered = exchange(pairs, "x")
    weights.append(lax.ppermute(weights[0], TP, back))
    pairs, prefix = call(
        compose_kernel, [((n_z, W, W), BF16), ((2 * W, W), F32)], pos, gathered, scalars=1
    )
    gathered = exchange(pairs, "z")
    gathered, weights[1] = lax.optimization_barrier((gathered, weights[1]))
    weights.append(lax.ppermute(weights[1], TP, ring))
    send, mixed, hot, slots = call(
        readout_kernel,
        [
            ((n_y, tokens, W), BF16),
            ((tokens, W), BF16),
            ((4 * tokens, tokens), BF16),
            ((2, tokens), F32),
        ],
        pos,
        gathered,
        prefix,
        state_map,
        local,
        head_gain[None],
        blender,
        ids.T,
        scalars=1,
    )
    keep = call(branch_keep_kernel, [((n_y, tokens, W), BF16)], pos, mixed, blender, scalars=1)
    near = hold(weights[1])
    send, keep, near = lax.optimization_barrier((swap_cores(send), keep, near))
    branch = (keep.astype(F32) + send.astype(F32)).astype(BF16)
    parts = exchange(branch, "y")
    hidden, outgoing = call(
        dispatch_kernel,
        [((tokens, W), F32), ((n_z, n_y, n_x, 8, W), BF16)],
        pos,
        parts,
        skip,
        norm_gain[None],
        hot,
        scalars=1,
    )
    own = exchange(outgoing.reshape(n_z * n_x * n_y, 8, W), ("z", "y", "x"))
    own = own.reshape(n_z, n_y, n_x, 8, W)
    gains = norm_gain[None]
    weights[1] = near
    acts, squares = call(
        expert_own_kernel,
        [((4, tokens, 2 * W), F32), ((tokens, W), F32)],
        pos,
        own,
        gains,
        *weights,
        scalars=1,
    )
    high, low = call(
        weigh_kernel,
        [((tokens, 4 * tokens), BF16)] * 2,
        slots,
        cluster_chance[None],
        within_chance.T,
    )
    other, acts = lax.optimization_barrier((swap_cores(own), acts))
    send, units = call(
        expert_kernel,
        [((n_z, n_y, n_x, 8, W), BF16), ((tokens, 4 * W), BF16)],
        pos,
        other,
        gains,
        acts,
        squares,
        *weights,
        scalars=1,
    )
    keep = call(
        expert_keep_kernel, [((n_z, n_y, n_x, 8, W), BF16)], pos, units, *weights, scalars=1
    )
    send, keep, high, low = lax.optimization_barrier((swap_cores(send), keep, high, low))
    summed = (keep.astype(F32) + send.astype(F32)).astype(BF16)
    returned = exchange(summed.reshape(n_z * n_x * n_y, 8, W), ("z", "y", "x"))
    returned = returned.reshape(n_z, n_y, n_x, 8, W)
    copies = call(combine_kernel, [((n_y, tokens, W), BF16)], returned, hidden, high, low)
    own = exchange(copies, "y")
    other = swap_cores(own)
    half = output_call(own_out_kernel, (tokens, width), pos, own)
    return output_call(other_out_kernel, (tokens, width), pos, other, half)


def solution(mesh):
    split = Mesh(mesh.devices.reshape(8, 4, 8, 2), ("z", "x", "y", "c"))
    in_specs = (
        P(SP, TP),
        P(SP, TP),
        P(SP, TP),
        P(SP, TP),
        P(SP, TP),
        P(SP, TP),
        P(TP),
        P(SP, None),
        P(TP, None),
        P(),
        P(SP),
        P(SP, None),
        P(SP, None),
        P(SP, None, TP),
        P(SP, None, TP),
        P(SP, TP, None),
    )
    out_specs = P(SP, None)

    return jax.shard_map(body, mesh=split, in_specs=in_specs, out_specs=out_specs, check_vma=False)
```
